32 devices in a mesh: sp: 4 (over x, core), dp: 8 (over z, y).
Axes of the slice: x: 2, y: 2, z: 4, core: 2. Of those that a mesh axis runs over, the one named last changes fastest.
Arguments:
- content_features_raw: bfloat16 [8, 512, 3072], P('dp', 'sp'), may hold values from -6 to 6
- memory_entering_matrix: bfloat16 [8, 512, 2048], P('dp', 'sp'), may hold values from -6 to 6
- memory_leaving_matrix: bfloat16 [8, 512, 2048], P('dp', 'sp'), may hold values from -6 to 6
- feature_switch_signal: bfloat16 [8, 512, 3072], P('dp', 'sp'), may hold values from -6 to 6
- ahead_increment_raw: float32 [8, 512, 48], P('dp', 'sp'), may hold values from -5 to 5
- reverse_increment_raw: float32 [8, 512, 48], P('dp', 'sp'), may hold values from -5 to 5
- additional_fading: float32 [8, 512, 48], P('dp', 'sp'), as said below
- content_filter_weights: bfloat16 [4, 3072], P(None, 'sp'), may hold values from -3 to 3
- entering_filter_weights: bfloat16 [4, 2048], P(None, 'sp'), may hold values from -3 to 3
- leaving_filter_weights: bfloat16 [4, 2048], P(None, 'sp'), may hold values from -3 to 3
- increment_offset_lanes: float32 [2, 48], P(None, 'sp'), may hold values from -0.5 to 0.5
- fading_speed_exponents: float32 [2, 48], P(None, 'sp'), as said below
- result_scaling_factor: bfloat16 [3072], replicated, may hold values from 0.099609375 to 1.8984375
Outputs:
- out: bfloat16 [8, 512, 3072], P('dp', 'sp')
The draws below stay inside these ranges and needn't reach their ends.
Inputs may be any that keep to these rules, and one draw needn't show every extreme that they name: Each head's row has a rate exp(fading_speed_exponents) between 0.3 / 4096 and 0.05. `additional_fading`: zero at most positions; elsewhere between log(0.5) and log(0.8).
All inputs are finite; a program needn't handle non-finite values.
Results may differ from the reference program's by a relative error of at most 0.0051.
Values may be sent and summed in bfloat16 or wider, within the bound.
A program may use at most 64 MiB of HBM per device.

```python
import math
import jax
import jax.numpy as jnp
from jax import lax

ATTENTION_LANES = 48
HEAD_DIM = 64
GROUPS = 16
STATE = 128
TAPS = 4
BLK = 128
TOK_DEV = 128
SEGMENTS = 8
SEG_LEN = 512
SEQ_LEN = 4096
D_SSM = 3072


def draw_fading_speed_exponents(key, part):
    first_key, second_key, third_key = jax.random.split(key, 3)
    share = 0.5
    slow_pick = jax.random.uniform(first_key, (2, ATTENTION_LANES), jnp.float32) < share
    slow_low = math.log(0.3 / SEQ_LEN)
    slow_high = math.log(min(2.0 / SEG_LEN, 0.015))
    slow_rate = jax.random.uniform(second_key, (2, ATTENTION_LANES), jnp.float32, slow_low, slow_high)
    fast_rate = jax.random.uniform(third_key, (2, ATTENTION_LANES), jnp.float32, math.log(0.015), math.log(0.05))
    return jnp.where(slow_pick, slow_rate, fast_rate).astype(jnp.float32)


def step_rates(key, salt):
    folded = jax.random.fold_in(key, salt)
    first_key, second_key = jax.random.split(folded)
    block_count = SEQ_LEN // TOK_DEV
    noise_draw = jnp.clip(jax.random.normal(first_key, (block_count, TOK_DEV, ATTENTION_LANES), jnp.float32), -3.0, 3.0)
    offset = jax.random.uniform(second_key, (block_count, 1, ATTENTION_LANES), jnp.float32, -1.2, 1.2)
    return (noise_draw + offset).reshape(SEGMENTS, SEG_LEN, ATTENTION_LANES).astype(jnp.float32)


def draw_ahead_increment_raw(key, part):
    return step_rates(key, 11)


def draw_reverse_increment_raw(key, part):
    return step_rates(key, 23)


def draw_additional_fading(key, part):
    first_key, second_key = jax.random.split(key)
    struck = jax.random.uniform(first_key, (SEGMENTS, SEG_LEN, ATTENTION_LANES), jnp.float32) < 3.0 / SEQ_LEN
    loss_log = jnp.log(jax.random.uniform(second_key, (SEGMENTS, SEG_LEN, ATTENTION_LANES), jnp.float32, 0.5, 0.8))
    return jnp.where(struck, loss_log, 0.0).astype(jnp.float32)


def levels(rng, extent, cuts, low, largest):
    def one(position, shards_of):
        steps = jax.random.uniform(jax.random.fold_in(jax.random.fold_in(rng, 6), position), (shards_of,), jnp.float32, low / len(cuts), largest / len(cuts))
        return jnp.repeat(jnp.exp(steps), extent[position] // shards_of).reshape((-1,) + (1,) * (len(extent) - position - 1))

    level = one(*cuts[0])
    for cut in cuts[1:]:
        level = level * one(*cut)
    return level


def gaussian(stream_key, extent, spread, limit, shards=(), kind=jnp.bfloat16):
    values = jax.random.normal(stream_key, extent, jnp.float32) * spread
    if len(shards) > 0:
        values = levels(stream_key, extent, shards, -0.22, 0.18) * values
    return jnp.clip(values, min=-limit, max=limit).astype(kind)


def setup_inputs(seed: int = 0) -> dict:
    streams_of = jax.random.split(jax.random.key(seed), 14)
    content_features_raw = gaussian(streams_of[0], (SEGMENTS, SEG_LEN, D_SSM), 1.0, 6.0, ((0, 8), (1, 4)))
    memory_entering_matrix = gaussian(streams_of[1], (SEGMENTS, SEG_LEN, GROUPS * STATE), 1.0, 6.0, ((0, 8), (1, 4)))
    memory_leaving_matrix = gaussian(streams_of[2], (SEGMENTS, SEG_LEN, GROUPS * STATE), 1.0, 6.0, ((0, 8), (1, 4)))
    feature_switch_signal = gaussian(streams_of[3], (SEGMENTS, SEG_LEN, D_SSM), 1.0, 6.0, ((0, 8), (1, 4)))
    ahead_increment_raw = draw_ahead_increment_raw(jax.random.fold_in(streams_of[13], 71), 0)
    reverse_increment_raw = draw_reverse_increment_raw(jax.random.fold_in(streams_of[13], 71), 0)
    additional_fading = draw_additional_fading(jax.random.fold_in(streams_of[13], 71), 0)
    content_filter_weights = gaussian(streams_of[7], (TAPS, D_SSM), TAPS ** -0.5, 3.0, ((1, 4),))
    entering_filter_weights = gaussian(streams_of[8], (TAPS, GROUPS * STATE), TAPS ** -0.5, 3.0, ((1, 4),))
    leaving_filter_weights = gaussian(streams_of[9], (TAPS, GROUPS * STATE), TAPS ** -0.5, 3.0, ((1, 4),))
    increment_offset_lanes = jnp.clip(jax.random.uniform(streams_of[10], (2, ATTENTION_LANES), jnp.float32, -0.5, 0.5) * levels(streams_of[10], (2, ATTENTION_LANES), ((1, 4),), -0.4, 0.0), -0.5, 0.5)
    fading_speed_exponents = draw_fading_speed_exponents(jax.random.fold_in(streams_of[13], 71), 0)
    result_scaling_factor = jnp.clip(1.0 + 0.18 * jax.random.normal(streams_of[12], (D_SSM,), jnp.float32), 0.099609375, 1.8984375).astype(jnp.bfloat16)
    return {"content_features_raw": content_features_raw, "memory_entering_matrix": memory_entering_matrix, "memory_leaving_matrix": memory_leaving_matrix, "feature_switch_signal": feature_switch_signal, "ahead_increment_raw": ahead_increment_raw, "reverse_increment_raw": reverse_increment_raw, "additional_fading": additional_fading, "content_filter_weights": content_filter_weights, "entering_filter_weights": entering_filter_weights, "leaving_filter_weights": leaving_filter_weights, "increment_offset_lanes": increment_offset_lanes, "fading_speed_exponents": fading_speed_exponents, "result_scaling_factor": result_scaling_factor}


def conv_silu(padded, weight, length):
    total_sum = padded[0:length].astype(jnp.float32) * weight[0].astype(jnp.float32)
    for lag_step in range(1, weight.shape[0]):
        total_sum = total_sum + padded[lag_step:lag_step + length].astype(jnp.float32) * weight[lag_step].astype(jnp.float32)
    return jax.nn.silu(total_sum).astype(jnp.bfloat16)

def direction(x_conv, b_conv, c_conv, rate, log_decay):
    overall_position_count = x_conv.shape[0]
    heads_within_group = rate.shape[1]
    block_count = overall_position_count // BLK
    x_blocks = x_conv.reshape(block_count, BLK, heads_within_group, HEAD_DIM)
    b_blocks = b_conv.reshape(block_count, BLK, STATE)
    c_blocks = c_conv.reshape(block_count, BLK, STATE)
    rate_blocks = rate.reshape(block_count, BLK, heads_within_group)
    log_blocks = log_decay.reshape(block_count, BLK, heads_within_group)
    lower_mask = jnp.tril(jnp.ones((BLK, BLK), bool))[:, :, None]

    def step(state, pieces):
        x_block, b_block, c_block, rate_block, log_block = pieces
        cum_log = jnp.cumsum(log_block, axis=0)
        scores = jnp.dot(c_block, b_block.T, preferred_element_type=jnp.float32)
        log_gaps = jnp.where(lower_mask, cum_log[:, None, :] - cum_log[None, :, :], -jnp.inf)
        weights = (scores[:, :, None] * jnp.exp(log_gaps) * rate_block[None, :, :]).astype(jnp.bfloat16)
        local_part = jnp.einsum('lsh,shp->lhp', weights.astype(jnp.float32), x_block.astype(jnp.float32))
        carried_part = jnp.einsum('ln,hpn->lhp', c_block.astype(jnp.float32), state, precision=lax.Precision.HIGHEST) * jnp.exp(cum_log)[:, :, None]
        block_log = cum_log[-1]
        scaled = (x_block.astype(jnp.float32) * (rate_block * jnp.exp(block_log[None, :] - cum_log))[:, :, None]).astype(jnp.bfloat16)
        update = jnp.einsum('shp,sn->hpn', scaled.astype(jnp.float32), b_block.astype(jnp.float32))
        new_state = state * jnp.exp(block_log)[:, None, None] + update
        return (new_state, local_part + carried_part)
    initial = jnp.zeros((heads_within_group, HEAD_DIM, STATE), jnp.float32)
    _, outputs = lax.scan(step, initial, (x_blocks, b_blocks, c_blocks, rate_blocks, log_blocks))
    return outputs.reshape(overall_position_count, heads_within_group * HEAD_DIM)

def reference(content_features_raw, memory_entering_matrix, memory_leaving_matrix, feature_switch_signal, ahead_increment_raw, reverse_increment_raw, additional_fading, content_filter_weights, entering_filter_weights, leaving_filter_weights, increment_offset_lanes, fading_speed_exponents, result_scaling_factor):
    overall_position_count = SEGMENTS * SEG_LEN
    width = ATTENTION_LANES * HEAD_DIM
    heads_within_group = ATTENTION_LANES // GROUPS
    group_width = heads_within_group * HEAD_DIM
    x_flat = content_features_raw.reshape(overall_position_count, width)
    b_flat = memory_entering_matrix.reshape(overall_position_count, GROUPS * STATE)
    c_flat = memory_leaving_matrix.reshape(overall_position_count, GROUPS * STATE)
    z_flat = feature_switch_signal.reshape(overall_position_count, width)
    fwd_flat = ahead_increment_raw.reshape(overall_position_count, ATTENTION_LANES)
    bwd_flat = reverse_increment_raw.reshape(overall_position_count, ATTENTION_LANES)
    additional_fading_flat_array = additional_fading.reshape(overall_position_count, ATTENTION_LANES)

    def one_group(group):
        col_x = (group * group_width).astype(jnp.int32)
        col_b = (group * STATE).astype(jnp.int32)
        column_per_head = (group * heads_within_group).astype(jnp.int32)
        x_part = lax.dynamic_slice_in_dim(x_flat, col_x, group_width, 1)
        b_part = lax.dynamic_slice_in_dim(b_flat, col_b, STATE, 1)
        c_part = lax.dynamic_slice_in_dim(c_flat, col_b, STATE, 1)
        z_part = lax.dynamic_slice_in_dim(z_flat, col_x, group_width, 1)
        pad_rows = ((2, TAPS - 3), (0, 0))
        x_conv = conv_silu(jnp.pad(x_part, pad_rows), lax.dynamic_slice_in_dim(content_filter_weights, col_x, group_width, 1), overall_position_count)
        b_conv = conv_silu(jnp.pad(b_part, pad_rows), lax.dynamic_slice_in_dim(entering_filter_weights, col_b, STATE, 1), overall_position_count)
        c_conv = conv_silu(jnp.pad(c_part, pad_rows), lax.dynamic_slice_in_dim(leaving_filter_weights, col_b, STATE, 1), overall_position_count)
        bias_part = lax.dynamic_slice_in_dim(increment_offset_lanes, column_per_head, heads_within_group, 1)
        decay_log_piece = lax.dynamic_slice_in_dim(fading_speed_exponents, column_per_head, heads_within_group, 1)
        spike_piece = lax.dynamic_slice_in_dim(additional_fading_flat_array, column_per_head, heads_within_group, 1)
        forward_step_rate = jax.nn.softplus(lax.dynamic_slice_in_dim(fwd_flat, column_per_head, heads_within_group, 1) + bias_part[0])
        backward_step_rate = jax.nn.softplus(lax.dynamic_slice_in_dim(bwd_flat, column_per_head, heads_within_group, 1) + bias_part[1])
        forward_log_decay = -jnp.exp(decay_log_piece[0]) * forward_step_rate + spike_piece
        backward_log_decay = -jnp.exp(decay_log_piece[1]) * backward_step_rate + spike_piece
        y_fwd = direction(x_conv, b_conv, c_conv, forward_step_rate, forward_log_decay)
        y_bwd = direction(x_conv[::-1], b_conv[::-1], c_conv[::-1], backward_step_rate[::-1], backward_log_decay[::-1])[::-1]
        mixed = (y_fwd + y_bwd).astype(jnp.bfloat16)
        gated = mixed.astype(jnp.float32) * jax.nn.silu(z_part.astype(jnp.float32))
        by_head = gated.reshape(overall_position_count, heads_within_group, HEAD_DIM)
        normed = by_head * lax.rsqrt(lax.optimization_barrier(jnp.mean(by_head * by_head, axis=-1, keepdims=True)) + 1e-06)
        gain_part = lax.dynamic_slice_in_dim(result_scaling_factor, col_x, group_width, 0).astype(jnp.float32)
        return (normed.reshape(overall_position_count, group_width) * gain_part).astype(jnp.bfloat16)
    results = lax.map(one_group, jnp.arange(GROUPS, dtype=jnp.int32))
    return jnp.transpose(results, (1, 0, 2)).reshape(SEGMENTS, SEG_LEN, width)
```

```python
import functools

import jax
import jax.numpy as jnp
from jax import lax
from jax.experimental import pallas as pl
from jax.experimental.pallas import tpu as pltpu
from jax.sharding import PartitionSpec as P

F32 = jnp.float32
BF16 = jnp.bfloat16
HEAD_DIM = 64
STATE = 128
EDGE = 8
HIGHEST = lax.Precision.HIGHEST


def levels_of(sp, dp, groups):
    found = []
    split = 1
    core = 2 if sp % 2 == 0 else 1
    inner = 2 if dp % 2 == 0 and groups % (2 * sp) == 0 else 1
    for axis, count, stride in (("sp", core, 1), ("sp", sp // core, core), ("dp", inner, 1)):
        if count > 1:
            found.append((axis, count, stride))
            split *= count
    return tuple(found), ("dp", dp // inner, inner)


def digit_of(level):
    axis, count, stride = level
    return lax.rem(lax.axis_index(axis) // stride, count)


def member_id(level, member):
    axis, count, stride = level
    return {axis: lax.axis_index(axis) + (member - digit_of(level)) * stride}


def kernel(levels, top, sizes, *refs):
    heads, pairs, chunks, sp, dp = sizes
    (x_ref, b_ref, c_ref, z_ref, ahead_ref, back_ref, spike_ref) = refs[:7]
    params = refs[7:12]
    gain_ref, out_ref = refs[12:14]
    (xc, bc, cc, y_ref, cum_ref, rate_ref, cum_t, rate_t, fac_ref) = refs[14:23]
    refs = refs[:14] + refs[23:]
    got, w_ref, prm_ref, halo_ref, edges, early_sem, edge_sem = (
        refs[14:19], refs[19], refs[20], refs[21], refs[22:28], refs[28], refs[29]
    )
    rest = list(refs[30:])
    depth = len(levels)
    logs = [rest.pop(0) for _ in range(depth + 1)]
    up_log = [rest.pop(0) for _ in range(depth + 1)]
    decay = [rest.pop(0) for _ in range(depth + 1)]
    log_sem = [rest.pop(0) for _ in range(depth + 1)]
    totals, up, down, stage, sems, incoming = ([] for _ in range(6))
    for _ in range(chunks):
        totals.append([rest.pop(0) for _ in range(depth + 1)])
        up.append([rest.pop(0) for _ in range(depth + 1)])
        down.append([rest.pop(0) for _ in range(depth)])
        stage.append([rest.pop(0) for _ in range(depth)])
        sems.append([rest.pop(0) for _ in range(depth + 1)])
        incoming.append(rest.pop(0))
    blk = x_ref.shape[0]
    per_pair = heads // pairs
    x_w = per_pair * HEAD_DIM
    b_w = 2 * STATE
    tiles = x_w // 128
    lane = lax.broadcasted_iota(jnp.int32, (blk, 128), 1)
    left = lane < HEAD_DIM
    row = lax.broadcasted_iota(jnp.int32, (blk, 128), 0)

    segment = ("sp", sp, 1)
    here, there = lax.axis_index("sp"), lax.axis_index("dp")
    rank = there * sp + here
    has_next, has_prev = rank < sp * dp - 1, rank > 0
    after = {"sp": lax.rem(here + 1, sp), "dp": lax.rem(there + (here + 1) // sp, dp)}
    before = {
        "sp": lax.rem(here + sp - 1, sp),
        "dp": lax.rem(there + dp - (sp - here) // sp, dp),
    }
    mesh_id = pl.DeviceIdType.MESH
    barrier = pltpu.get_barrier_semaphore()
    greeted = 0
    for level in levels + (top, segment):
        me = digit_of(level)
        for o in range(1, level[1]):
            target = member_id(level, lax.rem(me + o, level[1]))
            pl.semaphore_signal(barrier, inc=1, device_id=target, device_id_type=mesh_id)
            greeted += 1
    for present, target in ((has_next, after), (has_prev, before)):

        @pl.when(present)
        def _(target=target):
            pl.semaphore_signal(barrier, inc=1, device_id=target, device_id_type=mesh_id)

    filler = jnp.zeros((128 - 2 * heads, blk), F32)
    inc = jnp.concatenate([ahead_ref[...], back_ref[...], filler], axis=0).T
    spikes = jnp.concatenate([spike_ref[...], spike_ref[...], filler], axis=0).T
    count = sp * dp
    neighbours = (rank + count - 1) // count + (2 * count - 2 - rank) // count
    pl.semaphore_wait(barrier, greeted + neighbours)

    def edge_copy(i, direction):
        src = (x_ref, b_ref, c_ref)[i]
        start = blk - EDGE if direction == 0 else 0
        return pltpu.make_async_remote_copy(
            src_ref=src.at[pl.ds(start, EDGE), :],
            dst_ref=edges[3 * direction + i],
            send_sem=edge_sem.at[0, direction, i],
            recv_sem=edge_sem.at[1, direction, i],
            device_id=(after, before)[direction],
            device_id_type=mesh_id,
        )

    def param_copy(i, member, slot):
        return pltpu.make_async_remote_copy(
            src_ref=params[i],
            dst_ref=got[i].at[slot],
            send_sem=early_sem.at[0, i, member],
            recv_sem=early_sem.at[1, i, slot],
            device_id=member_id(segment, member),
            device_id_type=mesh_id,
        )

    for o in range(1, sp):
        for i in range(5):
            param_copy(i, lax.rem(here + o, sp), here).start()
    for direction, present in ((0, has_next), (1, has_prev)):

        @pl.when(present)
        def _(direction=direction):
            for i in range(3):
                edge_copy(i, direction).start()

    for i in range(5):
        got[i][here] = params[i][...]
    for o in range(1, sp):
        for i in range(5):
            s = lax.rem(here + o, sp)
            param_copy(i, s, s).wait_recv()
    prm_ref[...] = jnp.zeros_like(prm_ref)
    wide = got[3].shape[2]
    for q in range(sp):
        for kind in range(2):
            for d in range(2):
                at = slice(d * heads + q * wide, d * heads + (q + 1) * wide)
                prm_ref[kind : kind + 1, at] = got[3 + kind][q, d : d + 1, :]
        off = 0
        for i in range(3):
            n = got[i].shape[2]
            w_ref[0:4, off + q * n : off + (q + 1) * n] = got[i][q].astype(F32)
            off += n * sp
    rate = jax.nn.softplus(inc + prm_ref[0:1, :])
    log_decay = -jnp.exp(prm_ref[1:2, :]) * rate + spikes
    lower = (lane <= row).astype(F32)
    upper = (lane >= row).astype(F32)
    cum_f = jnp.dot(lower, log_decay, precision=HIGHEST, preferred_element_type=F32)
    cum_b = jnp.dot(upper, log_decay, precision=HIGHEST, preferred_element_type=F32)
    cum = jnp.where(lane < heads, cum_f, cum_b)
    lane1 = lane[0:1]
    last = jnp.where(lane1 < heads, cum_f[blk - 1 : blk], cum_b[0:1])
    cum_ref[...] = cum
    rate_ref[...] = rate
    cum_t[...] = cum.T
    rate_t[...] = rate.T
    fac_ref[...] = rate * jnp.exp(last - cum)
    logs[0][...] = jnp.broadcast_to(last, (8, 128))

    def rolled(ref, p):
        return pltpu.roll(ref[...], lax.rem(128 - p * per_pair, 128), 1)

    def two(cols, i):
        return jnp.where(left, cols[:, i : i + 1], cols[:, i + 1 : i + 2])

    def conv(src, col, width, off):
        at = pl.ds(pl.multiple_of(off + col, 128), width)
        v = src[:, pl.ds(pl.multiple_of(col, 128), width)].astype(F32)
        r = lax.broadcasted_iota(jnp.int32, (blk, width), 0)
        h0, h1, h2 = halo_ref[0:1, at], halo_ref[1:2, at], halo_ref[2:3, at]
        m1 = jnp.where(r == 0, h1, pltpu.roll(v, 1, 0))
        m2 = jnp.where(r == 0, h0, jnp.where(r == 1, h1, pltpu.roll(v, 2, 0)))
        p1 = jnp.where(r == blk - 1, h2, pltpu.roll(v, blk - 1, 0))
        s = m2 * w_ref[0:1, at] + m1 * w_ref[1:2, at] + v * w_ref[2:3, at] + p1 * w_ref[3:4, at]
        return (s / (1.0 + jnp.exp(-s))).astype(BF16)

    share = pairs // chunks
    x_total = x_ref.shape[1]
    b_total = b_ref.shape[1]

    def first(c, p, _):
        x_at = pl.ds(pl.multiple_of(p * x_w, 128), x_w)
        b_at = pl.ds(pl.multiple_of(p * b_w, 128), b_w)
        xv = conv(x_ref, p * x_w, x_w, 0)
        bv = conv(b_ref, p * b_w, b_w, x_total)
        xc[:, x_at] = xv
        bc[:, b_at] = bv
        cc[:, b_at] = conv(c_ref, p * b_w, b_w, x_total + b_total)
        cols = rolled(fac_ref, p)
        xf = xv.astype(F32)
        for d in range(2):
            scaled = jnp.concatenate(
                [
                    (xf[:, k * 128 : (k + 1) * 128] * two(cols, d * heads + 2 * k)).astype(BF16)
                    for k in range(tiles)
                ],
                axis=1,
            )
            u = lax.dot_general(scaled, bv, (((0,), (0,)), ((), ())), preferred_element_type=F32)
            half = x_w // 2
            rows = pl.ds(pl.multiple_of((p - c * share) * x_w, 128), x_w)
            totals[c][0][d, rows, :] = jnp.concatenate(
                [u[:half, :STATE], u[half:, STATE:]], axis=0
            ).astype(BF16)
        return 0

    for direction, present in ((0, has_prev), (1, has_next)):

        @pl.when(present)
        def _(direction=direction):
            for i in range(3):
                edge_copy(i, direction).wait_recv()

    off = 0
    for i in range(3):
        n = edges[i].shape[1]
        low = edges[i][...].astype(F32)
        high = edges[3 + i][...].astype(F32)
        halo_ref[0:2, off : off + n] = jnp.where(has_prev, low[EDGE - 2 :], 0.0)
        halo_ref[2:3, off : off + n] = jnp.where(has_next, high[0:1], 0.0)
        off += n
    def inner(p, _):
        x_at = pl.ds(pl.multiple_of(p * x_w, 128), x_w)
        b_at = pl.ds(pl.multiple_of(p * b_w, 128), b_w)
        bv, cv, xv = bc[:, b_at], cc[:, b_at], xc[:, x_at]
        cols = rolled(cum_ref, p)
        parts = []
        for g in range(2):
            scores = lax.dot_general(
                cv[:, g * STATE : (g + 1) * STATE],
                bv[:, g * STATE : (g + 1) * STATE],
                (((1,), (1,)), ((), ())),
                preferred_element_type=F32,
            )
            for i in range(per_pair // 2):
                h = g * (per_pair // 2) + i
                hf = p * per_pair + h
                gap_f = cols[:, h : h + 1] - cum_t[pl.ds(hf, 1), :]
                gap_b = cols[:, heads + h : heads + h + 1] - cum_t[pl.ds(heads + hf, 1), :]
                gap = jnp.where(lane < row, gap_f, jnp.where(lane > row, gap_b, 0.0))
                rf, rb = rate_t[pl.ds(hf, 1), :], rate_t[pl.ds(heads + hf, 1), :]
                scale = jnp.where(lane < row, rf, jnp.where(lane > row, rb, rf + rb))
                parts.append((scores * jnp.exp(gap) * scale).astype(BF16))
        for k in range(tiles):
            xt = xv[:, k * 128 : (k + 1) * 128]
            zero = jnp.zeros_like(xt)
            both = jnp.concatenate([jnp.where(left, xt, zero), jnp.where(left, zero, xt)], axis=0)
            w = jnp.concatenate([parts[2 * k], parts[2 * k + 1]], axis=1)
            y_ref[:, pl.ds(pl.multiple_of(p * x_w + k * 128, 128), 128)] = jnp.dot(
                w, both, preferred_element_type=F32
            )
        return 0

    def copy(src, dst, send, recv, level, member):
        return pltpu.make_async_remote_copy(
            src_ref=src,
            dst_ref=dst,
            send_sem=send,
            recv_sem=recv,
            device_id=member_id(level, member),
            device_id_type=pl.DeviceIdType.MESH,
        )

    every_level = levels + (top,)
    head_share = heads // chunks
    bases = [jnp.int32(0)]
    size = head_share
    for level in levels:
        size = size // level[1]
        bases.append(bases[-1] + digit_of(level) * size)
    pending = [[] for _ in range(chunks)]

    def head_rows(h):
        return pl.ds(pl.multiple_of(h * HEAD_DIM, HEAD_DIM), HEAD_DIM)

    def log_copy(k, member, slot):
        sem = log_sem[k]
        return copy(
            logs[k], up_log[k].at[slot], sem.at[0, member], sem.at[1, slot], every_level[k], member
        )

    def start_up(c, k):
        level = every_level[k]
        n, me = level[1], digit_of(level)
        total, sem = totals[c][k], sems[c][k]
        rows = total.shape[1] // n
        for o in range(1, n):
            m = lax.rem(me + o, n)
            if c == 0:
                pending[c].append(log_copy(k, m, me))
            if k < depth:
                part = total.at[:, pl.ds(pl.multiple_of(m * rows, 64), rows), :]
            else:
                part = total.at[jnp.where(m < me, 1, 0)]
            pending[c].append(
                copy(part, up[c][k].at[me], sem.at[0, m], sem.at[1, me], level, m)
            )
        for one in pending[c]:
            one.start()
        if k < depth:
            up[c][k][me] = total[:, pl.ds(pl.multiple_of(me * rows, 64), rows), :]
        if c == 0:
            up_log[k][me] = logs[k][...]

    def flush(c):
        for one in pending[c]:
            one.wait_send()
        pending[c].clear()

    def finish_up(c, k):
        level = every_level[k]
        n, me = level[1], digit_of(level)
        total, sem = totals[c][k], sems[c][k]
        flush(c)
        for o in range(1, n):
            s = lax.rem(me + o, n)
            if c == 0:
                log_copy(k, s, s).wait_recv()
            part = total.at[:, pl.ds(0, total.shape[1] // n), :] if k < depth else total.at[0]
            copy(part, up[c][k].at[s], sem.at[0, s], sem.at[1, s], level, s).wait_recv()
        if c == 0:

            def expand(m, _):
                decay[k][m] = jnp.exp(jnp.broadcast_to(up_log[k][m][0:1, :], (128, 128)).T)
                return 0

            lax.fori_loop(0, n, expand, 0)
            if k < depth:
                log_sum = up_log[k][0]
                for m in range(1, n):
                    log_sum = log_sum + up_log[k][m]
                logs[k + 1][...] = log_sum

    def gather(c, k):
        n = levels[k][1]
        base = c * head_share + bases[k + 1]
        part, new = up[c][k], totals[c][k + 1]

        def one_head(h, _):
            at = head_rows(h)
            f = part[0, 0, at, :].astype(F32)
            b = part[n - 1, 1, at, :].astype(F32)
            for m in range(1, n):
                r = n - 1 - m
                f = f * decay[k][m, pl.ds(base + h, 1), :] + part[m, 0, at, :].astype(F32)
                b = b * decay[k][r, pl.ds(heads + base + h, 1), :] + part[r, 1, at, :].astype(F32)
            new[0, at, :] = f.astype(BF16)
            new[1, at, :] = b.astype(BF16)
            return 0

        lax.fori_loop(0, new.shape[1] // HEAD_DIM, one_head, 0)

    def enter(c):
        n, me = top[1], digit_of(top)
        base = c * head_share + bases[-1]
        into = incoming[c]
        into[...] = jnp.zeros_like(into)

        def carry(s, d):
            def one_head(h, _):
                at = head_rows(h)
                factor = decay[depth][s, pl.ds(d * heads + base + h, 1), :]
                into[d, at, :] = into[d, at, :] * factor + up[c][depth][s, at, :].astype(F32)
                return 0

            lax.fori_loop(0, into.shape[1] // HEAD_DIM, one_head, 0)
            return 0

        lax.fori_loop(0, me, lambda s, _: carry(s, 0), 0)
        lax.fori_loop(0, n - 1 - me, lambda i, _: carry(n - 1 - i, 1), 0)

    def start_down(c, k):
        level = levels[k]
        n, me = level[1], digit_of(level)
        sem = sems[c][k]
        rows = totals[c][k].shape[1] // n
        base = c * head_share + bases[k + 1]
        source = incoming[c] if k == depth - 1 else down[c][k + 1]
        part, out = up[c][k], stage[c][k]

        def spread(h, _):
            at = head_rows(h)
            f = source[0, at, :].astype(F32)
            b = source[1, at, :].astype(F32)
            for m in range(n):
                r = n - 1 - m
                out[m, 0, at, :] = f.astype(BF16)
                out[r, 1, at, :] = b.astype(BF16)
                if m < n - 1:
                    f = f * decay[k][m, pl.ds(base + h, 1), :] + part[m, 0, at, :].astype(F32)
                    down_factor = decay[k][r, pl.ds(heads + base + h, 1), :]
                    b = b * down_factor + part[r, 1, at, :].astype(F32)
            return 0

        lax.fori_loop(0, rows // HEAD_DIM, spread, 0)
        mine = pl.ds(pl.multiple_of(me * rows, 64), rows)
        for o in range(1, n):
            m = lax.rem(me + o, n)
            pending[c].append(
                copy(out.at[m], down[c][k].at[:, mine, :], sem.at[2, m], sem.at[3, me], level, m)
            )
        for one in pending[c]:
            one.start()
        down[c][k][:, mine, :] = out[me]

    def finish_down(c, k):
        level = levels[k]
        n, me = level[1], digit_of(level)
        sem = sems[c][k]
        rows = totals[c][k].shape[1] // n
        flush(c)
        for o in range(1, n):
            s = lax.rem(me + o, n)
            theirs = pl.ds(pl.multiple_of(s * rows, 64), rows)
            copy(
                stage[c][k].at[s], down[c][k].at[:, theirs, :], sem.at[2, s], sem.at[3, s], level, s
            ).wait_recv()

    for c in range(chunks):
        lax.fori_loop(c * share, (c + 1) * share, functools.partial(first, c), 0)
        start_up(c, 0)
    for o in range(1, sp):
        for i in range(5):
            param_copy(i, lax.rem(here + o, sp), here).wait_send()
    for direction, present in ((0, has_next), (1, has_prev)):

        @pl.when(present)
        def _(direction=direction):
            for i in range(3):
                edge_copy(i, direction).wait_send()


    gaps = chunks * depth
    cuts = [(i * pairs) // gaps for i in range(gaps + 1)]
    for k in range(depth):
        for c in range(chunks):
            finish_up(c, k)
            gather(c, k)
            start_up(c, k + 1)
            at = k * chunks + c
            lax.fori_loop(cuts[at], cuts[at + 1], inner, 0)
    for c in range(chunks):
        finish_up(c, depth)
        enter(c)
        start_down(c, depth - 1)
    for k in reversed(range(1, depth)):
        for c in range(chunks):
            finish_down(c, k)
            start_down(c, k - 1)

    cum_ref[...] = jnp.exp(cum_ref[...])

    def last_part(c, p, _):
        cv = cc[:, pl.ds(pl.multiple_of(p * b_w, 128), b_w)]
        cols = rolled(cum_ref, p)
        carried = []
        for d in range(2):
            st = down[c][0][d, pl.ds(pl.multiple_of((p - c * share) * x_w, 128), x_w), :]
            got = [
                lax.dot_general(
                    cv[:, g * STATE : (g + 1) * STATE],
                    st,
                    (((1,), (1,)), ((), ())),
                    preferred_element_type=F32,
                )
                for g in range(2)
            ]
            carried.append(got)
        for k in range(tiles):
            cut = slice(k * 128, (k + 1) * 128)
            at = pl.ds(pl.multiple_of(p * x_w + k * 128, 128), 128)
            y = y_ref[:, at]
            for d in range(2):
                a, b = carried[d][0][:, cut], carried[d][1][:, cut]
                if 2 * k + 1 < per_pair // 2:
                    v = a
                elif 2 * k >= per_pair // 2:
                    v = b
                else:
                    v = jnp.where(left, a, b)
                y = y + v * two(cols, d * heads + 2 * k)
            z = z_ref[:, at].astype(F32)
            gated = y.astype(BF16).astype(F32) * (z / (1.0 + jnp.exp(-z)))
            square = gated * gated
            low = jnp.sum(jnp.where(left, square, 0.0), axis=1, keepdims=True)
            high = jnp.sum(jnp.where(left, 0.0, square), axis=1, keepdims=True)
            mean = jnp.where(left, low, high) * (1.0 / HEAD_DIM)
            out_ref[:, at] = (gated * lax.rsqrt(mean + 1e-6) * gain_ref[0:1, at]).astype(BF16)
        return 0

    for c in range(chunks):
        finish_down(c, 0)
        lax.fori_loop(c * share, (c + 1) * share, functools.partial(last_part, c), 0)


def local(sp, dp, x, b, c, z, ahead, back, spike, wx, wb, wc, offset, fading, gain):
    x, b, c, z = x[0], b[0], c[0], z[0]
    blk, x_total = x.shape
    groups = b.shape[1] // STATE
    heads = ahead.shape[2]
    pairs = groups // 2
    levels, top = levels_of(sp, dp, groups)
    scratch = [
        pltpu.VMEM((blk, x_total), BF16),
        pltpu.VMEM((blk, groups * STATE), BF16),
        pltpu.VMEM((blk, groups * STATE), BF16),
        pltpu.VMEM((blk, x_total), F32),
    ]
    scratch += [pltpu.VMEM((128, 128), F32)] * 5
    params = (wx, wb, wc, offset, fading)
    width = x_total + 2 * b.shape[1]
    early = [pltpu.VMEM((sp,) + one.shape, one.dtype) for one in params]
    early += [pltpu.VMEM((8, width), F32), pltpu.VMEM((8, 128), F32), pltpu.VMEM((8, width), F32)]
    early += [pltpu.VMEM((EDGE, one.shape[1]), BF16) for one in (x, b, c)] * 2
    early += [pltpu.SemaphoreType.DMA((2, 5, sp)), pltpu.SemaphoreType.DMA((2, 2, 3))]
    scratch += early
    split = 1
    for level in levels:
        split *= level[1]
    chunks = 2 if groups % (2 * split) == 0 else 1
    counts = [level[1] for level in levels] + [top[1]]
    scratch += [pltpu.VMEM((8, 128), F32)] * len(counts)
    scratch += [pltpu.VMEM((n, 8, 128), F32) for n in counts]
    scratch += [pltpu.VMEM((n, 128, 128), F32) for n in counts]
    scratch += [pltpu.SemaphoreType.DMA((2, n)) for n in counts]
    for _ in range(chunks):
        held = [x_total // chunks]
        for n in counts[:-1]:
            held.append(held[-1] // n)
        slabs = list(zip(counts[:-1], held[1:]))
        scratch += [pltpu.VMEM((2, rows, STATE), BF16) for rows in held]
        scratch += [pltpu.VMEM((n, 2, rows, STATE), BF16) for n, rows in slabs]
        scratch += [pltpu.VMEM((counts[-1], held[-1], STATE), BF16)]
        scratch += [pltpu.VMEM((2, rows, STATE), BF16) for rows in held[:-1]]
        scratch += [pltpu.VMEM((n, 2, rows, STATE), BF16) for n, rows in slabs]
        scratch += [pltpu.SemaphoreType.DMA((4, n)) for n in counts]
        scratch += [pltpu.VMEM((2, held[-1], STATE), F32)]
    out = pl.pallas_call(
        functools.partial(kernel, levels, top, (heads, pairs, chunks, sp, dp)),
        out_shape=jax.ShapeDtypeStruct((blk, x_total), BF16),
        in_specs=[pl.BlockSpec(memory_space=pltpu.VMEM)] * 13,
        out_specs=pl.BlockSpec(memory_space=pltpu.VMEM),
        scratch_shapes=scratch,
        compiler_params=pltpu.CompilerParams(
            collective_id=0, has_side_effects=True, vmem_limit_bytes=60 * 2**20
        ),
        name="mixer",
    )(x, b, c, z, ahead[0].T, back[0].T, spike[0].T, *params, gain.astype(F32)[None])
    return out[None]


def quad_kernel(sizes, *refs):
    heads, pairs, sp, dp = sizes
    nz = dp // 2
    rounds = nz.bit_length() - 1
    (x_hbm, b_hbm, c_hbm, z_hbm, ahead_hbm, back_hbm, spike_hbm) = refs[:7]
    params = refs[7:12]
    gain_hbm, out_hbm = refs[12:14]
    (in_x, in_b, in_c, in_z, inc, inc_out, gain_in, px, pb, pc) = refs[14:24]
    own, got = refs[24:29], refs[29:34]
    edges = refs[34:40]
    (work, w_ref, prm_ref, gain_ref, cum_ref, fac_ref, col_ref, cum_t, rate_t, mid_t) = refs[40:50]
    (xc, bt, cc, y_ref, sup, up_in, down_out, down_in) = refs[50:58]
    (logs, qlog, zsum, zlog, dec, wup, zdec, zwt) = refs[58:66]
    (tz, zin, zs, zr, mix_out, mix_in, out_v) = refs[66:73]
    (load_sem, prm_sem, edge_sem, half_sem, inc_sem, qlog_sem, zlog_sem) = refs[73:80]
    (up_sem, zsend_sem, zrecv_sem, down_sem, mix_sem, out_sem) = refs[80:86]

    hh = heads // 2
    hp = pairs // 2
    per_pair = heads // pairs
    tiles = per_pair * HEAD_DIM // 128
    blk = in_x.shape[0]
    tokens = 2 * blk
    x_half = in_x.shape[1] // 2
    b_half = in_b.shape[1] // 2
    x_w = per_pair * HEAD_DIM
    mesh_id = pl.DeviceIdType.MESH

    here, there = lax.axis_index("sp"), lax.axis_index("dp")
    core, cx = lax.rem(here, 2), here // 2
    cy, cz = lax.rem(there, 2), there // 2
    other = 1 - core
    me = cy * 2 + cx
    chip = there * 2 + cx
    chips = dp * 2
    has_next, has_prev = chip < chips - 1, chip > 0
    after, before = lax.rem(chip + 1, chips), lax.rem(chip + chips - 1, chips)
    partner = {"sp": cx * 2 + other}

    def chip_id(c, k):
        return {"sp": lax.rem(c, 2) * 2 + k, "dp": c // 2}

    def quad_id(qy, qx):
        return {"sp": qx * 2 + core, "dp": cz * 2 + qy}

    def z_id(z):
        return {"dp": z * 2 + cy}

    def member(i):
        qy = lax.rem(cy + lax.rem(i + 1, 2), 2)
        qx = lax.rem(cx + (3 - i) // 2, 2)
        return qy, qx, qy * 2 + qx

    def remote(src, dst, send, recv, target):
        return pltpu.make_async_remote_copy(
            src_ref=src, dst_ref=dst, send_sem=send, recv_sem=recv,
            device_id=target, device_id_type=mesh_id,
        )

    barrier = pltpu.get_barrier_semaphore()

    def greet(target):
        pl.semaphore_signal(barrier, inc=1, device_id=target, device_id_type=mesh_id)

    for o in range(1, sp):
        greet({"sp": lax.rem(here + o, sp)})
    for i in range(3):
        qy, qx, _ = member(i)
        greet(quad_id(qy, qx))
    for o in range(1, nz):
        greet(z_id(lax.rem(cz + o, nz)))
    for present, neighbour in ((has_next, after), (has_prev, before)):

        @pl.when(present)
        def _(neighbour=neighbour):
            for k in range(2):
                greet(chip_id(neighbour, k))

    loads = []

    def load(src, dst):
        one = pltpu.make_async_copy(src, dst, load_sem.at[len(loads)])
        one.start()
        loads.append(one)
        return one

    param_loads = [load(params[i], own[i]) for i in range(5)]
    mine = pl.ds(pl.multiple_of(core * hh, 8), hh)
    theirs = pl.ds(pl.multiple_of(other * hh, 8), hh)
    raw = (ahead_hbm, back_hbm, spike_hbm)
    inc_stage = [load(raw[i].at[theirs, :], inc_out.at[i]) for i in range(3)]
    inc_loads = [load(raw[i].at[mine, :], inc.at[core, i]) for i in range(3)]
    b_load = load(b_hbm, in_b)
    x_load = load(x_hbm, in_x)
    c_load = load(c_hbm, in_c)
    gain_load = load(gain_hbm, gain_in)
    z_load = load(z_hbm, in_z)

    for one in param_loads + inc_stage:
        one.wait()
    chip_greets = 2 * ((chip + chips - 1) // chips + (2 * chips - 2 - chip) // chips)
    pl.semaphore_wait(barrier, (sp - 1) + 3 + (nz - 1) + chip_greets)

    holder = here // 2
    slot = lax.rem(here, 2)

    def param_copy(i, x):
        return remote(
            own[i], got[i].at[slot], prm_sem.at[0, i, x], prm_sem.at[1, i, slot],
            {"sp": x * 2 + holder},
        )

    for x in range(2):
        elsewhere = x * 2 + holder != here

        @pl.when(elsewhere)
        def _(x=x):
            for i in range(5):
                param_copy(i, x).start()

        @pl.when(jnp.logical_not(elsewhere))
        def _():
            for i in range(5):
                got[i][slot] = own[i][...]

    def inc_copy(i):
        return remote(
            inc_out.at[i], inc.at[core, i], inc_sem.at[0, i], inc_sem.at[1, i], partner
        )

    for i in range(3):
        inc_copy(i).start()

    sources = (in_x, in_b, in_c)
    halves = (x_half, b_half, b_half)

    def edge_copy(i, low, k):
        half = halves[i]
        start = blk - EDGE if low else 0
        return remote(
            sources[i].at[pl.ds(start, EDGE), pl.ds(k * half, half)],
            edges[i if low else 3 + i],
            edge_sem.at[0, i, k],
            edge_sem.at[1, i, 0 if low else 1],
            chip_id(after if low else before, k),
        )

    sends_low = jnp.logical_and(core == 1, has_next)
    sends_high = jnp.logical_and(core == 0, has_prev)

    def half_copy(i):
        cut = pl.ds(pl.multiple_of(other * halves[i], 128), halves[i])
        return remote(
            sources[i].at[:, cut], (px, pb, pc)[i], half_sem.at[0, i], half_sem.at[1, i], partner
        )

    for i, one in ((1, b_load), (0, x_load), (2, c_load)):
        one.wait()

        @pl.when(sends_low)
        def _(i=i):
            for k in range(2):
                edge_copy(i, True, k).start()

        @pl.when(sends_high)
        def _(i=i):
            for k in range(2):
                edge_copy(i, False, k).start()

        half_copy(i).start()

    lane = lax.broadcasted_iota(jnp.int32, (blk, 128), 1)
    row = lax.broadcasted_iota(jnp.int32, (blk, 128), 0)
    left = lane < HEAD_DIM
    left1 = left[0:1]
    lower = (lane <= row).astype(F32)
    upper = (lane >= row).astype(F32)
    filler = jnp.zeros((128 - 2 * hh, blk), F32)

    for q in range(2):
        from_q = 2 * core + q != here

        @pl.when(from_q)
        def _(q=q):
            for i in range(5):
                remote(
                    own[i], got[i].at[q], prm_sem.at[0, i, 0], prm_sem.at[1, i, q], partner
                ).wait_recv()

    for one in inc_loads:
        one.wait()
    for i in range(3):
        remote(
            inc_out.at[i], inc.at[other, i], inc_sem.at[0, i], inc_sem.at[1, i], partner
        ).wait_recv()
    prm_ref[...] = jnp.zeros_like(prm_ref)
    wide = own[3].shape[1]
    for q in range(2):
        for kind in range(2):
            for d in range(2):
                at = slice(d * hh + q * wide, d * hh + (q + 1) * wide)
                prm_ref[kind : kind + 1, at] = got[3 + kind][q, d : d + 1, :]
        off = 0
        for i in range(3):
            n = own[i].shape[1]
            w_ref[0:4, off + q * n : off + (q + 1) * n] = got[i][q].astype(F32)
            off += 2 * n

    cums, rates = [], []
    for j in range(2):
        pre = jnp.concatenate([inc[j, 0], inc[j, 1], filler], axis=0).T
        spikes = jnp.concatenate([inc[j, 2], inc[j, 2], filler], axis=0).T
        rate = jax.nn.softplus(pre + prm_ref[0:1, :])
        log_decay = -jnp.exp(prm_ref[1:2, :]) * rate + spikes
        cum_f = jnp.dot(lower, log_decay, precision=HIGHEST, preferred_element_type=F32)
        cum_b = jnp.dot(upper, log_decay, precision=HIGHEST, preferred_element_type=F32)
        cums.append((cum_f, cum_b))
        rates.append(rate)
    ahead_lane = lane < hh
    ahead1 = ahead_lane[0:1]
    mid_f, mid_b = cums[0][0][blk - 1 : blk], cums[1][1][0:1]
    total = jnp.where(ahead1, mid_f + cums[1][0][blk - 1 : blk], cums[0][1][0:1] + mid_b)
    logs[...] = jnp.broadcast_to(total, (8, 128))

    def qlog_copy(i):
        qy, qx, q = member(i)
        return remote(
            logs, qlog.at[me], qlog_sem.at[0, i], qlog_sem.at[1, me], quad_id(qy, qx)
        )

    for i in range(3):
        qlog_copy(i).start()
    qlog[me] = logs[...]
    for j in range(2):
        cum_f, cum_b = cums[j]
        far = jnp.where(ahead_lane, mid_f if j == 1 else 0.0, mid_b if j == 0 else 0.0)
        near = jnp.where(ahead_lane, cum_f, cum_b)
        at = slice(j * blk, (j + 1) * blk)
        cum = near + far
        cum_ref[at, :] = jnp.exp(cum)
        fac_ref[at, :] = rates[j] * jnp.exp(total - cum)
        col_ref[at, :] = cum
        cum_t[:, at] = cum.T
        rate_t[:, at] = rates[j].T
        mid = rates[j] * jnp.exp(jnp.minimum((mid_f if j == 0 else mid_b) - near, 0.0))
        mid_t[:, at] = mid.T

    for k in range(gain_in.shape[0]):
        if k == 0:
            gain_load.wait()
        gain_ref[0:1, k * 128 : (k + 1) * 128] = gain_in[k : k + 1, :].astype(F32)

    for i in range(3):
        remote(sources[i].at[:, pl.ds(0, halves[i])], (px, pb, pc)[i], half_sem.at[0, i],
               half_sem.at[1, i], partner).wait_recv()
    for low, present in ((True, has_prev), (False, has_next)):

        @pl.when(present)
        def _(low=low):
            for i in range(3):
                edge_copy(i, low, 0).wait_recv()

    def rolled(v, p):
        return pltpu.roll(v, lax.rem(128 - p * per_pair, 128), 1)

    def two(cols, i):
        mask = lax.broadcasted_iota(jnp.int32, (cols.shape[0], 128), 1) < HEAD_DIM
        return jnp.where(mask, cols[:, i : i + 1], cols[:, i + 1 : i + 2])

    offsets = (0, 2 * own[0].shape[1], 2 * own[0].shape[1] + 2 * own[1].shape[1])

    def conv(i, col, spot):
        half = halves[i]
        mine_at = pl.ds(pl.multiple_of(core * half + col, 128), 128)
        at = pl.ds(pl.multiple_of(col, 128), 128)
        buf = work.at[spot]
        buf[pl.ds(pl.multiple_of(8 + core * blk, 8), blk), :] = sources[i][:, mine_at].astype(F32)
        buf[pl.ds(pl.multiple_of(8 + other * blk, 8), blk), :] = (px, pb, pc)[i][:, at].astype(F32)
        buf[0:8, :] = jnp.where(has_prev, edges[i][:, at].astype(F32), 0.0)
        high = jnp.where(has_next, edges[3 + i][:, at].astype(F32), 0.0)
        buf[8 + tokens : 16 + tokens, :] = high
        w_at = pl.ds(pl.multiple_of(offsets[i] + col, 128), 128)
        s = buf[6 : 6 + tokens, :] * w_ref[0:1, w_at]
        for k in range(1, 4):
            s = s + buf[6 + k : 6 + k + tokens, :] * w_ref[k : k + 1, w_at]
        h = 0.5 * s
        return h + h * jnp.tanh(h)

    def up_copy(k, i):
        qy, qx, q = member(i)
        return remote(
            sup.at[k, q], up_in.at[k, me], up_sem.at[0, k, i], up_sem.at[1, k, me],
            quad_id(qy, qx),
        )

    def wide_left(n):
        return lax.rem(lax.broadcasted_iota(jnp.int32, (128, n), 1), 128) < HEAD_DIM

    def first(k, i, _):
        _, _, p = member(i)
        if k < 2:
            g = 2 * p + k
            bt[g] = conv(1, g * 128, 0).T.astype(BF16)
        col = p * x_w + k * 128
        xv = conv(0, col, 1).astype(BF16)
        xc[:, pl.ds(pl.multiple_of(col, 128), 128)] = xv
        xf = xv.astype(F32)
        cols = rolled(fac_ref[...], p)
        rhs = jnp.concatenate(
            [(xf * two(cols, d * hh + 2 * k)).astype(BF16) for d in range(2)], axis=1
        )
        u = jnp.dot(bt[2 * p + k // 2], rhs, preferred_element_type=F32)
        if k == 1:
            v = jnp.dot(bt[2 * p + 1], rhs, preferred_element_type=F32)
            u = jnp.where(wide_left(256), u, v)
        u = u.astype(BF16)

        @pl.when(i < 3)
        def _():
            sup[k, p, 0] = u[:, :128]
            sup[k, p, 1] = u[:, 128:]
            up_copy(k, i).start()

        @pl.when(i == 3)
        def _():
            up_in[k, p, 0] = u[:, :128]
            up_in[k, p, 1] = u[:, 128:]

        return 0

    def inner(p, _):
        x_at = [pl.ds(pl.multiple_of(p * x_w + k * 128, 128), 128) for k in range(tiles)]
        for g in range(2):
            at = pl.ds(pl.multiple_of((2 * p + g) * 128, 128), 128)
            cc[:, at] = conv(2, (2 * p + g) * 128, g).astype(BF16)
        for r in range(2):
            rows = slice(r * blk, (r + 1) * blk)
            cols = rolled(col_ref[rows, :], p)
            mid_row = mid_f if r == 1 else mid_b
            shift = rolled(jnp.exp(jnp.minimum(col_ref[rows, :] - mid_row, 0.0)), p)
            parts = []
            for g in range(2):
                at = pl.ds(pl.multiple_of((2 * p + g) * 128, 128), 128)
                scores = jnp.dot(cc[rows, at], bt[2 * p + g], preferred_element_type=F32)
                on = scores[:, r * blk : (r + 1) * blk]
                away = scores[:, (1 - r) * blk : (2 - r) * blk]
                for h in range(g * per_pair // 2, (g + 1) * per_pair // 2):
                    f = pl.ds(p * per_pair + h, 1)
                    b = pl.ds(hh + p * per_pair + h, 1)
                    gap_f = cols[:, h : h + 1] - cum_t[f, rows]
                    gap_b = cols[:, hh + h : hh + h + 1] - cum_t[b, rows]
                    gap = jnp.where(lane < row, gap_f, jnp.where(lane > row, gap_b, 0.0))
                    rf, rb = rate_t[f, rows], rate_t[b, rows]
                    scale = jnp.where(lane < row, rf, jnp.where(lane > row, rb, rf + rb))
                    near = (on * jnp.exp(gap) * scale).astype(BF16)
                    d = 1 - r
                    c = d * hh + h
                    far_rows = slice((1 - r) * blk, (2 - r) * blk)
                    far_row = mid_t[f if d == 0 else b, far_rows]
                    far = (away * shift[:, c : c + 1] * far_row).astype(BF16)
                    parts.append(jnp.concatenate([near, far] if r == 0 else [far, near], axis=1))
            for k in range(tiles):
                xt = xc[:, x_at[k]]
                zero = jnp.zeros_like(xt)
                mask = lax.broadcasted_iota(jnp.int32, xt.shape, 1) < HEAD_DIM
                both = jnp.concatenate(
                    [jnp.where(mask, xt, zero), jnp.where(mask, zero, xt)], axis=0
                )
                w = jnp.concatenate([parts[2 * k], parts[2 * k + 1]], axis=1)
                y_ref[rows, x_at[k]] = jnp.dot(w, both, preferred_element_type=F32)
        return 0

    def zlog_copy(o):
        return remote(
            zsum, zlog.at[cz], zlog_sem.at[0, o], zlog_sem.at[1, cz], z_id(lax.rem(cz + o, nz))
        )

    def lanes_of(log_row, d, k):
        return two(rolled(log_row, me), d * hh + 2 * k)

    def quad_logs():
        for i in range(3):
            _, _, q = member(i)
            remote(
                logs, qlog.at[q], qlog_sem.at[0, i], qlog_sem.at[1, q], partner
            ).wait_recv()
        zsum[...] = qlog[0] + qlog[1] + qlog[2] + qlog[3]
        for o in range(1, nz):
            zlog_copy(o).start()
        zlog[cz] = zsum[...]
        for d in range(2):
            for k in range(tiles):
                each = [lanes_of(qlog[q], d, k) for q in range(4)]
                reach = jnp.zeros_like(each[0])
                for q in reversed(range(4)) if d == 0 else range(4):
                    dec[q, d, k] = jnp.exp(each[q])
                    wup[q, d, k] = jnp.exp(reach)
                    reach = reach + each[q]

    def z_logs():
        for o in range(1, nz):
            s = lax.rem(cz + o, nz)
            remote(
                zsum, zlog.at[s], zlog_sem.at[0, o], zlog_sem.at[1, s], partner
            ).wait_recv()
        reach = [[jnp.zeros((8, 128), F32) for _ in range(2)] for _ in range(rounds)]
        for s in range(nz):
            for r in range(rounds):
                h = 1 << r
                pos = lax.rem(cz, 2 * h)
                middle = cz - pos + h
                f_in = jnp.logical_and(s >= middle, s < cz)
                b_in = jnp.logical_and(s > cz, s < middle)
                reach[r][0] = reach[r][0] + jnp.where(f_in, zlog[s], 0.0)
                reach[r][1] = reach[r][1] + jnp.where(b_in, zlog[s], 0.0)
        for d in range(2):
            for k in range(tiles):
                zdec[d, k] = jnp.exp(lanes_of(zsum[...], d, k))
                for r in range(rounds):
                    zwt[r, d, k] = jnp.exp(lanes_of(reach[r][d], d, k))

    def combine(k):
        for i in range(3):
            _, _, q = member(i)
            remote(
                sup.at[k, q], up_in.at[k, q], up_sem.at[0, k, i], up_sem.at[1, k, q], partner
            ).wait_recv()
        for d in range(2):
            acc = up_in[k, 0, d].astype(F32) * wup[0, d, k, 0:1, :]
            for q in range(1, 4):
                acc = acc + up_in[k, q, d].astype(F32) * wup[q, d, k, 0:1, :]
            tz[k, d] = acc
            zin[k, d] = jnp.zeros_like(acc)

    def z_copy(r, k, o, d):
        return remote(
            zs.at[r, k], zr.at[r, k], zsend_sem.at[r, k, o - 1], zrecv_sem.at[r, k],
            z_id(cz + o if d == 0 else cz - o),
        )

    def z_parts(r):
        h = 1 << r
        pos = lax.rem(cz, 2 * h)
        return h, pos, ((0, pos == h - 1), (1, pos == h))

    def z_send(r, k):
        h, pos, senders = z_parts(r)
        for d, sender in senders:

            @pl.when(sender)
            def _(d=d):
                zs[r, k] = (zin[k, d] * zdec[d, k, 0:1, :] + tz[k, d]).astype(BF16)
                for o in reversed(range(1, h + 1)):
                    z_copy(r, k, o, d).start()

    def z_recv(r, k):
        h, pos, _ = z_parts(r)
        z_copy(r, k, 1, 0).wait_recv()
        for d, receiver in ((0, pos >= h), (1, pos < h)):

            @pl.when(receiver)
            def _(d=d):
                zin[k, d] = zin[k, d] + zr[r, k].astype(F32) * zwt[r, d, k, 0:1, :]

    def down_copy(k, i):
        qy, qx, q = member(i)
        return remote(
            down_out.at[k, q], down_in.at[k, me], down_sem.at[0, k, i], down_sem.at[1, k, me],
            quad_id(qy, qx),
        )

    def down(k):
        for d in range(2):
            g = zin[k, d]
            order = list(range(4)) if d == 0 else list(reversed(range(4)))
            for q in order:
                down_out[k, q, d] = g.astype(BF16)
                if q != order[-1]:
                    g = g * dec[q, d, k, 0:1, :] + up_in[k, q, d].astype(F32)
        for i in range(3):
            down_copy(k, i).start()
        down_in[k, me] = down_out[k, me]

    def gate(mixed, at):
        z = in_z[:, at].astype(F32)
        half_z = 0.5 * z
        gated = mixed.astype(F32) * (half_z + half_z * jnp.tanh(half_z))
        square = gated * gated
        low = jnp.sum(jnp.where(left, square, 0.0), axis=1, keepdims=True)
        high = jnp.sum(jnp.where(left, 0.0, square), axis=1, keepdims=True)
        mean = jnp.where(left, low, high) * (1.0 / HEAD_DIM)
        out_v[:, at] = (gated * lax.rsqrt(mean + 1e-6) * gain_ref[0:1, at]).astype(BF16)

    def mix_copy(k, p):
        return remote(
            mix_out.at[k, p], mix_in.at[k, p], mix_sem.at[0, k, p], mix_sem.at[1, k, p], partner
        )

    def last(k, j, _):
        i = 3 - j
        _, _, p = member(i)

        @pl.when(i < 3)
        def _():
            remote(
                down_out.at[k, p], down_in.at[k, p], down_sem.at[0, k, i], down_sem.at[1, k, p],
                partner,
            ).wait_recv()

        rhs = jnp.concatenate([down_in[k, p, 0], down_in[k, p, 1]], axis=1)
        at = pl.ds(pl.multiple_of(p * x_w + k * 128, 128), 128)
        for mine in (False, True):
            start = pl.multiple_of((core if mine else other) * blk, 128)
            rows = pl.ds(start, blk)
            c_at = [pl.ds(pl.multiple_of((2 * p + g) * 128, 128), 128) for g in range(2)]
            v = jnp.dot(cc[rows, c_at[k // 2]], rhs, preferred_element_type=F32)
            if k == 1:
                u = jnp.dot(cc[rows, c_at[1]], rhs, preferred_element_type=F32)
                v = jnp.where(wide_left(256), v, u)
            cols = rolled(cum_ref[rows, :], p)
            y = y_ref[rows, at] + v[:, :128] * two(cols, 2 * k) + v[:, 128:] * two(cols, hh + 2 * k)
            mixed = y.astype(BF16)
            if mine:
                gate(mixed, pl.ds(pl.multiple_of(core * x_half + p * x_w + k * 128, 128), 128))
            else:
                mix_out[k, p] = mixed
                mix_copy(k, p).start()
        return 0

    def out_copy(k, half, p):
        at = pl.ds(pl.multiple_of(half * x_half + p * x_w + k * 128, 128), 128)
        return pltpu.make_async_copy(out_v.at[:, at], out_hbm.at[:, at], out_sem.at[k, half, p])

    def take(k, p, _):
        mix_copy(k, p).wait_recv()
        gate(mix_in[k, p], pl.ds(pl.multiple_of(other * x_half + p * x_w + k * 128, 128), 128))
        return 0

    def finish(k):
        lax.fori_loop(0, hp, functools.partial(take, k), 0)
        for half in range(2):
            for p in range(hp):
                out_copy(k, half, p).start()

    lax.fori_loop(0, 4, functools.partial(first, 0), 0)
    quad_logs()
    lax.fori_loop(0, 4, functools.partial(first, 1), 0)
    z_logs()
    combine(0)
    z_send(0, 0)
    lax.fori_loop(0, 4, functools.partial(first, 2), 0)
    lax.fori_loop(0, 1, inner, 0)
    z_recv(0, 0)
    for r in range(1, rounds):
        z_send(r, 0)
        if r < rounds - 1:
            z_recv(r, 0)
    combine(1)
    z_send(0, 1)
    lax.fori_loop(1, 2, inner, 0)
    z_recv(0, 1)
    for r in range(1, rounds):
        z_send(r, 1)
        if r < rounds - 1:
            z_recv(r, 1)
    combine(2)
    z_send(0, 2)
    if rounds > 1:
        z_recv(rounds - 1, 0)
    down(0)
    lax.fori_loop(2, 3, inner, 0)
    z_recv(0, 2)
    for r in range(1, rounds):
        z_send(r, 2)
        if r < rounds - 1:
            z_recv(r, 2)
    if rounds > 1:
        z_recv(rounds - 1, 1)
    down(1)
    lax.fori_loop(3, hp, inner, 0)
    if rounds > 1:
        z_recv(rounds - 1, 2)
    down(2)
    z_load.wait()
    for k in range(3):
        lax.fori_loop(0, 4, functools.partial(last, k), 0)
        if k > 0:
            finish(k - 1)
    finish(2)

    for x in range(2):

        @pl.when(x * 2 + holder != here)
        def _(x=x):
            for i in range(5):
                param_copy(i, x).wait_send()

    for low, sends in ((True, sends_low), (False, sends_high)):

        @pl.when(sends)
        def _(low=low):
            for i in range(3):
                for k in range(2):
                    edge_copy(i, low, k).wait_send()

    for i in range(3):
        inc_copy(i).wait_send()
        half_copy(i).wait_send()
        qlog_copy(i).wait_send()
    for o in range(1, nz):
        zlog_copy(o).wait_send()
    for k in range(3):
        for i in range(3):
            up_copy(k, i).wait_send()
            down_copy(k, i).wait_send()
        for p in range(hp):
            mix_copy(k, p).wait_send()
        for r in range(rounds):
            h, _, senders = z_parts(r)
            for d, sender in senders:

                @pl.when(sender)
                def _(k=k, r=r, d=d, h=h):
                    for o in range(1, h + 1):
                        z_copy(r, k, o, d).wait_send()

    for k in range(3):
        for half in range(2):
            for p in range(hp):
                out_copy(k, half, p).wait()


def fits_quad(sp, dp, blk, heads, groups):
    nz = dp // 2
    power = dp % 2 == 0 and nz > 1 and nz & (nz - 1) == 0
    shares = sp == 4 and groups % 4 == 0 and groups // 4 == sp
    return power and shares and blk == 128 and 2 * heads * HEAD_DIM == 3 * groups * 128


def quad_local(sp, dp, x, b, c, z, ahead, back, spike, wx, wb, wc, offset, fading, gain):
    x, b, c, z = x[0], b[0], c[0], z[0]
    blk, x_total = x.shape
    b_total = b.shape[1]
    groups = b_total // STATE
    heads = ahead.shape[2]
    pairs = groups // 2
    nz = dp // 2
    rounds = nz.bit_length() - 1
    tiles = heads // pairs * HEAD_DIM // 128
    hp, hh = pairs // 2, heads // 2
    x_half, b_half = x_total // 2, b_total // 2
    width = x_half + 2 * b_half
    params = (wx, wb, wc, offset, fading)
    vm = pltpu.VMEM
    gains = gain.reshape(x_total // 128, 128)
    scratch = [vm(one.shape, BF16) for one in (x, b, c, z)]
    scratch += [vm((2, 3, hh, blk), F32), vm((3, hh, blk), F32), vm(gains.shape, BF16)]
    scratch += [vm((blk, x_half), BF16), vm((blk, b_half), BF16), vm((blk, b_half), BF16)]
    scratch += [vm(one.shape, one.dtype) for one in params]
    scratch += [vm((2,) + one.shape, one.dtype) for one in params]
    scratch += [vm((EDGE, n), BF16) for n in (x_half, b_half, b_half)] * 2
    scratch += [vm((2, 2 * blk + 16, 128), F32), vm((8, width), F32), vm((8, 128), F32)]
    scratch += [vm((8, x_total), F32)] + [vm((2 * blk, 128), F32)] * 3
    scratch += [vm((128, 2 * blk), F32)] * 3
    scratch += [vm((2 * blk, x_half), BF16), vm((2 * hp, STATE, 2 * blk), BF16)]
    scratch += [vm((2 * blk, b_half), BF16), vm((2 * blk, x_half), F32)]
    scratch += [vm((tiles, 4, 2, STATE, 128), BF16)] * 4
    scratch += [vm((8, 128), F32), vm((4, 8, 128), F32), vm((8, 128), F32), vm((nz, 8, 128), F32)]
    scratch += [vm((4, 2, tiles, 8, 128), F32)] * 2 + [vm((2, tiles, 8, 128), F32)]
    scratch += [vm((rounds, 2, tiles, 8, 128), F32)]
    scratch += [vm((tiles, 2, STATE, 128), F32)] * 2 + [vm((rounds, tiles, STATE, 128), BF16)] * 2
    scratch += [vm((tiles, hp, blk, 128), BF16)] * 2 + [vm((blk, x_total), BF16)]
    dma = pltpu.SemaphoreType.DMA
    scratch += [dma((16,)), dma((2, 5, 2)), dma((2, 3, 2)), dma((2, 3)), dma((2, 3))]
    scratch += [dma((2, 4)), dma((2, nz)), dma((2, tiles, 4)), dma((rounds, tiles, nz))]
    scratch += [dma((rounds, tiles)), dma((2, tiles, 4)), dma((2, tiles, hp)), dma((tiles, 2, hp))]
    out = pl.pallas_call(
        functools.partial(quad_kernel, (heads, pairs, sp, dp)),
        out_shape=jax.ShapeDtypeStruct((blk, x_total), BF16),
        in_specs=[pl.BlockSpec(memory_space=pl.ANY)] * 13,
        out_specs=pl.BlockSpec(memory_space=pl.ANY),
        scratch_shapes=scratch,
        compiler_params=pltpu.CompilerParams(
            collective_id=0, has_side_effects=True, vmem_limit_bytes=40 * 2**20
        ),
        name="mixer",
    )(x, b, c, z, ahead[0].T, back[0].T, spike[0].T, *params, gains)
    return out[None]


def pick(sp, dp, x, b, *rest):
    blk, heads = x.shape[1], rest[2].shape[2]
    if fits_quad(sp, dp, blk, heads, b.shape[2] // STATE):
        return quad_local(sp, dp, x, b, *rest)
    return local(sp, dp, x, b, *rest)


def solution(mesh):
    tokens = P("dp", "sp", None)
    placed = (tokens,) * 7 + (P(None, "sp"),) * 5 + (P(),)
    return jax.shard_map(
        functools.partial(pick, mesh.shape["sp"], mesh.shape["dp"]),
        mesh=mesh,
        in_specs=placed,
        out_specs=tokens,
        check_vma=False,
    )
```

```python
import functools

import jax
import jax.numpy as jnp
from jax import lax
from jax.experimental import pallas as pl
from jax.experimental.pallas import tpu as pltpu
from jax.sharding import PartitionSpec as P

F32 = jnp.float32
BF16 = jnp.bfloat16
HEAD_DIM = 64
STATE = 128
EDGE = 8
HIGHEST = lax.Precision.HIGHEST


def levels_of(sp, dp, groups):
    found = []
    split = 1
    core = 2 if sp % 2 == 0 else 1
    inner = 2 if dp % 2 == 0 and groups % (2 * sp) == 0 else 1
    for axis, count, stride in (("sp", core, 1), ("sp", sp // core, core), ("dp", inner, 1)):
        if count > 1:
            found.append((axis, count, stride))
            split *= count
    return tuple(found), ("dp", dp // inner, inner)


def digit_of(level):
    axis, count, stride = level
    return lax.rem(lax.axis_index(axis) // stride, count)


def member_id(level, member):
    axis, count, stride = level
    return {axis: lax.axis_index(axis) + (member - digit_of(level)) * stride}


def kernel(levels, top, sizes, *refs):
    heads, pairs, chunks, sp, dp = sizes
    (x_ref, b_ref, c_ref, z_ref, ahead_ref, back_ref, spike_ref) = refs[:7]
    params = refs[7:12]
    gain_ref, out_ref = refs[12:14]
    (xc, bc, cc, y_ref, cum_ref, rate_ref, cum_t, rate_t, fac_ref) = refs[14:23]
    refs = refs[:14] + refs[23:]
    got, w_ref, prm_ref, halo_ref, edges, early_sem, edge_sem = (
        refs[14:19], refs[19], refs[20], refs[21], refs[22:28], refs[28], refs[29]
    )
    rest = list(refs[30:])
    depth = len(levels)
    logs = [rest.pop(0) for _ in range(depth + 1)]
    up_log = [rest.pop(0) for _ in range(depth + 1)]
    decay = [rest.pop(0) for _ in range(depth + 1)]
    log_sem = [rest.pop(0) for _ in range(depth + 1)]
    totals, up, down, stage, sems, incoming = ([] for _ in range(6))
    for _ in range(chunks):
        totals.append([rest.pop(0) for _ in range(depth + 1)])
        up.append([rest.pop(0) for _ in range(depth + 1)])
        down.append([rest.pop(0) for _ in range(depth)])
        stage.append([rest.pop(0) for _ in range(depth)])
        sems.append([rest.pop(0) for _ in range(depth + 1)])
        incoming.append(rest.pop(0))
    blk = x_ref.shape[0]
    per_pair = heads // pairs
    x_w = per_pair * HEAD_DIM
    b_w = 2 * STATE
    tiles = x_w // 128
    lane = lax.broadcasted_iota(jnp.int32, (blk, 128), 1)
    left = lane < HEAD_DIM
    row = lax.broadcasted_iota(jnp.int32, (blk, 128), 0)

    segment = ("sp", sp, 1)
    here, there = lax.axis_index("sp"), lax.axis_index("dp")
    rank = there * sp + here
    has_next, has_prev = rank < sp * dp - 1, rank > 0
    after = {"sp": lax.rem(here + 1, sp), "dp": lax.rem(there + (here + 1) // sp, dp)}
    before = {
        "sp": lax.rem(here + sp - 1, sp),
        "dp": lax.rem(there + dp - (sp - here) // sp, dp),
    }
    mesh_id = pl.DeviceIdType.MESH
    barrier = pltpu.get_barrier_semaphore()
    greeted = 0
    for level in levels + (top, segment):
        me = digit_of(level)
        for o in range(1, level[1]):
            target = member_id(level, lax.rem(me + o, level[1]))
            pl.semaphore_signal(barrier, inc=1, device_id=target, device_id_type=mesh_id)
            greeted += 1
    for present, target in ((has_next, after), (has_prev, before)):

        @pl.when(present)
        def _(target=target):
            pl.semaphore_signal(barrier, inc=1, device_id=target, device_id_type=mesh_id)

    filler = jnp.zeros((128 - 2 * heads, blk), F32)
    inc = jnp.concatenate([ahead_ref[...], back_ref[...], filler], axis=0).T
    spikes = jnp.concatenate([spike_ref[...], spike_ref[...], filler], axis=0).T
    count = sp * dp
    neighbours = (rank + count - 1) // count + (2 * count - 2 - rank) // count
    pl.semaphore_wait(barrier, greeted + neighbours)

    def edge_copy(i, direction):
        src = (x_ref, b_ref, c_ref)[i]
        start = blk - EDGE if direction == 0 else 0
        return pltpu.make_async_remote_copy(
            src_ref=src.at[pl.ds(start, EDGE), :],
            dst_ref=edges[3 * direction + i],
            send_sem=edge_sem.at[0, direction, i],
            recv_sem=edge_sem.at[1, direction, i],
            device_id=(after, before)[direction],
            device_id_type=mesh_id,
        )

    def param_copy(i, member, slot):
        return pltpu.make_async_remote_copy(
            src_ref=params[i],
            dst_ref=got[i].at[slot],
            send_sem=early_sem.at[0, i, member],
            recv_sem=early_sem.at[1, i, slot],
            device_id=member_id(segment, member),
            device_id_type=mesh_id,
        )

    for o in range(1, sp):
        for i in range(5):
            param_copy(i, lax.rem(here + o, sp), here).start()
    for direction, present in ((0, has_next), (1, has_prev)):

        @pl.when(present)
        def _(direction=direction):
            for i in range(3):
                edge_copy(i, direction).start()

    for i in range(5):
        got[i][here] = params[i][...]
    for o in range(1, sp):
        for i in range(5):
            s = lax.rem(here + o, sp)
            param_copy(i, s, s).wait_recv()
    prm_ref[...] = jnp.zeros_like(prm_ref)
    wide = got[3].shape[2]
    for q in range(sp):
        for kind in range(2):
            for d in range(2):
                at = slice(d * heads + q * wide, d * heads + (q + 1) * wide)
                prm_ref[kind : kind + 1, at] = got[3 + kind][q, d : d + 1, :]
        off = 0
        for i in range(3):
            n = got[i].shape[2]
            w_ref[0:4, off + q * n : off + (q + 1) * n] = got[i][q].astype(F32)
            off += n * sp
    rate = jax.nn.softplus(inc + prm_ref[0:1, :])
    log_decay = -jnp.exp(prm_ref[1:2, :]) * rate + spikes
    lower = (lane <= row).astype(F32)
    upper = (lane >= row).astype(F32)
    cum_f = jnp.dot(lower, log_decay, precision=HIGHEST, preferred_element_type=F32)
    cum_b = jnp.dot(upper, log_decay, precision=HIGHEST, preferred_element_type=F32)
    cum = jnp.where(lane < heads, cum_f, cum_b)
    lane1 = lane[0:1]
    last = jnp.where(lane1 < heads, cum_f[blk - 1 : blk], cum_b[0:1])
    cum_ref[...] = cum
    rate_ref[...] = rate
    cum_t[...] = cum.T
    rate_t[...] = rate.T
    fac_ref[...] = rate * jnp.exp(last - cum)
    logs[0][...] = jnp.broadcast_to(last, (8, 128))

    def rolled(ref, p):
        return pltpu.roll(ref[...], lax.rem(128 - p * per_pair, 128), 1)

    def two(cols, i):
        return jnp.where(left, cols[:, i : i + 1], cols[:, i + 1 : i + 2])

    def conv(src, col, width, off):
        at = pl.ds(pl.multiple_of(off + col, 128), width)
        v = src[:, pl.ds(pl.multiple_of(col, 128), width)].astype(F32)
        r = lax.broadcasted_iota(jnp.int32, (blk, width), 0)
        h0, h1, h2 = halo_ref[0:1, at], halo_ref[1:2, at], halo_ref[2:3, at]
        m1 = jnp.where(r == 0, h1, pltpu.roll(v, 1, 0))
        m2 = jnp.where(r == 0, h0, jnp.where(r == 1, h1, pltpu.roll(v, 2, 0)))
        p1 = jnp.where(r == blk - 1, h2, pltpu.roll(v, blk - 1, 0))
        s = m2 * w_ref[0:1, at] + m1 * w_ref[1:2, at] + v * w_ref[2:3, at] + p1 * w_ref[3:4, at]
        return (s / (1.0 + jnp.exp(-s))).astype(BF16)

    share = pairs // chunks
    x_total = x_ref.shape[1]
    b_total = b_ref.shape[1]

    def first(c, p, _):
        x_at = pl.ds(pl.multiple_of(p * x_w, 128), x_w)
        b_at = pl.ds(pl.multiple_of(p * b_w, 128), b_w)
        xv = conv(x_ref, p * x_w, x_w, 0)
        bv = conv(b_ref, p * b_w, b_w, x_total)
        xc[:, x_at] = xv
        bc[:, b_at] = bv
        cc[:, b_at] = conv(c_ref, p * b_w, b_w, x_total + b_total)
        cols = rolled(fac_ref, p)
        xf = xv.astype(F32)
        for d in range(2):
            scaled = jnp.concatenate(
                [
                    (xf[:, k * 128 : (k + 1) * 128] * two(cols, d * heads + 2 * k)).astype(BF16)
                    for k in range(tiles)
                ],
                axis=1,
            )
            u = lax.dot_general(scaled, bv, (((0,), (0,)), ((), ())), preferred_element_type=F32)
            half = x_w // 2
            rows = pl.ds(pl.multiple_of((p - c * share) * x_w, 128), x_w)
            totals[c][0][d, rows, :] = jnp.concatenate(
                [u[:half, :STATE], u[half:, STATE:]], axis=0
            ).astype(BF16)
        return 0

    for direction, present in ((0, has_prev), (1, has_next)):

        @pl.when(present)
        def _(direction=direction):
            for i in range(3):
                edge_copy(i, direction).wait_recv()

    off = 0
    for i in range(3):
        n = edges[i].shape[1]
        low = edges[i][...].astype(F32)
        high = edges[3 + i][...].astype(F32)
        halo_ref[0:2, off : off + n] = jnp.where(has_prev, low[EDGE - 2 :], 0.0)
        halo_ref[2:3, off : off + n] = jnp.where(has_next, high[0:1], 0.0)
        off += n
    def inner(p, _):
        x_at = pl.ds(pl.multiple_of(p * x_w, 128), x_w)
        b_at = pl.ds(pl.multiple_of(p * b_w, 128), b_w)
        bv, cv, xv = bc[:, b_at], cc[:, b_at], xc[:, x_at]
        cols = rolled(cum_ref, p)
        parts = []
        for g in range(2):
            scores = lax.dot_general(
                cv[:, g * STATE : (g + 1) * STATE],
                bv[:, g * STATE : (g + 1) * STATE],
                (((1,), (1,)), ((), ())),
                preferred_element_type=F32,
            )
            for i in range(per_pair // 2):
                h = g * (per_pair // 2) + i
                hf = p * per_pair + h
                gap_f = cols[:, h : h + 1] - cum_t[pl.ds(hf, 1), :]
                gap_b = cols[:, heads + h : heads + h + 1] - cum_t[pl.ds(heads + hf, 1), :]
                gap = jnp.where(lane < row, gap_f, jnp.where(lane > row, gap_b, 0.0))
                rf, rb = rate_t[pl.ds(hf, 1), :], rate_t[pl.ds(heads + hf, 1), :]
                scale = jnp.where(lane < row, rf, jnp.where(lane > row, rb, rf + rb))
                parts.append((scores * jnp.exp(gap) * scale).astype(BF16))
        for k in range(tiles):
            xt = xv[:, k * 128 : (k + 1) * 128]
            zero = jnp.zeros_like(xt)
            both = jnp.concatenate([jnp.where(left, xt, zero), jnp.where(left, zero, xt)], axis=0)
            w = jnp.concatenate([parts[2 * k], parts[2 * k + 1]], axis=1)
            y_ref[:, pl.ds(pl.multiple_of(p * x_w + k * 128, 128), 128)] = jnp.dot(
                w, both, preferred_element_type=F32
            )
        return 0

    def copy(src, dst, send, recv, level, member):
        return pltpu.make_async_remote_copy(
            src_ref=src,
            dst_ref=dst,
            send_sem=send,
            recv_sem=recv,
            device_id=member_id(level, member),
            device_id_type=pl.DeviceIdType.MESH,
        )

    every_level = levels + (top,)
    head_share = heads // chunks
    bases = [jnp.int32(0)]
    size = head_share
    for level in levels:
        size = size // level[1]
        bases.append(bases[-1] + digit_of(level) * size)
    pending = [[] for _ in range(chunks)]

    def head_rows(h):
        return pl.ds(pl.multiple_of(h * HEAD_DIM, HEAD_DIM), HEAD_DIM)

    def log_copy(k, member, slot):
        sem = log_sem[k]
        return copy(
            logs[k], up_log[k].at[slot], sem.at[0, member], sem.at[1, slot], every_level[k], member
        )

    def start_up(c, k):
        level = every_level[k]
        n, me = level[1], digit_of(level)
        total, sem = totals[c][k], sems[c][k]
        rows = total.shape[1] // n
        for o in range(1, n):
            m = lax.rem(me + o, n)
            if c == 0:
                pending[c].append(log_copy(k, m, me))
            if k < depth:
                part = total.at[:, pl.ds(pl.multiple_of(m * rows, 64), rows), :]
            else:
                part = total.at[jnp.where(m < me, 1, 0)]
            pending[c].append(
                copy(part, up[c][k].at[me], sem.at[0, m], sem.at[1, me], level, m)
            )
        for one in pending[c]:
            one.start()
        if k < depth:
            up[c][k][me] = total[:, pl.ds(pl.multiple_of(me * rows, 64), rows), :]
        if c == 0:
            up_log[k][me] = logs[k][...]

    def flush(c):
        for one in pending[c]:
            one.wait_send()
        pending[c].clear()

    def finish_up(c, k):
        level = every_level[k]
        n, me = level[1], digit_of(level)
        total, sem = totals[c][k], sems[c][k]
        flush(c)
        for o in range(1, n):
            s = lax.rem(me + o, n)
            if c == 0:
                log_copy(k, s, s).wait_recv()
            part = total.at[:, pl.ds(0, total.shape[1] // n), :] if k < depth else total.at[0]
            copy(part, up[c][k].at[s], sem.at[0, s], sem.at[1, s], level, s).wait_recv()
        if c == 0:

            def expand(m, _):
                decay[k][m] = jnp.exp(jnp.broadcast_to(up_log[k][m][0:1, :], (128, 128)).T)
                return 0

            lax.fori_loop(0, n, expand, 0)
            if k < depth:
                log_sum = up_log[k][0]
                for m in range(1, n):
                    log_sum = log_sum + up_log[k][m]
                logs[k + 1][...] = log_sum

    def gather(c, k):
        n = levels[k][1]
        base = c * head_share + bases[k + 1]
        part, new = up[c][k], totals[c][k + 1]

        def one_head(h, _):
            at = head_rows(h)
            f = part[0, 0, at, :].astype(F32)
            b = part[n - 1, 1, at, :].astype(F32)
            for m in range(1, n):
                r = n - 1 - m
                f = f * decay[k][m, pl.ds(base + h, 1), :] + part[m, 0, at, :].astype(F32)
                b = b * decay[k][r, pl.ds(heads + base + h, 1), :] + part[r, 1, at, :].astype(F32)
            new[0, at, :] = f.astype(BF16)
            new[1, at, :] = b.astype(BF16)
            return 0

        lax.fori_loop(0, new.shape[1] // HEAD_DIM, one_head, 0)

    def enter(c):
        n, me = top[1], digit_of(top)
        base = c * head_share + bases[-1]
        into = incoming[c]
        into[...] = jnp.zeros_like(into)

        def carry(s, d):
            def one_head(h, _):
                at = head_rows(h)
                factor = decay[depth][s, pl.ds(d * heads + base + h, 1), :]
                into[d, at, :] = into[d, at, :] * factor + up[c][depth][s, at, :].astype(F32)
                return 0

            lax.fori_loop(0, into.shape[1] // HEAD_DIM, one_head, 0)
            return 0

        lax.fori_loop(0, me, lambda s, _: carry(s, 0), 0)
        lax.fori_loop(0, n - 1 - me, lambda i, _: carry(n - 1 - i, 1), 0)

    def start_down(c, k):
        level = levels[k]
        n, me = level[1], digit_of(level)
        sem = sems[c][k]
        rows = totals[c][k].shape[1] // n
        base = c * head_share + bases[k + 1]
        source = incoming[c] if k == depth - 1 else down[c][k + 1]
        part, out = up[c][k], stage[c][k]

        def spread(h, _):
            at = head_rows(h)
            f = source[0, at, :].astype(F32)
            b = source[1, at, :].astype(F32)
            for m in range(n):
                r = n - 1 - m
                out[m, 0, at, :] = f.astype(BF16)
                out[r, 1, at, :] = b.astype(BF16)
                if m < n - 1:
                    f = f * decay[k][m, pl.ds(base + h, 1), :] + part[m, 0, at, :].astype(F32)
                    down_factor = decay[k][r, pl.ds(heads + base + h, 1), :]
                    b = b * down_factor + part[r, 1, at, :].astype(F32)
            return 0

        lax.fori_loop(0, rows // HEAD_DIM, spread, 0)
        mine = pl.ds(pl.multiple_of(me * rows, 64), rows)
        for o in range(1, n):
            m = lax.rem(me + o, n)
            pending[c].append(
                copy(out.at[m], down[c][k].at[:, mine, :], sem.at[2, m], sem.at[3, me], level, m)
            )
        for one in pending[c]:
            one.start()
        down[c][k][:, mine, :] = out[me]

    def finish_down(c, k):
        level = levels[k]
        n, me = level[1], digit_of(level)
        sem = sems[c][k]
        rows = totals[c][k].shape[1] // n
        flush(c)
        for o in range(1, n):
            s = lax.rem(me + o, n)
            theirs = pl.ds(pl.multiple_of(s * rows, 64), rows)
            copy(
                stage[c][k].at[s], down[c][k].at[:, theirs, :], sem.at[2, s], sem.at[3, s], level, s
            ).wait_recv()

    for c in range(chunks):
        lax.fori_loop(c * share, (c + 1) * share, functools.partial(first, c), 0)
        start_up(c, 0)
    for o in range(1, sp):
        for i in range(5):
            param_copy(i, lax.rem(here + o, sp), here).wait_send()
    for direction, present in ((0, has_next), (1, has_prev)):

        @pl.when(present)
        def _(direction=direction):
            for i in range(3):
                edge_copy(i, direction).wait_send()


    gaps = chunks * depth
    cuts = [(i * pairs) // gaps for i in range(gaps + 1)]
    for k in range(depth):
        for c in range(chunks):
            finish_up(c, k)
            gather(c, k)
            start_up(c, k + 1)
            at = k * chunks + c
            lax.fori_loop(cuts[at], cuts[at + 1], inner, 0)
    for c in range(chunks):
        finish_up(c, depth)
        enter(c)
        start_down(c, depth - 1)
    for k in reversed(range(1, depth)):
        for c in range(chunks):
            finish_down(c, k)
            start_down(c, k - 1)

    cum_ref[...] = jnp.exp(cum_ref[...])

    def last_part(c, p, _):
        cv = cc[:, pl.ds(pl.multiple_of(p * b_w, 128), b_w)]
        cols = rolled(cum_ref, p)
        carried = []
        for d in range(2):
            st = down[c][0][d, pl.ds(pl.multiple_of((p - c * share) * x_w, 128), x_w), :]
            got = [
                lax.dot_general(
                    cv[:, g * STATE : (g + 1) * STATE],
                    st,
                    (((1,), (1,)), ((), ())),
                    preferred_element_type=F32,
                )
                for g in range(2)
            ]
            carried.append(got)
        for k in range(tiles):
            cut = slice(k * 128, (k + 1) * 128)
            at = pl.ds(pl.multiple_of(p * x_w + k * 128, 128), 128)
            y = y_ref[:, at]
            for d in range(2):
                a, b = carried[d][0][:, cut], carried[d][1][:, cut]
                if 2 * k + 1 < per_pair // 2:
                    v = a
                elif 2 * k >= per_pair // 2:
                    v = b
                else:
                    v = jnp.where(left, a, b)
                y = y + v * two(cols, d * heads + 2 * k)
            z = z_ref[:, at].astype(F32)
            gated = y.astype(BF16).astype(F32) * (z / (1.0 + jnp.exp(-z)))
            square = gated * gated
            low = jnp.sum(jnp.where(left, square, 0.0), axis=1, keepdims=True)
            high = jnp.sum(jnp.where(left, 0.0, square), axis=1, keepdims=True)
            mean = jnp.where(left, low, high) * (1.0 / HEAD_DIM)
            out_ref[:, at] = (gated * lax.rsqrt(mean + 1e-6) * gain_ref[0:1, at]).astype(BF16)
        return 0

    for c in range(chunks):
        finish_down(c, 0)
        lax.fori_loop(c * share, (c + 1) * share, functools.partial(last_part, c), 0)


def local(sp, dp, x, b, c, z, ahead, back, spike, wx, wb, wc, offset, fading, gain):
    x, b, c, z = x[0], b[0], c[0], z[0]
    blk, x_total = x.shape
    groups = b.shape[1] // STATE
    heads = ahead.shape[2]
    pairs = groups // 2
    levels, top = levels_of(sp, dp, groups)
    scratch = [
        pltpu.VMEM((blk, x_total), BF16),
        pltpu.VMEM((blk, groups * STATE), BF16),
        pltpu.VMEM((blk, groups * STATE), BF16),
        pltpu.VMEM((blk, x_total), F32),
    ]
    scratch += [pltpu.VMEM((128, 128), F32)] * 5
    params = (wx, wb, wc, offset, fading)
    width = x_total + 2 * b.shape[1]
    early = [pltpu.VMEM((sp,) + one.shape, one.dtype) for one in params]
    early += [pltpu.VMEM((8, width), F32), pltpu.VMEM((8, 128), F32), pltpu.VMEM((8, width), F32)]
    early += [pltpu.VMEM((EDGE, one.shape[1]), BF16) for one in (x, b, c)] * 2
    early += [pltpu.SemaphoreType.DMA((2, 5, sp)), pltpu.SemaphoreType.DMA((2, 2, 3))]
    scratch += early
    split = 1
    for level in levels:
        split *= level[1]
    chunks = 2 if groups % (2 * split) == 0 else 1
    counts = [level[1] for level in levels] + [top[1]]
    scratch += [pltpu.VMEM((8, 128), F32)] * len(counts)
    scratch += [pltpu.VMEM((n, 8, 128), F32) for n in counts]
    scratch += [pltpu.VMEM((n, 128, 128), F32) for n in counts]
    scratch += [pltpu.SemaphoreType.DMA((2, n)) for n in counts]
    for _ in range(chunks):
        held = [x_total // chunks]
        for n in counts[:-1]:
            held.append(held[-1] // n)
        slabs = list(zip(counts[:-1], held[1:]))
        scratch += [pltpu.VMEM((2, rows, STATE), BF16) for rows in held]
        scratch += [pltpu.VMEM((n, 2, rows, STATE), BF16) for n, rows in slabs]
        scratch += [pltpu.VMEM((counts[-1], held[-1], STATE), BF16)]
        scratch += [pltpu.VMEM((2, rows, STATE), BF16) for rows in held[:-1]]
        scratch += [pltpu.VMEM((n, 2, rows, STATE), BF16) for n, rows in slabs]
        scratch += [pltpu.SemaphoreType.DMA((4, n)) for n in counts]
        scratch += [pltpu.VMEM((2, held[-1], STATE), F32)]
    out = pl.pallas_call(
        functools.partial(kernel, levels, top, (heads, pairs, chunks, sp, dp)),
        out_shape=jax.ShapeDtypeStruct((blk, x_total), BF16),
        in_specs=[pl.BlockSpec(memory_space=pltpu.VMEM)] * 13,
        out_specs=pl.BlockSpec(memory_space=pltpu.VMEM),
        scratch_shapes=scratch,
        compiler_params=pltpu.CompilerParams(
            collective_id=0, has_side_effects=True, vmem_limit_bytes=60 * 2**20
        ),
        name="mixer",
    )(x, b, c, z, ahead[0].T, back[0].T, spike[0].T, *params, gain.astype(F32)[None])
    return out[None]


def quad_kernel(sizes, *refs):
    heads, pairs, sp, dp = sizes
    nz = dp // 2
    rounds = nz.bit_length() - 1
    (x_hbm, b_hbm, c_hbm, z_hbm, ahead_hbm, back_hbm, spike_hbm) = refs[:7]
    params = refs[7:12]
    gain_hbm, out_ref = refs[12:14]
    (in_x, in_b, in_c, in_z, inc, inc_out, gain_in, px, pb, pc) = refs[14:24]
    own, got = refs[24:29], refs[29:34]
    edges = refs[34:40]
    (work, w_ref, prm_ref, gain_ref, cum_ref, fac_ref, col_ref, cum_t, rate_t, mid_t) = refs[40:50]
    (xc, bt, cc, y_ref, sup, up_in, down_out, down_in) = refs[50:58]
    (logs, qlog, zsum, zlog, dec, wup, zdec, zwt) = refs[58:66]
    (tz, zin, zs, zr, mix_out, mix_in) = refs[66:72]
    (load_sem, prm_sem, edge_sem, half_sem, inc_sem, qlog_sem, zlog_sem) = refs[72:79]
    (up_sem, zsend_sem, zrecv_sem, down_sem, mix_sem) = refs[79:84]

    hh = heads // 2
    hp = pairs // 2
    per_pair = heads // pairs
    tiles = per_pair * HEAD_DIM // 128
    blk = in_x.shape[0]
    tokens = 2 * blk
    x_half = in_x.shape[1] // 2
    b_half = in_b.shape[1] // 2
    x_w = per_pair * HEAD_DIM
    mesh_id = pl.DeviceIdType.MESH

    here, there = lax.axis_index("sp"), lax.axis_index("dp")
    core, cx = lax.rem(here, 2), here // 2
    cy, cz = lax.rem(there, 2), there // 2
    other = 1 - core
    me = cy * 2 + cx
    chip = there * 2 + cx
    chips = dp * 2
    has_next, has_prev = chip < chips - 1, chip > 0
    after, before = lax.rem(chip + 1, chips), lax.rem(chip + chips - 1, chips)
    partner = {"sp": cx * 2 + other}

    def chip_id(c, k):
        return {"sp": lax.rem(c, 2) * 2 + k, "dp": c // 2}

    def quad_id(qy, qx):
        return {"sp": qx * 2 + core, "dp": cz * 2 + qy}

    def z_id(z):
        return {"dp": z * 2 + cy}

    def member(i):
        qy = lax.rem(cy + lax.rem(i + 1, 2), 2)
        qx = lax.rem(cx + (3 - i) // 2, 2)
        return qy, qx, qy * 2 + qx

    def remote(src, dst, send, recv, target):
        return pltpu.make_async_remote_copy(
            src_ref=src, dst_ref=dst, send_sem=send, recv_sem=recv,
            device_id=target, device_id_type=mesh_id,
        )

    barrier = pltpu.get_barrier_semaphore()

    def greet(target):
        pl.semaphore_signal(barrier, inc=1, device_id=target, device_id_type=mesh_id)

    for o in range(1, sp):
        greet({"sp": lax.rem(here + o, sp)})
    for i in range(3):
        qy, qx, _ = member(i)
        greet(quad_id(qy, qx))
    for o in range(1, nz):
        greet(z_id(lax.rem(cz + o, nz)))
    for present, neighbour in ((has_next, after), (has_prev, before)):

        @pl.when(present)
        def _(neighbour=neighbour):
            for k in range(2):
                greet(chip_id(neighbour, k))

    loads = []

    def load(src, dst):
        one = pltpu.make_async_copy(src, dst, load_sem.at[len(loads)])
        one.start()
        loads.append(one)
        return one

    param_loads = [load(params[i], own[i]) for i in range(5)]
    mine = pl.ds(pl.multiple_of(core * hh, 8), hh)
    theirs = pl.ds(pl.multiple_of(other * hh, 8), hh)
    raw = (ahead_hbm, back_hbm, spike_hbm)
    inc_stage = [load(raw[i].at[theirs, :], inc_out.at[i]) for i in range(3)]
    inc_loads = [load(raw[i].at[mine, :], inc.at[core, i]) for i in range(3)]
    b_load = load(b_hbm, in_b)
    x_load = load(x_hbm, in_x)
    c_load = load(c_hbm, in_c)
    gain_load = load(gain_hbm, gain_in)
    z_load = load(z_hbm, in_z)

    for one in param_loads + inc_stage:
        one.wait()
    chip_greets = 2 * ((chip + chips - 1) // chips + (2 * chips - 2 - chip) // chips)
    pl.semaphore_wait(barrier, (sp - 1) + 3 + (nz - 1) + chip_greets)

    holder = here // 2
    slot = lax.rem(here, 2)

    def param_copy(i, x):
        return remote(
            own[i], got[i].at[slot], prm_sem.at[0, i, x], prm_sem.at[1, i, slot],
            {"sp": x * 2 + holder},
        )

    for x in range(2):
        elsewhere = x * 2 + holder != here

        @pl.when(elsewhere)
        def _(x=x):
            for i in range(5):
                param_copy(i, x).start()

        @pl.when(jnp.logical_not(elsewhere))
        def _():
            for i in range(5):
                got[i][slot] = own[i][...]

    def inc_copy(i):
        return remote(
            inc_out.at[i], inc.at[core, i], inc_sem.at[0, i], inc_sem.at[1, i], partner
        )

    for i in range(3):
        inc_copy(i).start()

    sources = (in_x, in_b, in_c)
    halves = (x_half, b_half, b_half)

    def edge_copy(i, low, k):
        half = halves[i]
        start = blk - EDGE if low else 0
        return remote(
            sources[i].at[pl.ds(start, EDGE), pl.ds(k * half, half)],
            edges[i if low else 3 + i],
            edge_sem.at[0, i, k],
            edge_sem.at[1, i, 0 if low else 1],
            chip_id(after if low else before, k),
        )

    sends_low = jnp.logical_and(core == 1, has_next)
    sends_high = jnp.logical_and(core == 0, has_prev)

    def half_copy(i):
        cut = pl.ds(pl.multiple_of(other * halves[i], 128), halves[i])
        return remote(
            sources[i].at[:, cut], (px, pb, pc)[i], half_sem.at[0, i], half_sem.at[1, i], partner
        )

    for i, one in ((1, b_load), (0, x_load), (2, c_load)):
        one.wait()

        @pl.when(sends_low)
        def _(i=i):
            for k in range(2):
                edge_copy(i, True, k).start()

        @pl.when(sends_high)
        def _(i=i):
            for k in range(2):
                edge_copy(i, False, k).start()

        half_copy(i).start()

    lane = lax.broadcasted_iota(jnp.int32, (blk, 128), 1)
    row = lax.broadcasted_iota(jnp.int32, (blk, 128), 0)
    left = lane < HEAD_DIM
    left1 = left[0:1]
    lower = (lane <= row).astype(F32)
    upper = (lane >= row).astype(F32)
    filler = jnp.zeros((128 - 2 * hh, blk), F32)

    for q in range(2):
        from_q = 2 * core + q != here

        @pl.when(from_q)
        def _(q=q):
            for i in range(5):
                remote(
                    own[i], got[i].at[q], prm_sem.at[0, i, 0], prm_sem.at[1, i, q], partner
                ).wait_recv()

    for one in inc_loads:
        one.wait()
    for i in range(3):
        remote(
            inc_out.at[i], inc.at[other, i], inc_sem.at[0, i], inc_sem.at[1, i], partner
        ).wait_recv()
    prm_ref[...] = jnp.zeros_like(prm_ref)
    wide = own[3].shape[1]
    for q in range(2):
        for kind in range(2):
            for d in range(2):
                at = slice(d * hh + q * wide, d * hh + (q + 1) * wide)
                prm_ref[kind : kind + 1, at] = got[3 + kind][q, d : d + 1, :]
        off = 0
        for i in range(3):
            n = own[i].shape[1]
            w_ref[0:4, off + q * n : off + (q + 1) * n] = got[i][q].astype(F32)
            off += 2 * n

    cums, rates = [], []
    for j in range(2):
        pre = jnp.concatenate([inc[j, 0], inc[j, 1], filler], axis=0).T
        spikes = jnp.concatenate([inc[j, 2], inc[j, 2], filler], axis=0).T
        rate = jax.nn.softplus(pre + prm_ref[0:1, :])
        log_decay = -jnp.exp(prm_ref[1:2, :]) * rate + spikes
        cum_f = jnp.dot(lower, log_decay, precision=HIGHEST, preferred_element_type=F32)
        cum_b = jnp.dot(upper, log_decay, precision=HIGHEST, preferred_element_type=F32)
        cums.append((cum_f, cum_b))
        rates.append(rate)
    ahead_lane = lane < hh
    ahead1 = ahead_lane[0:1]
    mid_f, mid_b = cums[0][0][blk - 1 : blk], cums[1][1][0:1]
    total = jnp.where(ahead1, mid_f + cums[1][0][blk - 1 : blk], cums[0][1][0:1] + mid_b)
    logs[...] = jnp.broadcast_to(total, (8, 128))

    def qlog_copy(i):
        qy, qx, q = member(i)
        return remote(
            logs, qlog.at[me], qlog_sem.at[0, i], qlog_sem.at[1, me], quad_id(qy, qx)
        )

    for i in range(3):
        qlog_copy(i).start()
    qlog[me] = logs[...]
    for j in range(2):
        cum_f, cum_b = cums[j]
        far = jnp.where(ahead_lane, mid_f if j == 1 else 0.0, mid_b if j == 0 else 0.0)
        near = jnp.where(ahead_lane, cum_f, cum_b)
        at = slice(j * blk, (j + 1) * blk)
        cum = near + far
        cum_ref[at, :] = jnp.exp(cum)
        fac_ref[at, :] = rates[j] * jnp.exp(total - cum)
        col_ref[at, :] = cum
        cum_t[:, at] = cum.T
        rate_t[:, at] = rates[j].T
        mid = rates[j] * jnp.exp(jnp.minimum((mid_f if j == 0 else mid_b) - near, 0.0))
        mid_t[:, at] = mid.T

    for k in range(gain_in.shape[0]):
        if k == 0:
            gain_load.wait()
        gain_ref[0:1, k * 128 : (k + 1) * 128] = gain_in[k : k + 1, :].astype(F32)

    for i in range(3):
        remote(sources[i].at[:, pl.ds(0, halves[i])], (px, pb, pc)[i], half_sem.at[0, i],
               half_sem.at[1, i], partner).wait_recv()
    for low, present in ((True, has_prev), (False, has_next)):

        @pl.when(present)
        def _(low=low):
            for i in range(3):
                edge_copy(i, low, 0).wait_recv()

    def rolled(v, p):
        return pltpu.roll(v, lax.rem(128 - p * per_pair, 128), 1)

    def two(cols, i):
        mask = lax.broadcasted_iota(jnp.int32, (cols.shape[0], 128), 1) < HEAD_DIM
        return jnp.where(mask, cols[:, i : i + 1], cols[:, i + 1 : i + 2])

    offsets = (0, 2 * own[0].shape[1], 2 * own[0].shape[1] + 2 * own[1].shape[1])

    def conv(i, col, spot):
        half = halves[i]
        mine_at = pl.ds(pl.multiple_of(core * half + col, 128), 128)
        at = pl.ds(pl.multiple_of(col, 128), 128)
        buf = work.at[spot]
        buf[pl.ds(pl.multiple_of(8 + core * blk, 8), blk), :] = sources[i][:, mine_at].astype(F32)
        buf[pl.ds(pl.multiple_of(8 + other * blk, 8), blk), :] = (px, pb, pc)[i][:, at].astype(F32)
        buf[0:8, :] = jnp.where(has_prev, edges[i][:, at].astype(F32), 0.0)
        high = jnp.where(has_next, edges[3 + i][:, at].astype(F32), 0.0)
        buf[8 + tokens : 16 + tokens, :] = high
        w_at = pl.ds(pl.multiple_of(offsets[i] + col, 128), 128)
        s = buf[6 : 6 + tokens, :] * w_ref[0:1, w_at]
        for k in range(1, 4):
            s = s + buf[6 + k : 6 + k + tokens, :] * w_ref[k : k + 1, w_at]
        h = 0.5 * s
        return h + h * jnp.tanh(h)

    def up_copy(k, i):
        qy, qx, q = member(i)
        return remote(
            sup.at[k, q], up_in.at[k, me], up_sem.at[0, k, i], up_sem.at[1, k, me],
            quad_id(qy, qx),
        )

    def wide_left(n):
        return lax.rem(lax.broadcasted_iota(jnp.int32, (128, n), 1), 128) < HEAD_DIM

    def first(k, i, _):
        _, _, p = member(i)
        if k < 2:
            g = 2 * p + k
            bt[g] = conv(1, g * 128, 0).T.astype(BF16)
        col = p * x_w + k * 128
        xv = conv(0, col, 1).astype(BF16)
        xc[:, pl.ds(pl.multiple_of(col, 128), 128)] = xv
        xf = xv.astype(F32)
        cols = rolled(fac_ref[...], p)
        rhs = jnp.concatenate(
            [(xf * two(cols, d * hh + 2 * k)).astype(BF16) for d in range(2)], axis=1
        )
        u = jnp.dot(bt[2 * p + k // 2], rhs, preferred_element_type=F32)
        if k == 1:
            v = jnp.dot(bt[2 * p + 1], rhs, preferred_element_type=F32)
            u = jnp.where(wide_left(256), u, v)
        u = u.astype(BF16)

        @pl.when(i < 3)
        def _():
            sup[k, p, 0] = u[:, :128]
            sup[k, p, 1] = u[:, 128:]
            up_copy(k, i).start()

        @pl.when(i == 3)
        def _():
            up_in[k, p, 0] = u[:, :128]
            up_in[k, p, 1] = u[:, 128:]

        return 0

    def inner(p, _):
        x_at = [pl.ds(pl.multiple_of(p * x_w + k * 128, 128), 128) for k in range(tiles)]
        for g in range(2):
            at = pl.ds(pl.multiple_of((2 * p + g) * 128, 128), 128)
            cc[:, at] = conv(2, (2 * p + g) * 128, g).astype(BF16)
        for r in range(2):
            rows = slice(r * blk, (r + 1) * blk)
            cols = rolled(col_ref[rows, :], p)
            mid_row = mid_f if r == 1 else mid_b
            shift = rolled(jnp.exp(jnp.minimum(col_ref[rows, :] - mid_row, 0.0)), p)
            parts = []
            for g in range(2):
                at = pl.ds(pl.multiple_of((2 * p + g) * 128, 128), 128)
                scores = jnp.dot(cc[rows, at], bt[2 * p + g], preferred_element_type=F32)
                on = scores[:, r * blk : (r + 1) * blk]
                away = scores[:, (1 - r) * blk : (2 - r) * blk]
                for h in range(g * per_pair // 2, (g + 1) * per_pair // 2):
                    f = pl.ds(p * per_pair + h, 1)
                    b = pl.ds(hh + p * per_pair + h, 1)
                    gap_f = cols[:, h : h + 1] - cum_t[f, rows]
                    gap_b = cols[:, hh + h : hh + h + 1] - cum_t[b, rows]
                    gap = jnp.where(lane < row, gap_f, jnp.where(lane > row, gap_b, 0.0))
                    rf, rb = rate_t[f, rows], rate_t[b, rows]
                    scale = jnp.where(lane < row, rf, jnp.where(lane > row, rb, rf + rb))
                    near = (on * jnp.exp(gap) * scale).astype(BF16)
                    d = 1 - r
                    c = d * hh + h
                    far_rows = slice((1 - r) * blk, (2 - r) * blk)
                    far_row = mid_t[f if d == 0 else b, far_rows]
                    far = (away * shift[:, c : c + 1] * far_row).astype(BF16)
                    parts.append(jnp.concatenate([near, far] if r == 0 else [far, near], axis=1))
            for k in range(tiles):
                xt = xc[:, x_at[k]]
                zero = jnp.zeros_like(xt)
                mask = lax.broadcasted_iota(jnp.int32, xt.shape, 1) < HEAD_DIM
                both = jnp.concatenate(
                    [jnp.where(mask, xt, zero), jnp.where(mask, zero, xt)], axis=0
                )
                w = jnp.concatenate([parts[2 * k], parts[2 * k + 1]], axis=1)
                y_ref[rows, x_at[k]] = jnp.dot(w, both, preferred_element_type=F32)
        return 0

    def zlog_copy(o):
        return remote(
            zsum, zlog.at[cz], zlog_sem.at[0, o], zlog_sem.at[1, cz], z_id(lax.rem(cz + o, nz))
        )

    def lanes_of(log_row, d, k):
        return two(rolled(log_row, me), d * hh + 2 * k)

    def quad_logs():
        for i in range(3):
            _, _, q = member(i)
            remote(
                logs, qlog.at[q], qlog_sem.at[0, i], qlog_sem.at[1, q], partner
            ).wait_recv()
        zsum[...] = qlog[0] + qlog[1] + qlog[2] + qlog[3]
        for o in range(1, nz):
            zlog_copy(o).start()
        zlog[cz] = zsum[...]
        for d in range(2):
            for k in range(tiles):
                each = [lanes_of(qlog[q], d, k) for q in range(4)]
                reach = jnp.zeros_like(each[0])
                for q in reversed(range(4)) if d == 0 else range(4):
                    dec[q, d, k] = jnp.exp(each[q])
                    wup[q, d, k] = jnp.exp(reach)
                    reach = reach + each[q]

    def z_logs():
        for o in range(1, nz):
            s = lax.rem(cz + o, nz)
            remote(
                zsum, zlog.at[s], zlog_sem.at[0, o], zlog_sem.at[1, s], partner
            ).wait_recv()
        reach = [[jnp.zeros((8, 128), F32) for _ in range(2)] for _ in range(rounds)]
        for s in range(nz):
            for r in range(rounds):
                h = 1 << r
                pos = lax.rem(cz, 2 * h)
                middle = cz - pos + h
                f_in = jnp.logical_and(s >= middle, s < cz)
                b_in = jnp.logical_and(s > cz, s < middle)
                reach[r][0] = reach[r][0] + jnp.where(f_in, zlog[s], 0.0)
                reach[r][1] = reach[r][1] + jnp.where(b_in, zlog[s], 0.0)
        for d in range(2):
            for k in range(tiles):
                zdec[d, k] = jnp.exp(lanes_of(zsum[...], d, k))
                for r in range(rounds):
                    zwt[r, d, k] = jnp.exp(lanes_of(reach[r][d], d, k))

    def combine(k):
        for i in range(3):
            _, _, q = member(i)
            remote(
                sup.at[k, q], up_in.at[k, q], up_sem.at[0, k, i], up_sem.at[1, k, q], partner
            ).wait_recv()
        for d in range(2):
            acc = up_in[k, 0, d].astype(F32) * wup[0, d, k, 0:1, :]
            for q in range(1, 4):
                acc = acc + up_in[k, q, d].astype(F32) * wup[q, d, k, 0:1, :]
            tz[k, d] = acc
            zin[k, d] = jnp.zeros_like(acc)

    def z_copy(r, k, o, d):
        return remote(
            zs.at[r, k], zr.at[r, k], zsend_sem.at[r, k, o - 1], zrecv_sem.at[r, k],
            z_id(cz + o if d == 0 else cz - o),
        )

    def z_parts(r):
        h = 1 << r
        pos = lax.rem(cz, 2 * h)
        return h, pos, ((0, pos == h - 1), (1, pos == h))

    def z_send(r, k):
        h, pos, senders = z_parts(r)
        for d, sender in senders:

            @pl.when(sender)
            def _(d=d):
                zs[r, k] = (zin[k, d] * zdec[d, k, 0:1, :] + tz[k, d]).astype(BF16)
                for o in reversed(range(1, h + 1)):
                    z_copy(r, k, o, d).start()

    def z_recv(r, k):
        h, pos, _ = z_parts(r)
        z_copy(r, k, 1, 0).wait_recv()
        for d, receiver in ((0, pos >= h), (1, pos < h)):

            @pl.when(receiver)
            def _(d=d):
                zin[k, d] = zin[k, d] + zr[r, k].astype(F32) * zwt[r, d, k, 0:1, :]

    def down_copy(k, i):
        qy, qx, q = member(i)
        return remote(
            down_out.at[k, q], down_in.at[k, me], down_sem.at[0, k, i], down_sem.at[1, k, me],
            quad_id(qy, qx),
        )

    def down(k):
        for d in range(2):
            g = zin[k, d]
            order = list(range(4)) if d == 0 else list(reversed(range(4)))
            for q in order:
                down_out[k, q, d] = g.astype(BF16)
                if q != order[-1]:
                    g = g * dec[q, d, k, 0:1, :] + up_in[k, q, d].astype(F32)
        for i in range(3):
            down_copy(k, i).start()
        down_in[k, me] = down_out[k, me]

    def gate(mixed, at):
        z = in_z[:, at].astype(F32)
        half_z = 0.5 * z
        gated = mixed.astype(F32) * (half_z + half_z * jnp.tanh(half_z))
        square = gated * gated
        low = jnp.sum(jnp.where(left, square, 0.0), axis=1, keepdims=True)
        high = jnp.sum(jnp.where(left, 0.0, square), axis=1, keepdims=True)
        mean = jnp.where(left, low, high) * (1.0 / HEAD_DIM)
        out_ref[:, at] = (gated * lax.rsqrt(mean + 1e-6) * gain_ref[0:1, at]).astype(BF16)

    def mix_copy(k, p):
        return remote(
            mix_out.at[k, p], mix_in.at[k, p], mix_sem.at[0, k, p], mix_sem.at[1, k, p], partner
        )

    def last(k, j, _):
        i = 3 - j
        _, _, p = member(i)

        @pl.when(i < 3)
        def _():
            remote(
                down_out.at[k, p], down_in.at[k, p], down_sem.at[0, k, i], down_sem.at[1, k, p],
                partner,
            ).wait_recv()

        rhs = jnp.concatenate([down_in[k, p, 0], down_in[k, p, 1]], axis=1)
        at = pl.ds(pl.multiple_of(p * x_w + k * 128, 128), 128)
        for mine in (False, True):
            start = pl.multiple_of((core if mine else other) * blk, 128)
            rows = pl.ds(start, blk)
            c_at = [pl.ds(pl.multiple_of((2 * p + g) * 128, 128), 128) for g in range(2)]
            v = jnp.dot(cc[rows, c_at[k // 2]], rhs, preferred_element_type=F32)
            if k == 1:
                u = jnp.dot(cc[rows, c_at[1]], rhs, preferred_element_type=F32)
                v = jnp.where(wide_left(256), v, u)
            cols = rolled(cum_ref[rows, :], p)
            y = y_ref[rows, at] + v[:, :128] * two(cols, 2 * k) + v[:, 128:] * two(cols, hh + 2 * k)
            mixed = y.astype(BF16)
            if mine:
                gate(mixed, pl.ds(pl.multiple_of(core * x_half + p * x_w + k * 128, 128), 128))
            else:
                mix_out[k, p] = mixed
                mix_copy(k, p).start()
        return 0

    def take(k, p, _):
        mix_copy(k, p).wait_recv()
        gate(mix_in[k, p], pl.ds(pl.multiple_of(other * x_half + p * x_w + k * 128, 128), 128))
        return 0

    def finish(k):
        lax.fori_loop(0, hp, functools.partial(take, k), 0)

    lax.fori_loop(0, 4, functools.partial(first, 0), 0)
    quad_logs()
    lax.fori_loop(0, 4, functools.partial(first, 1), 0)
    z_logs()
    combine(0)
    z_send(0, 0)
    lax.fori_loop(0, 4, functools.partial(first, 2), 0)
    lax.fori_loop(0, 1, inner, 0)
    z_recv(0, 0)
    for r in range(1, rounds):
        z_send(r, 0)
        if r < rounds - 1:
            z_recv(r, 0)
    combine(1)
    z_send(0, 1)
    lax.fori_loop(1, 2, inner, 0)
    z_recv(0, 1)
    for r in range(1, rounds):
        z_send(r, 1)
        if r < rounds - 1:
            z_recv(r, 1)
    combine(2)
    z_send(0, 2)
    if rounds > 1:
        z_recv(rounds - 1, 0)
    down(0)
    lax.fori_loop(2, 3, inner, 0)
    z_recv(0, 2)
    for r in range(1, rounds):
        z_send(r, 2)
        if r < rounds - 1:
            z_recv(r, 2)
    if rounds > 1:
        z_recv(rounds - 1, 1)
    down(1)
    lax.fori_loop(3, hp, inner, 0)
    if rounds > 1:
        z_recv(rounds - 1, 2)
    down(2)
    z_load.wait()
    for k in range(3):
        lax.fori_loop(0, 4, functools.partial(last, k), 0)
        if k > 0:
            finish(k - 1)
    finish(2)

    for x in range(2):

        @pl.when(x * 2 + holder != here)
        def _(x=x):
            for i in range(5):
                param_copy(i, x).wait_send()

    for low, sends in ((True, sends_low), (False, sends_high)):

        @pl.when(sends)
        def _(low=low):
            for i in range(3):
                for k in range(2):
                    edge_copy(i, low, k).wait_send()

    for i in range(3):
        inc_copy(i).wait_send()
        half_copy(i).wait_send()
        qlog_copy(i).wait_send()
    for o in range(1, nz):
        zlog_copy(o).wait_send()
    for k in range(3):
        for i in range(3):
            up_copy(k, i).wait_send()
            down_copy(k, i).wait_send()
        for p in range(hp):
            mix_copy(k, p).wait_send()
        for r in range(rounds):
            h, _, senders = z_parts(r)
            for d, sender in senders:

                @pl.when(sender)
                def _(k=k, r=r, d=d, h=h):
                    for o in range(1, h + 1):
                        z_copy(r, k, o, d).wait_send()


def fits_quad(sp, dp, blk, heads, groups):
    nz = dp // 2
    power = dp % 2 == 0 and nz > 1 and nz & (nz - 1) == 0
    shares = sp == 4 and groups % 4 == 0 and groups // 4 == sp
    return power and shares and blk == 128 and 2 * heads * HEAD_DIM == 3 * groups * 128


def quad_local(sp, dp, x, b, c, z, ahead, back, spike, wx, wb, wc, offset, fading, gain):
    x, b, c, z = x[0], b[0], c[0], z[0]
    blk, x_total = x.shape
    b_total = b.shape[1]
    groups = b_total // STATE
    heads = ahead.shape[2]
    pairs = groups // 2
    nz = dp // 2
    rounds = nz.bit_length() - 1
    tiles = heads // pairs * HEAD_DIM // 128
    hp, hh = pairs // 2, heads // 2
    x_half, b_half = x_total // 2, b_total // 2
    width = x_half + 2 * b_half
    params = (wx, wb, wc, offset, fading)
    vm = pltpu.VMEM
    gains = gain.reshape(x_total // 128, 128)
    scratch = [vm(one.shape, BF16) for one in (x, b, c, z)]
    scratch += [vm((2, 3, hh, blk), F32), vm((3, hh, blk), F32), vm(gains.shape, BF16)]
    scratch += [vm((blk, x_half), BF16), vm((blk, b_half), BF16), vm((blk, b_half), BF16)]
    scratch += [vm(one.shape, one.dtype) for one in params]
    scratch += [vm((2,) + one.shape, one.dtype) for one in params]
    scratch += [vm((EDGE, n), BF16) for n in (x_half, b_half, b_half)] * 2
    scratch += [vm((2, 2 * blk + 16, 128), F32), vm((8, width), F32), vm((8, 128), F32)]
    scratch += [vm((8, x_total), F32)] + [vm((2 * blk, 128), F32)] * 3
    scratch += [vm((128, 2 * blk), F32)] * 3
    scratch += [vm((2 * blk, x_half), BF16), vm((2 * hp, STATE, 2 * blk), BF16)]
    scratch += [vm((2 * blk, b_half), BF16), vm((2 * blk, x_half), F32)]
    scratch += [vm((tiles, 4, 2, STATE, 128), BF16)] * 4
    scratch += [vm((8, 128), F32), vm((4, 8, 128), F32), vm((8, 128), F32), vm((nz, 8, 128), F32)]
    scratch += [vm((4, 2, tiles, 8, 128), F32)] * 2 + [vm((2, tiles, 8, 128), F32)]
    scratch += [vm((rounds, 2, tiles, 8, 128), F32)]
    scratch += [vm((tiles, 2, STATE, 128), F32)] * 2 + [vm((rounds, tiles, STATE, 128), BF16)] * 2
    scratch += [vm((tiles, hp, blk, 128), BF16)] * 2
    dma = pltpu.SemaphoreType.DMA
    scratch += [dma((16,)), dma((2, 5, 2)), dma((2, 3, 2)), dma((2, 3)), dma((2, 3))]
    scratch += [dma((2, 4)), dma((2, nz)), dma((2, tiles, 4)), dma((rounds, tiles, nz))]
    scratch += [dma((rounds, tiles)), dma((2, tiles, 4)), dma((2, tiles, hp))]
    out = pl.pallas_call(
        functools.partial(quad_kernel, (heads, pairs, sp, dp)),
        out_shape=pltpu.VMEM((blk, x_total), BF16),
        in_specs=[pl.BlockSpec(memory_space=pltpu.HBM)] * 13,
        out_specs=pl.BlockSpec(memory_space=pltpu.VMEM),
        scratch_shapes=scratch,
        compiler_params=pltpu.CompilerParams(
            collective_id=0, has_side_effects=True, vmem_limit_bytes=60 * 2**20
        ),
        name="mixer",
    )(x, b, c, z, ahead[0].T, back[0].T, spike[0].T, *params, gains)
    return out[None]


def pick(sp, dp, x, b, *rest):
    blk, heads = x.shape[1], rest[2].shape[2]
    if fits_quad(sp, dp, blk, heads, b.shape[2] // STATE):
        return quad_local(sp, dp, x, b, *rest)
    return local(sp, dp, x, b, *rest)


def solution(mesh):
    tokens = P("dp", "sp", None)
    placed = (tokens,) * 7 + (P(None, "sp"),) * 5 + (P(),)
    return jax.shard_map(
        functools.partial(pick, mesh.shape["sp"], mesh.shape["dp"]),
        mesh=mesh,
        in_specs=placed,
        out_specs=tokens,
        check_vma=False,
    )
```

```python
import functools

import jax
import jax.numpy as jnp
from jax import lax
from jax.experimental import pallas as pl
from jax.experimental.pallas import tpu as pltpu
from jax.sharding import PartitionSpec as P

F32 = jnp.float32
BF16 = jnp.bfloat16
HEAD_DIM = 64
STATE = 128
EDGE = 8
HIGHEST = lax.Precision.HIGHEST


def levels_of(sp, dp, groups):
    found = []
    split = 1
    core = 2 if sp % 2 == 0 else 1
    inner = 2 if dp % 2 == 0 and groups % (2 * sp) == 0 else 1
    for axis, count, stride in (("sp", core, 1), ("sp", sp // core, core), ("dp", inner, 1)):
        if count > 1:
            found.append((axis, count, stride))
            split *= count
    return tuple(found), ("dp", dp // inner, inner)


def digit_of(level):
    axis, count, stride = level
    return lax.rem(lax.axis_index(axis) // stride, count)


def member_id(level, member):
    axis, count, stride = level
    return {axis: lax.axis_index(axis) + (member - digit_of(level)) * stride}


def kernel(levels, top, sizes, *refs):
    heads, pairs, chunks, sp, dp = sizes
    (x_ref, b_ref, c_ref, z_ref, ahead_ref, back_ref, spike_ref) = refs[:7]
    params = refs[7:12]
    gain_ref, out_ref = refs[12:14]
    (xc, bc, cc, y_ref, cum_ref, rate_ref, cum_t, rate_t, fac_ref) = refs[14:23]
    refs = refs[:14] + refs[23:]
    got, w_ref, prm_ref, halo_ref, edges, early_sem, edge_sem = (
        refs[14:19], refs[19], refs[20], refs[21], refs[22:28], refs[28], refs[29]
    )
    rest = list(refs[30:])
    depth = len(levels)
    logs = [rest.pop(0) for _ in range(depth + 1)]
    up_log = [rest.pop(0) for _ in range(depth + 1)]
    decay = [rest.pop(0) for _ in range(depth + 1)]
    log_sem = [rest.pop(0) for _ in range(depth + 1)]
    totals, up, down, stage, sems, incoming = ([] for _ in range(6))
    for _ in range(chunks):
        totals.append([rest.pop(0) for _ in range(depth + 1)])
        up.append([rest.pop(0) for _ in range(depth + 1)])
        down.append([rest.pop(0) for _ in range(depth)])
        stage.append([rest.pop(0) for _ in range(depth)])
        sems.append([rest.pop(0) for _ in range(depth + 1)])
        incoming.append(rest.pop(0))
    blk = x_ref.shape[0]
    per_pair = heads // pairs
    x_w = per_pair * HEAD_DIM
    b_w = 2 * STATE
    tiles = x_w // 128
    lane = lax.broadcasted_iota(jnp.int32, (blk, 128), 1)
    left = lane < HEAD_DIM
    row = lax.broadcasted_iota(jnp.int32, (blk, 128), 0)

    segment = ("sp", sp, 1)
    here, there = lax.axis_index("sp"), lax.axis_index("dp")
    rank = there * sp + here
    has_next, has_prev = rank < sp * dp - 1, rank > 0
    after = {"sp": lax.rem(here + 1, sp), "dp": lax.rem(there + (here + 1) // sp, dp)}
    before = {
        "sp": lax.rem(here + sp - 1, sp),
        "dp": lax.rem(there + dp - (sp - here) // sp, dp),
    }
    mesh_id = pl.DeviceIdType.MESH
    barrier = pltpu.get_barrier_semaphore()
    greeted = 0
    for level in levels + (top, segment):
        me = digit_of(level)
        for o in range(1, level[1]):
            target = member_id(level, lax.rem(me + o, level[1]))
            pl.semaphore_signal(barrier, inc=1, device_id=target, device_id_type=mesh_id)
            greeted += 1
    for present, target in ((has_next, after), (has_prev, before)):

        @pl.when(present)
        def _(target=target):
            pl.semaphore_signal(barrier, inc=1, device_id=target, device_id_type=mesh_id)

    filler = jnp.zeros((128 - 2 * heads, blk), F32)
    inc = jnp.concatenate([ahead_ref[...], back_ref[...], filler], axis=0).T
    spikes = jnp.concatenate([spike_ref[...], spike_ref[...], filler], axis=0).T
    count = sp * dp
    neighbours = (rank + count - 1) // count + (2 * count - 2 - rank) // count
    pl.semaphore_wait(barrier, greeted + neighbours)

    def edge_copy(i, direction):
        src = (x_ref, b_ref, c_ref)[i]
        start = blk - EDGE if direction == 0 else 0
        return pltpu.make_async_remote_copy(
            src_ref=src.at[pl.ds(start, EDGE), :],
            dst_ref=edges[3 * direction + i],
            send_sem=edge_sem.at[0, direction, i],
            recv_sem=edge_sem.at[1, direction, i],
            device_id=(after, before)[direction],
            device_id_type=mesh_id,
        )

    def param_copy(i, member, slot):
        return pltpu.make_async_remote_copy(
            src_ref=params[i],
            dst_ref=got[i].at[slot],
            send_sem=early_sem.at[0, i, member],
            recv_sem=early_sem.at[1, i, slot],
            device_id=member_id(segment, member),
            device_id_type=mesh_id,
        )

    for o in range(1, sp):
        for i in range(5):
            param_copy(i, lax.rem(here + o, sp), here).start()
    for direction, present in ((0, has_next), (1, has_prev)):

        @pl.when(present)
        def _(direction=direction):
            for i in range(3):
                edge_copy(i, direction).start()

    for i in range(5):
        got[i][here] = params[i][...]
    for o in range(1, sp):
        for i in range(5):
            s = lax.rem(here + o, sp)
            param_copy(i, s, s).wait_recv()
    prm_ref[...] = jnp.zeros_like(prm_ref)
    wide = got[3].shape[2]
    for q in range(sp):
        for kind in range(2):
            for d in range(2):
                at = slice(d * heads + q * wide, d * heads + (q + 1) * wide)
                prm_ref[kind : kind + 1, at] = got[3 + kind][q, d : d + 1, :]
        off = 0
        for i in range(3):
            n = got[i].shape[2]
            w_ref[0:4, off + q * n : off + (q + 1) * n] = got[i][q].astype(F32)
            off += n * sp
    rate = jax.nn.softplus(inc + prm_ref[0:1, :])
    log_decay = -jnp.exp(prm_ref[1:2, :]) * rate + spikes
    lower = (lane <= row).astype(F32)
    upper = (lane >= row).astype(F32)
    cum_f = jnp.dot(lower, log_decay, precision=HIGHEST, preferred_element_type=F32)
    cum_b = jnp.dot(upper, log_decay, precision=HIGHEST, preferred_element_type=F32)
    cum = jnp.where(lane < heads, cum_f, cum_b)
    lane1 = lane[0:1]
    last = jnp.where(lane1 < heads, cum_f[blk - 1 : blk], cum_b[0:1])
    cum_ref[...] = cum
    rate_ref[...] = rate
    cum_t[...] = cum.T
    rate_t[...] = rate.T
    fac_ref[...] = rate * jnp.exp(last - cum)
    logs[0][...] = jnp.broadcast_to(last, (8, 128))

    def rolled(ref, p):
        return pltpu.roll(ref[...], lax.rem(128 - p * per_pair, 128), 1)

    def two(cols, i):
        return jnp.where(left, cols[:, i : i + 1], cols[:, i + 1 : i + 2])

    def conv(src, col, width, off):
        at = pl.ds(pl.multiple_of(off + col, 128), width)
        v = src[:, pl.ds(pl.multiple_of(col, 128), width)].astype(F32)
        r = lax.broadcasted_iota(jnp.int32, (blk, width), 0)
        h0, h1, h2 = halo_ref[0:1, at], halo_ref[1:2, at], halo_ref[2:3, at]
        m1 = jnp.where(r == 0, h1, pltpu.roll(v, 1, 0))
        m2 = jnp.where(r == 0, h0, jnp.where(r == 1, h1, pltpu.roll(v, 2, 0)))
        p1 = jnp.where(r == blk - 1, h2, pltpu.roll(v, blk - 1, 0))
        s = m2 * w_ref[0:1, at] + m1 * w_ref[1:2, at] + v * w_ref[2:3, at] + p1 * w_ref[3:4, at]
        return (s / (1.0 + jnp.exp(-s))).astype(BF16)

    share = pairs // chunks
    x_total = x_ref.shape[1]
    b_total = b_ref.shape[1]

    def first(c, p, _):
        x_at = pl.ds(pl.multiple_of(p * x_w, 128), x_w)
        b_at = pl.ds(pl.multiple_of(p * b_w, 128), b_w)
        xv = conv(x_ref, p * x_w, x_w, 0)
        bv = conv(b_ref, p * b_w, b_w, x_total)
        xc[:, x_at] = xv
        bc[:, b_at] = bv
        cc[:, b_at] = conv(c_ref, p * b_w, b_w, x_total + b_total)
        cols = rolled(fac_ref, p)
        xf = xv.astype(F32)
        for d in range(2):
            scaled = jnp.concatenate(
                [
                    (xf[:, k * 128 : (k + 1) * 128] * two(cols, d * heads + 2 * k)).astype(BF16)
                    for k in range(tiles)
                ],
                axis=1,
            )
            u = lax.dot_general(scaled, bv, (((0,), (0,)), ((), ())), preferred_element_type=F32)
            half = x_w // 2
            rows = pl.ds(pl.multiple_of((p - c * share) * x_w, 128), x_w)
            totals[c][0][d, rows, :] = jnp.concatenate(
                [u[:half, :STATE], u[half:, STATE:]], axis=0
            ).astype(BF16)
        return 0

    for direction, present in ((0, has_prev), (1, has_next)):

        @pl.when(present)
        def _(direction=direction):
            for i in range(3):
                edge_copy(i, direction).wait_recv()

    off = 0
    for i in range(3):
        n = edges[i].shape[1]
        low = edges[i][...].astype(F32)
        high = edges[3 + i][...].astype(F32)
        halo_ref[0:2, off : off + n] = jnp.where(has_prev, low[EDGE - 2 :], 0.0)
        halo_ref[2:3, off : off + n] = jnp.where(has_next, high[0:1], 0.0)
        off += n
    def inner(p, _):
        x_at = pl.ds(pl.multiple_of(p * x_w, 128), x_w)
        b_at = pl.ds(pl.multiple_of(p * b_w, 128), b_w)
        bv, cv, xv = bc[:, b_at], cc[:, b_at], xc[:, x_at]
        cols = rolled(cum_ref, p)
        parts = []
        for g in range(2):
            scores = lax.dot_general(
                cv[:, g * STATE : (g + 1) * STATE],
                bv[:, g * STATE : (g + 1) * STATE],
                (((1,), (1,)), ((), ())),
                preferred_element_type=F32,
            )
            for i in range(per_pair // 2):
                h = g * (per_pair // 2) + i
                hf = p * per_pair + h
                gap_f = cols[:, h : h + 1] - cum_t[pl.ds(hf, 1), :]
                gap_b = cols[:, heads + h : heads + h + 1] - cum_t[pl.ds(heads + hf, 1), :]
                gap = jnp.where(lane < row, gap_f, jnp.where(lane > row, gap_b, 0.0))
                rf, rb = rate_t[pl.ds(hf, 1), :], rate_t[pl.ds(heads + hf, 1), :]
                scale = jnp.where(lane < row, rf, jnp.where(lane > row, rb, rf + rb))
                parts.append((scores * jnp.exp(gap) * scale).astype(BF16))
        for k in range(tiles):
            xt = xv[:, k * 128 : (k + 1) * 128]
            zero = jnp.zeros_like(xt)
            both = jnp.concatenate([jnp.where(left, xt, zero), jnp.where(left, zero, xt)], axis=0)
            w = jnp.concatenate([parts[2 * k], parts[2 * k + 1]], axis=1)
            y_ref[:, pl.ds(pl.multiple_of(p * x_w + k * 128, 128), 128)] = jnp.dot(
                w, both, preferred_element_type=F32
            )
        return 0

    def copy(src, dst, send, recv, level, member):
        return pltpu.make_async_remote_copy(
            src_ref=src,
            dst_ref=dst,
            send_sem=send,
            recv_sem=recv,
            device_id=member_id(level, member),
            device_id_type=pl.DeviceIdType.MESH,
        )

    every_level = levels + (top,)
    head_share = heads // chunks
    bases = [jnp.int32(0)]
    size = head_share
    for level in levels:
        size = size // level[1]
        bases.append(bases[-1] + digit_of(level) * size)
    pending = [[] for _ in range(chunks)]

    def head_rows(h):
        return pl.ds(pl.multiple_of(h * HEAD_DIM, HEAD_DIM), HEAD_DIM)

    def log_copy(k, member, slot):
        sem = log_sem[k]
        return copy(
            logs[k], up_log[k].at[slot], sem.at[0, member], sem.at[1, slot], every_level[k], member
        )

    def start_up(c, k):
        level = every_level[k]
        n, me = level[1], digit_of(level)
        total, sem = totals[c][k], sems[c][k]
        rows = total.shape[1] // n
        for o in range(1, n):
            m = lax.rem(me + o, n)
            if c == 0:
                pending[c].append(log_copy(k, m, me))
            if k < depth:
                part = total.at[:, pl.ds(pl.multiple_of(m * rows, 64), rows), :]
            else:
                part = total.at[jnp.where(m < me, 1, 0)]
            pending[c].append(
                copy(part, up[c][k].at[me], sem.at[0, m], sem.at[1, me], level, m)
            )
        for one in pending[c]:
            one.start()
        if k < depth:
            up[c][k][me] = total[:, pl.ds(pl.multiple_of(me * rows, 64), rows), :]
        if c == 0:
            up_log[k][me] = logs[k][...]

    def flush(c):
        for one in pending[c]:
            one.wait_send()
        pending[c].clear()

    def finish_up(c, k):
        level = every_level[k]
        n, me = level[1], digit_of(level)
        total, sem = totals[c][k], sems[c][k]
        flush(c)
        for o in range(1, n):
            s = lax.rem(me + o, n)
            if c == 0:
                log_copy(k, s, s).wait_recv()
            part = total.at[:, pl.ds(0, total.shape[1] // n), :] if k < depth else total.at[0]
            copy(part, up[c][k].at[s], sem.at[0, s], sem.at[1, s], level, s).wait_recv()
        if c == 0:

            def expand(m, _):
                decay[k][m] = jnp.exp(jnp.broadcast_to(up_log[k][m][0:1, :], (128, 128)).T)
                return 0

            lax.fori_loop(0, n, expand, 0)
            if k < depth:
                log_sum = up_log[k][0]
                for m in range(1, n):
                    log_sum = log_sum + up_log[k][m]
                logs[k + 1][...] = log_sum

    def gather(c, k):
        n = levels[k][1]
        base = c * head_share + bases[k + 1]
        part, new = up[c][k], totals[c][k + 1]

        def one_head(h, _):
            at = head_rows(h)
            f = part[0, 0, at, :].astype(F32)
            b = part[n - 1, 1, at, :].astype(F32)
            for m in range(1, n):
                r = n - 1 - m
                f = f * decay[k][m, pl.ds(base + h, 1), :] + part[m, 0, at, :].astype(F32)
                b = b * decay[k][r, pl.ds(heads + base + h, 1), :] + part[r, 1, at, :].astype(F32)
            new[0, at, :] = f.astype(BF16)
            new[1, at, :] = b.astype(BF16)
            return 0

        lax.fori_loop(0, new.shape[1] // HEAD_DIM, one_head, 0)

    def enter(c):
        n, me = top[1], digit_of(top)
        base = c * head_share + bases[-1]
        into = incoming[c]
        into[...] = jnp.zeros_like(into)

        def carry(s, d):
            def one_head(h, _):
                at = head_rows(h)
                factor = decay[depth][s, pl.ds(d * heads + base + h, 1), :]
                into[d, at, :] = into[d, at, :] * factor + up[c][depth][s, at, :].astype(F32)
                return 0

            lax.fori_loop(0, into.shape[1] // HEAD_DIM, one_head, 0)
            return 0

        lax.fori_loop(0, me, lambda s, _: carry(s, 0), 0)
        lax.fori_loop(0, n - 1 - me, lambda i, _: carry(n - 1 - i, 1), 0)

    def start_down(c, k):
        level = levels[k]
        n, me = level[1], digit_of(level)
        sem = sems[c][k]
        rows = totals[c][k].shape[1] // n
        base = c * head_share + bases[k + 1]
        source = incoming[c] if k == depth - 1 else down[c][k + 1]
        part, out = up[c][k], stage[c][k]

        def spread(h, _):
            at = head_rows(h)
            f = source[0, at, :].astype(F32)
            b = source[1, at, :].astype(F32)
            for m in range(n):
                r = n - 1 - m
                out[m, 0, at, :] = f.astype(BF16)
                out[r, 1, at, :] = b.astype(BF16)
                if m < n - 1:
                    f = f * decay[k][m, pl.ds(base + h, 1), :] + part[m, 0, at, :].astype(F32)
                    down_factor = decay[k][r, pl.ds(heads + base + h, 1), :]
                    b = b * down_factor + part[r, 1, at, :].astype(F32)
            return 0

        lax.fori_loop(0, rows // HEAD_DIM, spread, 0)
        mine = pl.ds(pl.multiple_of(me * rows, 64), rows)
        for o in range(1, n):
            m = lax.rem(me + o, n)
            pending[c].append(
                copy(out.at[m], down[c][k].at[:, mine, :], sem.at[2, m], sem.at[3, me], level, m)
            )
        for one in pending[c]:
            one.start()
        down[c][k][:, mine, :] = out[me]

    def finish_down(c, k):
        level = levels[k]
        n, me = level[1], digit_of(level)
        sem = sems[c][k]
        rows = totals[c][k].shape[1] // n
        flush(c)
        for o in range(1, n):
            s = lax.rem(me + o, n)
            theirs = pl.ds(pl.multiple_of(s * rows, 64), rows)
            copy(
                stage[c][k].at[s], down[c][k].at[:, theirs, :], sem.at[2, s], sem.at[3, s], level, s
            ).wait_recv()

    for c in range(chunks):
        lax.fori_loop(c * share, (c + 1) * share, functools.partial(first, c), 0)
        start_up(c, 0)
    for o in range(1, sp):
        for i in range(5):
            param_copy(i, lax.rem(here + o, sp), here).wait_send()
    for direction, present in ((0, has_next), (1, has_prev)):

        @pl.when(present)
        def _(direction=direction):
            for i in range(3):
                edge_copy(i, direction).wait_send()


    gaps = chunks * depth
    cuts = [(i * pairs) // gaps for i in range(gaps + 1)]
    for k in range(depth):
        for c in range(chunks):
            finish_up(c, k)
            gather(c, k)
            start_up(c, k + 1)
            at = k * chunks + c
            lax.fori_loop(cuts[at], cuts[at + 1], inner, 0)
    for c in range(chunks):
        finish_up(c, depth)
        enter(c)
        start_down(c, depth - 1)
    for k in reversed(range(1, depth)):
        for c in range(chunks):
            finish_down(c, k)
            start_down(c, k - 1)

    cum_ref[...] = jnp.exp(cum_ref[...])

    def last_part(c, p, _):
        cv = cc[:, pl.ds(pl.multiple_of(p * b_w, 128), b_w)]
        cols = rolled(cum_ref, p)
        carried = []
        for d in range(2):
            st = down[c][0][d, pl.ds(pl.multiple_of((p - c * share) * x_w, 128), x_w), :]
            got = [
                lax.dot_general(
                    cv[:, g * STATE : (g + 1) * STATE],
                    st,
                    (((1,), (1,)), ((), ())),
                    preferred_element_type=F32,
                )
                for g in range(2)
            ]
            carried.append(got)
        for k in range(tiles):
            cut = slice(k * 128, (k + 1) * 128)
            at = pl.ds(pl.multiple_of(p * x_w + k * 128, 128), 128)
            y = y_ref[:, at]
            for d in range(2):
                a, b = carried[d][0][:, cut], carried[d][1][:, cut]
                if 2 * k + 1 < per_pair // 2:
                    v = a
                elif 2 * k >= per_pair // 2:
                    v = b
                else:
                    v = jnp.where(left, a, b)
                y = y + v * two(cols, d * heads + 2 * k)
            z = z_ref[:, at].astype(F32)
            gated = y.astype(BF16).astype(F32) * (z / (1.0 + jnp.exp(-z)))
            square = gated * gated
            low = jnp.sum(jnp.where(left, square, 0.0), axis=1, keepdims=True)
            high = jnp.sum(jnp.where(left, 0.0, square), axis=1, keepdims=True)
            mean = jnp.where(left, low, high) * (1.0 / HEAD_DIM)
            out_ref[:, at] = (gated * lax.rsqrt(mean + 1e-6) * gain_ref[0:1, at]).astype(BF16)
        return 0

    for c in range(chunks):
        finish_down(c, 0)
        lax.fori_loop(c * share, (c + 1) * share, functools.partial(last_part, c), 0)


def local(sp, dp, x, b, c, z, ahead, back, spike, wx, wb, wc, offset, fading, gain):
    x, b, c, z = x[0], b[0], c[0], z[0]
    blk, x_total = x.shape
    groups = b.shape[1] // STATE
    heads = ahead.shape[2]
    pairs = groups // 2
    levels, top = levels_of(sp, dp, groups)
    scratch = [
        pltpu.VMEM((blk, x_total), BF16),
        pltpu.VMEM((blk, groups * STATE), BF16),
        pltpu.VMEM((blk, groups * STATE), BF16),
        pltpu.VMEM((blk, x_total), F32),
    ]
    scratch += [pltpu.VMEM((128, 128), F32)] * 5
    params = (wx, wb, wc, offset, fading)
    width = x_total + 2 * b.shape[1]
    early = [pltpu.VMEM((sp,) + one.shape, one.dtype) for one in params]
    early += [pltpu.VMEM((8, width), F32), pltpu.VMEM((8, 128), F32), pltpu.VMEM((8, width), F32)]
    early += [pltpu.VMEM((EDGE, one.shape[1]), BF16) for one in (x, b, c)] * 2
    early += [pltpu.SemaphoreType.DMA((2, 5, sp)), pltpu.SemaphoreType.DMA((2, 2, 3))]
    scratch += early
    split = 1
    for level in levels:
        split *= level[1]
    chunks = 2 if groups % (2 * split) == 0 else 1
    counts = [level[1] for level in levels] + [top[1]]
    scratch += [pltpu.VMEM((8, 128), F32)] * len(counts)
    scratch += [pltpu.VMEM((n, 8, 128), F32) for n in counts]
    scratch += [pltpu.VMEM((n, 128, 128), F32) for n in counts]
    scratch += [pltpu.SemaphoreType.DMA((2, n)) for n in counts]
    for _ in range(chunks):
        held = [x_total // chunks]
        for n in counts[:-1]:
            held.append(held[-1] // n)
        slabs = list(zip(counts[:-1], held[1:]))
        scratch += [pltpu.VMEM((2, rows, STATE), BF16) for rows in held]
        scratch += [pltpu.VMEM((n, 2, rows, STATE), BF16) for n, rows in slabs]
        scratch += [pltpu.VMEM((counts[-1], held[-1], STATE), BF16)]
        scratch += [pltpu.VMEM((2, rows, STATE), BF16) for rows in held[:-1]]
        scratch += [pltpu.VMEM((n, 2, rows, STATE), BF16) for n, rows in slabs]
        scratch += [pltpu.SemaphoreType.DMA((4, n)) for n in counts]
        scratch += [pltpu.VMEM((2, held[-1], STATE), F32)]
    out = pl.pallas_call(
        functools.partial(kernel, levels, top, (heads, pairs, chunks, sp, dp)),
        out_shape=jax.ShapeDtypeStruct((blk, x_total), BF16),
        in_specs=[pl.BlockSpec(memory_space=pltpu.VMEM)] * 13,
        out_specs=pl.BlockSpec(memory_space=pltpu.VMEM),
        scratch_shapes=scratch,
        compiler_params=pltpu.CompilerParams(
            collective_id=0, has_side_effects=True, vmem_limit_bytes=60 * 2**20
        ),
        name="mixer",
    )(x, b, c, z, ahead[0].T, back[0].T, spike[0].T, *params, gain.astype(F32)[None])
    return out[None]


def quad_kernel(sizes, *refs):
    heads, pairs, sp, dp = sizes
    nz = dp // 2
    rounds = nz.bit_length() - 1
    (x_hbm, b_hbm, c_hbm, z_hbm, ahead_hbm, back_hbm, spike_hbm) = refs[:7]
    params = refs[7:12]
    gain_hbm, out_ref = refs[12:14]
    (in_x, in_b, in_c, in_z, inc, inc_out, gain_in, px, pb, pc) = refs[14:24]
    own, got = refs[24:29], refs[29:34]
    edges = refs[34:40]
    (work, w_ref, prm_ref, gain_ref, cum_ref, fac_ref, col_ref, cum_t, rate_t, mid_t) = refs[40:50]
    low_ref, high_ref, bc, zg = refs[50:54]
    refs = refs[:50] + refs[54:]
    (xc, bt, cc, y_ref, sup, up_in, down_out, down_in) = refs[50:58]
    (logs, qlog, zsum, zlog, dec, wup, zdec, zwt) = refs[58:66]
    (tz, zin, zs, zr, mix_out, mix_in) = refs[66:72]
    (load_sem, prm_sem, edge_sem, half_sem, inc_sem, qlog_sem, zlog_sem) = refs[72:79]
    (up_sem, zsend_sem, zrecv_sem, down_sem, mix_sem) = refs[79:84]

    hh = heads // 2
    hp = pairs // 2
    per_pair = heads // pairs
    tiles = per_pair * HEAD_DIM // 128
    blk = in_x.shape[0]
    tokens = 2 * blk
    x_half = in_x.shape[1] // 2
    b_half = in_b.shape[1] // 2
    x_w = per_pair * HEAD_DIM
    mesh_id = pl.DeviceIdType.MESH

    here, there = lax.axis_index("sp"), lax.axis_index("dp")
    core, cx = lax.rem(here, 2), here // 2
    cy, cz = lax.rem(there, 2), there // 2
    other = 1 - core
    me = cy * 2 + cx
    chip = there * 2 + cx
    chips = dp * 2
    has_next, has_prev = chip < chips - 1, chip > 0
    after, before = lax.rem(chip + 1, chips), lax.rem(chip + chips - 1, chips)
    partner = {"sp": cx * 2 + other}

    def chip_id(c, k):
        return {"sp": lax.rem(c, 2) * 2 + k, "dp": c // 2}

    def quad_id(qy, qx):
        return {"sp": qx * 2 + core, "dp": cz * 2 + qy}

    def z_id(z):
        return {"dp": z * 2 + cy}

    def member(i):
        qy = lax.rem(cy + lax.rem(i + 1, 2), 2)
        qx = lax.rem(cx + (3 - i) // 2, 2)
        return qy, qx, qy * 2 + qx

    def remote(src, dst, send, recv, target):
        return pltpu.make_async_remote_copy(
            src_ref=src, dst_ref=dst, send_sem=send, recv_sem=recv,
            device_id=target, device_id_type=mesh_id,
        )

    barrier = pltpu.get_barrier_semaphore()

    def greet(target):
        pl.semaphore_signal(barrier, inc=1, device_id=target, device_id_type=mesh_id)

    for o in range(1, sp):
        greet({"sp": lax.rem(here + o, sp)})
    for i in range(3):
        qy, qx, _ = member(i)
        greet(quad_id(qy, qx))
    for o in range(1, nz):
        greet(z_id(lax.rem(cz + o, nz)))
    for present, neighbour in ((has_next, after), (has_prev, before)):

        @pl.when(present)
        def _(neighbour=neighbour):
            for k in range(2):
                greet(chip_id(neighbour, k))

    loads = []

    def load(src, dst):
        one = pltpu.make_async_copy(src, dst, load_sem.at[len(loads)])
        one.start()
        loads.append(one)
        return one

    param_loads = [load(params[i], own[i]) for i in range(5)]
    mine = pl.ds(pl.multiple_of(core * hh, 8), hh)
    theirs = pl.ds(pl.multiple_of(other * hh, 8), hh)
    raw = (ahead_hbm, back_hbm, spike_hbm)
    inc_stage = [load(raw[i].at[theirs, :], inc_out.at[i]) for i in range(3)]
    inc_loads = [load(raw[i].at[mine, :], inc.at[core, i]) for i in range(3)]
    b_load = load(b_hbm, in_b)
    x_load = load(x_hbm, in_x)
    c_load = load(c_hbm, in_c)
    gain_load = load(gain_hbm, gain_in)
    z_load = load(z_hbm, in_z)

    for one in param_loads + inc_stage:
        one.wait()
    chip_greets = 2 * ((chip + chips - 1) // chips + (2 * chips - 2 - chip) // chips)
    pl.semaphore_wait(barrier, (sp - 1) + 3 + (nz - 1) + chip_greets)

    holder = here // 2
    slot = lax.rem(here, 2)

    def param_copy(i, x):
        return remote(
            own[i], got[i].at[slot], prm_sem.at[0, i, x], prm_sem.at[1, i, slot],
            {"sp": x * 2 + holder},
        )

    for x in range(2):
        elsewhere = x * 2 + holder != here

        @pl.when(elsewhere)
        def _(x=x):
            for i in range(5):
                param_copy(i, x).start()

        @pl.when(jnp.logical_not(elsewhere))
        def _():
            for i in range(5):
                got[i][slot] = own[i][...]

    def inc_copy(i):
        return remote(
            inc_out.at[i], inc.at[core, i], inc_sem.at[0, i], inc_sem.at[1, i], partner
        )

    for i in range(3):
        inc_copy(i).start()

    sources = (in_x, in_b, in_c)
    halves = (x_half, b_half, b_half)

    def edge_copy(i, low, k):
        half = halves[i]
        start = blk - EDGE if low else 0
        return remote(
            sources[i].at[pl.ds(start, EDGE), pl.ds(k * half, half)],
            edges[i if low else 3 + i],
            edge_sem.at[0, i, k],
            edge_sem.at[1, i, 0 if low else 1],
            chip_id(after if low else before, k),
        )

    sends_low = jnp.logical_and(core == 1, has_next)
    sends_high = jnp.logical_and(core == 0, has_prev)

    def half_copy(i):
        cut = pl.ds(pl.multiple_of(other * halves[i], 128), halves[i])
        return remote(
            sources[i].at[:, cut], (px, pb, pc)[i], half_sem.at[0, i], half_sem.at[1, i], partner
        )

    for i, one in ((1, b_load), (0, x_load), (2, c_load)):
        one.wait()

        @pl.when(sends_low)
        def _(i=i):
            for k in range(2):
                edge_copy(i, True, k).start()

        @pl.when(sends_high)
        def _(i=i):
            for k in range(2):
                edge_copy(i, False, k).start()

        half_copy(i).start()

    lane = lax.broadcasted_iota(jnp.int32, (blk, 128), 1)
    row = lax.broadcasted_iota(jnp.int32, (blk, 128), 0)
    left = lane < HEAD_DIM
    left1 = left[0:1]
    lower = (lane <= row).astype(F32)
    upper = (lane >= row).astype(F32)
    filler = jnp.zeros((128 - 2 * hh, blk), F32)

    for q in range(2):
        from_q = 2 * core + q != here

        @pl.when(from_q)
        def _(q=q):
            for i in range(5):
                remote(
                    own[i], got[i].at[q], prm_sem.at[0, i, 0], prm_sem.at[1, i, q], partner
                ).wait_recv()

    for one in inc_loads:
        one.wait()
    for i in range(3):
        remote(
            inc_out.at[i], inc.at[other, i], inc_sem.at[0, i], inc_sem.at[1, i], partner
        ).wait_recv()
    prm_ref[...] = jnp.zeros_like(prm_ref)
    wide = own[3].shape[1]
    for q in range(2):
        for kind in range(2):
            for d in range(2):
                at = slice(d * hh + q * wide, d * hh + (q + 1) * wide)
                prm_ref[kind : kind + 1, at] = got[3 + kind][q, d : d + 1, :]
        off = 0
        for i in range(3):
            n = own[i].shape[1]
            part = got[i][q].astype(F32)
            for t in range(n // 128):
                w_ref[off + q * (n // 128) + t, 0:4, :] = part[:, t * 128 : (t + 1) * 128]
            off += 2 * n // 128

    cums, rates = [], []
    for j in range(2):
        pre = jnp.concatenate([inc[j, 0], inc[j, 1], filler], axis=0).T
        spikes = jnp.concatenate([inc[j, 2], inc[j, 2], filler], axis=0).T
        rate = jax.nn.softplus(pre + prm_ref[0:1, :])
        log_decay = -jnp.exp(prm_ref[1:2, :]) * rate + spikes
        cum_f = jnp.dot(lower, log_decay, precision=HIGHEST, preferred_element_type=F32)
        cum_b = jnp.dot(upper, log_decay, precision=HIGHEST, preferred_element_type=F32)
        cums.append((cum_f, cum_b))
        rates.append(rate)
    ahead_lane = lane < hh
    ahead1 = ahead_lane[0:1]
    mid_f, mid_b = cums[0][0][blk - 1 : blk], cums[1][1][0:1]
    total = jnp.where(ahead1, mid_f + cums[1][0][blk - 1 : blk], cums[0][1][0:1] + mid_b)
    logs[...] = jnp.broadcast_to(total, (8, 128))

    def qlog_copy(i):
        qy, qx, q = member(i)
        return remote(
            logs, qlog.at[me], qlog_sem.at[0, i], qlog_sem.at[1, me], quad_id(qy, qx)
        )

    for i in range(3):
        qlog_copy(i).start()
    qlog[me] = logs[...]
    for j in range(2):
        cum_f, cum_b = cums[j]
        far = jnp.where(ahead_lane, mid_f if j == 1 else 0.0, mid_b if j == 0 else 0.0)
        near = jnp.where(ahead_lane, cum_f, cum_b)
        at = slice(j * blk, (j + 1) * blk)
        cum = near + far
        cum_ref[at, :] = jnp.exp(cum)
        fac_ref[at, :] = rates[j] * jnp.exp(total - cum)
        col_ref[at, :] = cum
        cum_t[:, at] = cum.T
        rate_t[:, at] = rates[j].T
        mid = rates[j] * jnp.exp(jnp.minimum((mid_f if j == 0 else mid_b) - near, 0.0))
        mid_t[:, at] = mid.T

    gain_load.wait()
    gain_ref[...] = gain_in[...].astype(F32)

    for i in range(3):
        remote(sources[i].at[:, pl.ds(0, halves[i])], (px, pb, pc)[i], half_sem.at[0, i],
               half_sem.at[1, i], partner).wait_recv()
    def rolled(v, p):
        return pltpu.roll(v, lax.rem(128 - p * per_pair, 128), 1)

    def two(cols, i):
        mask = lax.broadcasted_iota(jnp.int32, (cols.shape[0], 128), 1) < HEAD_DIM
        return jnp.where(mask, cols[:, i : i + 1], cols[:, i + 1 : i + 2])

    tiles_of = [half // 128 for half in halves]
    starts = (0, tiles_of[0], tiles_of[0] + tiles_of[1])

    def silu(s):
        h = 0.5 * s
        return h + h * jnp.tanh(h)

    def store(i, t, rows, v):
        if i == 1:
            bc[t, rows, :] = v
        else:
            (xc, None, cc)[i][t, rows, :] = v.astype(BF16)

    def conv(i, group, _):
        for spot in range(4):
            t = group * 4 + spot
            mine_at = pl.ds(pl.multiple_of(core * halves[i] + t * 128, 128), 128)
            at = pl.ds(pl.multiple_of(t * 128, 128), 128)
            buf = work.at[spot]
            here_at = pl.ds(pl.multiple_of(8 + core * blk, 8), blk)
            there_at = pl.ds(pl.multiple_of(8 + other * blk, 8), blk)
            buf[here_at, :] = sources[i][:, mine_at].astype(F32)
            buf[there_at, :] = (px, pb, pc)[i][:, at].astype(F32)
            s = buf[6 : 6 + tokens, :] * w_ref[starts[i] + t, 0:1, :]
            for k in range(1, 4):
                s = s + buf[6 + k : 6 + k + tokens, :] * w_ref[starts[i] + t, k : k + 1, :]
            store(i, t, slice(0, tokens), silu(s))
        return 0

    def edge_wait(i):
        for low, present in ((True, has_prev), (False, has_next)):

            @pl.when(present)
            def _(low=low):
                edge_copy(i, low, 0).wait_recv()

    def fix(i):
        half = halves[i]
        row16 = row[0:16]
        own_part = sources[i]
        their_part = (px, pb, pc)[i]
        for t in range(tiles_of[i]):
            mine_at = pl.ds(pl.multiple_of(core * half + t * 128, 128), 128)
            at = slice(t * 128, (t + 1) * 128)
            start = jnp.where(core == 0, own_part[0:8, mine_at], their_part[0:8, at])
            end = jnp.where(core == 1, own_part[blk - 8 :, mine_at], their_part[blk - 8 :, at])
            low_ref[t, 0:8, :] = jnp.where(has_prev, edges[i][:, at].astype(F32), 0.0)
            low_ref[t, 8:16, :] = start.astype(F32)
            high_ref[t, 8:16, :] = end.astype(F32)
            high_ref[t, 16:24, :] = jnp.where(has_next, edges[3 + i][:, at].astype(F32), 0.0)
        dst = (xc, bc, cc)[i]
        for t in range(tiles_of[i]):
            for ref, low in ((low_ref, True), (high_ref, False)):
                s = ref[t, 6:14, :] * w_ref[starts[i] + t, 0:1, :]
                for k in range(1, 4):
                    s = s + ref[t, 6 + k : 14 + k, :] * w_ref[starts[i] + t, k : k + 1, :]
                s = silu(s)
                rows = slice(0, 16) if low else slice(tokens - 16, tokens)
                s = jnp.concatenate([s, s], axis=0)
                keep = row16 >= 2 if low else row16 < 15
                store(i, t, rows, jnp.where(keep, dst[t, rows, :].astype(F32), s))

    def up_copy(k, i):
        qy, qx, q = member(i)
        return remote(
            sup.at[k, q], up_in.at[k, me], up_sem.at[0, k, i], up_sem.at[1, k, me],
            quad_id(qy, qx),
        )

    def wide_left(n):
        return lax.rem(lax.broadcasted_iota(jnp.int32, (128, n), 1), 128) < HEAD_DIM

    def first(k):
        fac = fac_ref[...]
        for p in range(hp):
            if k < 2:
                bt[2 * p + k] = bc[2 * p + k].T.astype(BF16)
            xf = xc[p * tiles + k].astype(F32)
            head = p * per_pair + 2 * k
            rhs = jnp.concatenate(
                [(xf * two(fac, d * hh + head)).astype(BF16) for d in range(2)], axis=1
            )
            u = jnp.dot(bt[2 * p + k // 2], rhs, preferred_element_type=F32)
            if k == 1:
                v = jnp.dot(bt[2 * p + 1], rhs, preferred_element_type=F32)
                u = jnp.where(wide_left(256), u, v)
            u = u.astype(BF16)
            sup[k, p, 0] = u[:, :128]
            sup[k, p, 1] = u[:, 128:]
        for i in range(3):
            up_copy(k, i).start()
        up_in[k, me] = sup[k, me]

    def inner(p, _):
        for r in range(2):
            rows = slice(r * blk, (r + 1) * blk)
            cols = rolled(col_ref[rows, :], p)
            mid_row = mid_f if r == 1 else mid_b
            shift = rolled(jnp.exp(jnp.minimum(col_ref[rows, :] - mid_row, 0.0)), p)
            parts = []
            for g in range(2):
                scores = jnp.dot(cc[2 * p + g, rows], bt[2 * p + g], preferred_element_type=F32)
                on = scores[:, r * blk : (r + 1) * blk]
                away = scores[:, (1 - r) * blk : (2 - r) * blk]
                for h in range(g * per_pair // 2, (g + 1) * per_pair // 2):
                    f = pl.ds(p * per_pair + h, 1)
                    b = pl.ds(hh + p * per_pair + h, 1)
                    gap_f = cols[:, h : h + 1] - cum_t[f, rows]
                    gap_b = cols[:, hh + h : hh + h + 1] - cum_t[b, rows]
                    gap = jnp.where(lane < row, gap_f, jnp.where(lane > row, gap_b, 0.0))
                    rf, rb = rate_t[f, rows], rate_t[b, rows]
                    scale = jnp.where(lane < row, rf, jnp.where(lane > row, rb, rf + rb))
                    near = (on * jnp.exp(gap) * scale).astype(BF16)
                    d = 1 - r
                    c = d * hh + h
                    far_rows = slice((1 - r) * blk, (2 - r) * blk)
                    far_row = mid_t[f if d == 0 else b, far_rows]
                    far = (away * shift[:, c : c + 1] * far_row).astype(BF16)
                    parts.append(jnp.concatenate([near, far] if r == 0 else [far, near], axis=1))
            for k in range(tiles):
                xt = xc[p * tiles + k]
                zero = jnp.zeros_like(xt)
                mask = lax.broadcasted_iota(jnp.int32, xt.shape, 1) < HEAD_DIM
                both = jnp.concatenate(
                    [jnp.where(mask, xt, zero), jnp.where(mask, zero, xt)], axis=0
                )
                w = jnp.concatenate([parts[2 * k], parts[2 * k + 1]], axis=1)
                y_ref[p * tiles + k, rows] = jnp.dot(w, both, preferred_element_type=F32)
        return 0

    def zlog_copy(o):
        return remote(
            zsum, zlog.at[cz], zlog_sem.at[0, o], zlog_sem.at[1, cz], z_id(lax.rem(cz + o, nz))
        )

    def lanes_of(log_row, d, k):
        return two(rolled(log_row, me), d * hh + 2 * k)

    def quad_logs():
        for i in range(3):
            _, _, q = member(i)
            remote(
                logs, qlog.at[q], qlog_sem.at[0, i], qlog_sem.at[1, q], partner
            ).wait_recv()
        zsum[...] = qlog[0] + qlog[1] + qlog[2] + qlog[3]
        for o in range(1, nz):
            zlog_copy(o).start()
        zlog[cz] = zsum[...]
        for d in range(2):
            for k in range(tiles):
                each = [lanes_of(qlog[q], d, k) for q in range(4)]
                reach = jnp.zeros_like(each[0])
                for q in reversed(range(4)) if d == 0 else range(4):
                    dec[q, d, k] = jnp.exp(each[q])
                    wup[q, d, k] = jnp.exp(reach)
                    reach = reach + each[q]

    def z_logs():
        for o in range(1, nz):
            s = lax.rem(cz + o, nz)
            remote(
                zsum, zlog.at[s], zlog_sem.at[0, o], zlog_sem.at[1, s], partner
            ).wait_recv()
        reach = [[jnp.zeros((8, 128), F32) for _ in range(2)] for _ in range(rounds)]
        for s in range(nz):
            for r in range(rounds):
                h = 1 << r
                pos = lax.rem(cz, 2 * h)
                middle = cz - pos + h
                f_in = jnp.logical_and(s >= middle, s < cz)
                b_in = jnp.logical_and(s > cz, s < middle)
                reach[r][0] = reach[r][0] + jnp.where(f_in, zlog[s], 0.0)
                reach[r][1] = reach[r][1] + jnp.where(b_in, zlog[s], 0.0)
        for d in range(2):
            for k in range(tiles):
                zdec[d, k] = jnp.exp(lanes_of(zsum[...], d, k))
                for r in range(rounds):
                    zwt[r, d, k] = jnp.exp(lanes_of(reach[r][d], d, k))

    def combine(k):
        for i in range(3):
            _, _, q = member(i)
            remote(
                sup.at[k, q], up_in.at[k, q], up_sem.at[0, k, i], up_sem.at[1, k, q], partner
            ).wait_recv()
        for d in range(2):
            acc = up_in[k, 0, d].astype(F32) * wup[0, d, k, 0:1, :]
            for q in range(1, 4):
                acc = acc + up_in[k, q, d].astype(F32) * wup[q, d, k, 0:1, :]
            tz[k, d] = acc
            zin[k, d] = jnp.zeros_like(acc)

    def z_copy(r, k, o, d):
        return remote(
            zs.at[r, k], zr.at[r, k], zsend_sem.at[r, k, o - 1], zrecv_sem.at[r, k],
            z_id(cz + o if d == 0 else cz - o),
        )

    def z_parts(r):
        h = 1 << r
        pos = lax.rem(cz, 2 * h)
        return h, pos, ((0, pos == h - 1), (1, pos == h))

    def z_send(r, k):
        h, pos, senders = z_parts(r)
        for d, sender in senders:

            @pl.when(sender)
            def _(d=d):
                zs[r, k] = (zin[k, d] * zdec[d, k, 0:1, :] + tz[k, d]).astype(BF16)
                for o in reversed(range(1, h + 1)):
                    z_copy(r, k, o, d).start()

    def z_recv(r, k):
        h, pos, _ = z_parts(r)
        z_copy(r, k, 1, 0).wait_recv()
        for d, receiver in ((0, pos >= h), (1, pos < h)):

            @pl.when(receiver)
            def _(d=d):
                zin[k, d] = zin[k, d] + zr[r, k].astype(F32) * zwt[r, d, k, 0:1, :]

    def down_copy(k, i):
        qy, qx, q = member(i)
        return remote(
            down_out.at[k, q], down_in.at[k, me], down_sem.at[0, k, i], down_sem.at[1, k, me],
            quad_id(qy, qx),
        )

    def down(k):
        for d in range(2):
            g = zin[k, d]
            order = list(range(4)) if d == 0 else list(reversed(range(4)))
            for q in order:
                down_out[k, q, d] = g.astype(BF16)
                if q != order[-1]:
                    g = g * dec[q, d, k, 0:1, :] + up_in[k, q, d].astype(F32)
        for i in range(3):
            down_copy(k, i).start()
        down_in[k, me] = down_out[k, me]

    def gates(group, _):
        for spot in range(4):
            t = group * 4 + spot
            z = in_z[:, pl.ds(pl.multiple_of(t * 128, 128), 128)].astype(F32)
            zg[t] = silu(z)
        return 0

    def gate(mixed, t):
        gated = mixed.astype(F32) * zg[t]
        square = gated * gated
        low = jnp.sum(jnp.where(left, square, 0.0), axis=1, keepdims=True)
        high = jnp.sum(jnp.where(left, 0.0, square), axis=1, keepdims=True)
        mean = jnp.where(left, low, high) * (1.0 / HEAD_DIM)
        scale = lax.rsqrt(mean + 1e-6) * gain_ref[pl.ds(t, 1), :]
        out_ref[:, pl.ds(pl.multiple_of(t * 128, 128), 128)] = (gated * scale).astype(BF16)

    def mix_copy(k):
        return remote(
            mix_out.at[k], mix_in.at[k], mix_sem.at[0, k], mix_sem.at[1, k], partner
        )

    def last(k):
        for i in range(3):
            _, _, q = member(i)
            remote(
                down_out.at[k, q], down_in.at[k, q], down_sem.at[0, k, i], down_sem.at[1, k, q],
                partner,
            ).wait_recv()
        for mine in (False, True):
            rows = pl.ds(pl.multiple_of((core if mine else other) * blk, 128), blk)
            cols = cum_ref[rows, :]
            for p in range(hp):
                rhs = jnp.concatenate([down_in[k, p, 0], down_in[k, p, 1]], axis=1)
                v = jnp.dot(cc[2 * p + k // 2, rows], rhs, preferred_element_type=F32)
                if k == 1:
                    u = jnp.dot(cc[2 * p + 1, rows], rhs, preferred_element_type=F32)
                    v = jnp.where(wide_left(256), v, u)
                head = p * per_pair + 2 * k
                t = p * tiles + k
                y = y_ref[t, rows] + v[:, :128] * two(cols, head) + v[:, 128:] * two(cols, hh + head)
                mixed = y.astype(BF16)
                if mine:
                    gate(mixed, core * tiles_of[0] + t)
                else:
                    mix_out[k, p] = mixed
            if not mine:
                mix_copy(k).start()

    def finish(k):
        mix_copy(k).wait_recv()
        for p in range(hp):
            gate(mix_in[k, p], other * tiles_of[0] + p * tiles + k)

    for spot in range(4):
        work[spot, 0:8, :] = jnp.zeros((8, 128), F32)
        work[spot, 8 + tokens :, :] = jnp.zeros((8, 128), F32)
    low_ref[...] = jnp.zeros_like(low_ref)
    high_ref[...] = jnp.zeros_like(high_ref)
    for i in (1, 0):
        lax.fori_loop(0, tiles_of[i] // 4, functools.partial(conv, i), 0)
    quad_logs()
    for i in (1, 0):
        edge_wait(i)
    for i in (1, 0):
        fix(i)
    first(0)
    first(1)
    first(2)
    lax.fori_loop(0, tiles_of[2] // 4, functools.partial(conv, 2), 0)
    edge_wait(2)
    fix(2)
    z_logs()
    combine(0)
    z_send(0, 0)
    lax.fori_loop(0, 1, inner, 0)
    z_recv(0, 0)
    for r in range(1, rounds):
        z_send(r, 0)
        if r < rounds - 1:
            z_recv(r, 0)
    combine(1)
    z_send(0, 1)
    lax.fori_loop(1, 2, inner, 0)
    z_recv(0, 1)
    for r in range(1, rounds):
        z_send(r, 1)
        if r < rounds - 1:
            z_recv(r, 1)
    combine(2)
    z_send(0, 2)
    if rounds > 1:
        z_recv(rounds - 1, 0)
    down(0)
    lax.fori_loop(2, 3, inner, 0)
    z_recv(0, 2)
    for r in range(1, rounds):
        z_send(r, 2)
        if r < rounds - 1:
            z_recv(r, 2)
    if rounds > 1:
        z_recv(rounds - 1, 1)
    down(1)
    lax.fori_loop(3, hp, inner, 0)
    if rounds > 1:
        z_recv(rounds - 1, 2)
    down(2)
    z_load.wait()
    lax.fori_loop(0, 2 * tiles_of[0] // 4, gates, 0)
    for k in range(3):
        last(k)
        if k > 0:
            finish(k - 1)
    finish(2)

    for x in range(2):

        @pl.when(x * 2 + holder != here)
        def _(x=x):
            for i in range(5):
                param_copy(i, x).wait_send()

    for low, sends in ((True, sends_low), (False, sends_high)):

        @pl.when(sends)
        def _(low=low):
            for i in range(3):
                for k in range(2):
                    edge_copy(i, low, k).wait_send()

    for i in range(3):
        inc_copy(i).wait_send()
        half_copy(i).wait_send()
        qlog_copy(i).wait_send()
    for o in range(1, nz):
        zlog_copy(o).wait_send()
    for k in range(3):
        for i in range(3):
            up_copy(k, i).wait_send()
            down_copy(k, i).wait_send()
        mix_copy(k).wait_send()
        for r in range(rounds):
            h, _, senders = z_parts(r)
            for d, sender in senders:

                @pl.when(sender)
                def _(k=k, r=r, d=d, h=h):
                    for o in range(1, h + 1):
                        z_copy(r, k, o, d).wait_send()


def fits_quad(sp, dp, blk, heads, groups):
    nz = dp // 2
    power = dp % 2 == 0 and nz > 1 and nz & (nz - 1) == 0
    shares = sp == 4 and groups % 4 == 0 and groups // 4 == sp
    return power and shares and blk == 128 and 2 * heads * HEAD_DIM == 3 * groups * 128


def quad_local(sp, dp, x, b, c, z, ahead, back, spike, wx, wb, wc, offset, fading, gain):
    x, b, c, z = x[0], b[0], c[0], z[0]
    blk, x_total = x.shape
    b_total = b.shape[1]
    groups = b_total // STATE
    heads = ahead.shape[2]
    pairs = groups // 2
    nz = dp // 2
    rounds = nz.bit_length() - 1
    tiles = heads // pairs * HEAD_DIM // 128
    hp, hh = pairs // 2, heads // 2
    x_half, b_half = x_total // 2, b_total // 2
    width = x_half + 2 * b_half
    params = (wx, wb, wc, offset, fading)
    vm = pltpu.VMEM
    gains = gain.reshape(x_total // 128, 128)
    scratch = [vm(one.shape, BF16) for one in (x, b, c, z)]
    scratch += [vm((2, 3, hh, blk), F32), vm((3, hh, blk), F32), vm(gains.shape, BF16)]
    scratch += [vm((blk, x_half), BF16), vm((blk, b_half), BF16), vm((blk, b_half), BF16)]
    scratch += [vm(one.shape, one.dtype) for one in params]
    scratch += [vm((2,) + one.shape, one.dtype) for one in params]
    scratch += [vm((EDGE, n), BF16) for n in (x_half, b_half, b_half)] * 2
    scratch += [vm((4, 2 * blk + 16, 128), F32), vm((width // 128, 8, 128), F32)]
    scratch += [vm((8, 128), F32), vm(gains.shape, F32)] + [vm((2 * blk, 128), F32)] * 3
    scratch += [vm((128, 2 * blk), F32)] * 3
    scratch += [vm((x_half // 128, 24, 128), F32)] * 2
    scratch += [vm((2 * hp, 2 * blk, STATE), F32), vm((x_total // 128, blk, 128), F32)]
    scratch += [vm((x_half // 128, 2 * blk, 128), BF16), vm((2 * hp, STATE, 2 * blk), BF16)]
    scratch += [vm((2 * hp, 2 * blk, 128), BF16), vm((x_half // 128, 2 * blk, 128), F32)]
    scratch += [vm((tiles, 4, 2, STATE, 128), BF16)] * 4
    scratch += [vm((8, 128), F32), vm((4, 8, 128), F32), vm((8, 128), F32), vm((nz, 8, 128), F32)]
    scratch += [vm((4, 2, tiles, 8, 128), F32)] * 2 + [vm((2, tiles, 8, 128), F32)]
    scratch += [vm((rounds, 2, tiles, 8, 128), F32)]
    scratch += [vm((tiles, 2, STATE, 128), F32)] * 2 + [vm((rounds, tiles, STATE, 128), BF16)] * 2
    scratch += [vm((tiles, hp, blk, 128), BF16)] * 2
    dma = pltpu.SemaphoreType.DMA
    scratch += [dma((16,)), dma((2, 5, 2)), dma((2, 3, 2)), dma((2, 3)), dma((2, 3))]
    scratch += [dma((2, 4)), dma((2, nz)), dma((2, tiles, 4)), dma((rounds, tiles, nz))]
    scratch += [dma((rounds, tiles)), dma((2, tiles, 4)), dma((2, tiles))]
    out = pl.pallas_call(
        functools.partial(quad_kernel, (heads, pairs, sp, dp)),
        out_shape=pltpu.VMEM((blk, x_total), BF16),
        in_specs=[pl.BlockSpec(memory_space=pltpu.HBM)] * 13,
        out_specs=pl.BlockSpec(memory_space=pltpu.VMEM),
        scratch_shapes=scratch,
        compiler_params=pltpu.CompilerParams(
            collective_id=0, has_side_effects=True, vmem_limit_bytes=60 * 2**20
        ),
        name="mixer",
    )(x, b, c, z, ahead[0].T, back[0].T, spike[0].T, *params, gains)
    return out[None]


def pick(sp, dp, x, b, *rest):
    blk, heads = x.shape[1], rest[2].shape[2]
    if fits_quad(sp, dp, blk, heads, b.shape[2] // STATE):
        return quad_local(sp, dp, x, b, *rest)
    return local(sp, dp, x, b, *rest)


def solution(mesh):
    tokens = P("dp", "sp", None)
    placed = (tokens,) * 7 + (P(None, "sp"),) * 5 + (P(),)
    return jax.shard_map(
        functools.partial(pick, mesh.shape["sp"], mesh.shape["dp"]),
        mesh=mesh,
        in_specs=placed,
        out_specs=tokens,
        check_vma=False,
    )
```

```python
import functools

import jax
import jax.numpy as jnp
from jax import lax
from jax.experimental import pallas as pl
from jax.experimental.pallas import tpu as pltpu
from jax.sharding import PartitionSpec as P

F32 = jnp.float32
BF16 = jnp.bfloat16
HEAD_DIM = 64
STATE = 128
EDGE = 8
HIGHEST = lax.Precision.HIGHEST


def levels_of(sp, dp, groups):
    found = []
    split = 1
    core = 2 if sp % 2 == 0 else 1
    inner = 2 if dp % 2 == 0 and groups % (2 * sp) == 0 else 1
    for axis, count, stride in (("sp", core, 1), ("sp", sp // core, core), ("dp", inner, 1)):
        if count > 1:
            found.append((axis, count, stride))
            split *= count
    return tuple(found), ("dp", dp // inner, inner)


def digit_of(level):
    axis, count, stride = level
    return lax.rem(lax.axis_index(axis) // stride, count)


def member_id(level, member):
    axis, count, stride = level
    return {axis: lax.axis_index(axis) + (member - digit_of(level)) * stride}


def kernel(levels, top, sizes, *refs):
    heads, pairs, chunks, sp, dp = sizes
    (x_ref, b_ref, c_ref, z_ref, ahead_ref, back_ref, spike_ref) = refs[:7]
    params = refs[7:12]
    gain_ref, out_ref = refs[12:14]
    (xc, bc, cc, y_ref, cum_ref, rate_ref, cum_t, rate_t, fac_ref) = refs[14:23]
    refs = refs[:14] + refs[23:]
    got, w_ref, prm_ref, halo_ref, edges, early_sem, edge_sem = (
        refs[14:19], refs[19], refs[20], refs[21], refs[22:28], refs[28], refs[29]
    )
    rest = list(refs[30:])
    depth = len(levels)
    logs = [rest.pop(0) for _ in range(depth + 1)]
    up_log = [rest.pop(0) for _ in range(depth + 1)]
    decay = [rest.pop(0) for _ in range(depth + 1)]
    log_sem = [rest.pop(0) for _ in range(depth + 1)]
    totals, up, down, stage, sems, incoming = ([] for _ in range(6))
    for _ in range(chunks):
        totals.append([rest.pop(0) for _ in range(depth + 1)])
        up.append([rest.pop(0) for _ in range(depth + 1)])
        down.append([rest.pop(0) for _ in range(depth)])
        stage.append([rest.pop(0) for _ in range(depth)])
        sems.append([rest.pop(0) for _ in range(depth + 1)])
        incoming.append(rest.pop(0))
    blk = x_ref.shape[0]
    per_pair = heads // pairs
    x_w = per_pair * HEAD_DIM
    b_w = 2 * STATE
    tiles = x_w // 128
    lane = lax.broadcasted_iota(jnp.int32, (blk, 128), 1)
    left = lane < HEAD_DIM
    row = lax.broadcasted_iota(jnp.int32, (blk, 128), 0)

    segment = ("sp", sp, 1)
    here, there = lax.axis_index("sp"), lax.axis_index("dp")
    rank = there * sp + here
    has_next, has_prev = rank < sp * dp - 1, rank > 0
    after = {"sp": lax.rem(here + 1, sp), "dp": lax.rem(there + (here + 1) // sp, dp)}
    before = {
        "sp": lax.rem(here + sp - 1, sp),
        "dp": lax.rem(there + dp - (sp - here) // sp, dp),
    }
    mesh_id = pl.DeviceIdType.MESH
    barrier = pltpu.get_barrier_semaphore()
    greeted = 0
    for level in levels + (top, segment):
        me = digit_of(level)
        for o in range(1, level[1]):
            target = member_id(level, lax.rem(me + o, level[1]))
            pl.semaphore_signal(barrier, inc=1, device_id=target, device_id_type=mesh_id)
            greeted += 1
    for present, target in ((has_next, after), (has_prev, before)):

        @pl.when(present)
        def _(target=target):
            pl.semaphore_signal(barrier, inc=1, device_id=target, device_id_type=mesh_id)

    filler = jnp.zeros((128 - 2 * heads, blk), F32)
    inc = jnp.concatenate([ahead_ref[...], back_ref[...], filler], axis=0).T
    spikes = jnp.concatenate([spike_ref[...], spike_ref[...], filler], axis=0).T
    count = sp * dp
    neighbours = (rank + count - 1) // count + (2 * count - 2 - rank) // count
    pl.semaphore_wait(barrier, greeted + neighbours)

    def edge_copy(i, direction):
        src = (x_ref, b_ref, c_ref)[i]
        start = blk - EDGE if direction == 0 else 0
        return pltpu.make_async_remote_copy(
            src_ref=src.at[pl.ds(start, EDGE), :],
            dst_ref=edges[3 * direction + i],
            send_sem=edge_sem.at[0, direction, i],
            recv_sem=edge_sem.at[1, direction, i],
            device_id=(after, before)[direction],
            device_id_type=mesh_id,
        )

    def param_copy(i, member, slot):
        return pltpu.make_async_remote_copy(
            src_ref=params[i],
            dst_ref=got[i].at[slot],
            send_sem=early_sem.at[0, i, member],
            recv_sem=early_sem.at[1, i, slot],
            device_id=member_id(segment, member),
            device_id_type=mesh_id,
        )

    for o in range(1, sp):
        for i in range(5):
            param_copy(i, lax.rem(here + o, sp), here).start()
    for direction, present in ((0, has_next), (1, has_prev)):

        @pl.when(present)
        def _(direction=direction):
            for i in range(3):
                edge_copy(i, direction).start()

    for i in range(5):
        got[i][here] = params[i][...]
    for o in range(1, sp):
        for i in range(5):
            s = lax.rem(here + o, sp)
            param_copy(i, s, s).wait_recv()
    prm_ref[...] = jnp.zeros_like(prm_ref)
    wide = got[3].shape[2]
    for q in range(sp):
        for kind in range(2):
            for d in range(2):
                at = slice(d * heads + q * wide, d * heads + (q + 1) * wide)
                prm_ref[kind : kind + 1, at] = got[3 + kind][q, d : d + 1, :]
        off = 0
        for i in range(3):
            n = got[i].shape[2]
            w_ref[0:4, off + q * n : off + (q + 1) * n] = got[i][q].astype(F32)
            off += n * sp
    rate = jax.nn.softplus(inc + prm_ref[0:1, :])
    log_decay = -jnp.exp(prm_ref[1:2, :]) * rate + spikes
    lower = (lane <= row).astype(F32)
    upper = (lane >= row).astype(F32)
    cum_f = jnp.dot(lower, log_decay, precision=HIGHEST, preferred_element_type=F32)
    cum_b = jnp.dot(upper, log_decay, precision=HIGHEST, preferred_element_type=F32)
    cum = jnp.where(lane < heads, cum_f, cum_b)
    lane1 = lane[0:1]
    last = jnp.where(lane1 < heads, cum_f[blk - 1 : blk], cum_b[0:1])
    cum_ref[...] = cum
    rate_ref[...] = rate
    cum_t[...] = cum.T
    rate_t[...] = rate.T
    fac_ref[...] = rate * jnp.exp(last - cum)
    logs[0][...] = jnp.broadcast_to(last, (8, 128))

    def rolled(ref, p):
        return pltpu.roll(ref[...], lax.rem(128 - p * per_pair, 128), 1)

    def two(cols, i):
        return jnp.where(left, cols[:, i : i + 1], cols[:, i + 1 : i + 2])

    def conv(src, col, width, off):
        at = pl.ds(pl.multiple_of(off + col, 128), width)
        v = src[:, pl.ds(pl.multiple_of(col, 128), width)].astype(F32)
        r = lax.broadcasted_iota(jnp.int32, (blk, width), 0)
        h0, h1, h2 = halo_ref[0:1, at], halo_ref[1:2, at], halo_ref[2:3, at]
        m1 = jnp.where(r == 0, h1, pltpu.roll(v, 1, 0))
        m2 = jnp.where(r == 0, h0, jnp.where(r == 1, h1, pltpu.roll(v, 2, 0)))
        p1 = jnp.where(r == blk - 1, h2, pltpu.roll(v, blk - 1, 0))
        s = m2 * w_ref[0:1, at] + m1 * w_ref[1:2, at] + v * w_ref[2:3, at] + p1 * w_ref[3:4, at]
        return (s / (1.0 + jnp.exp(-s))).astype(BF16)

    share = pairs // chunks
    x_total = x_ref.shape[1]
    b_total = b_ref.shape[1]

    def first(c, p, _):
        x_at = pl.ds(pl.multiple_of(p * x_w, 128), x_w)
        b_at = pl.ds(pl.multiple_of(p * b_w, 128), b_w)
        xv = conv(x_ref, p * x_w, x_w, 0)
        bv = conv(b_ref, p * b_w, b_w, x_total)
        xc[:, x_at] = xv
        bc[:, b_at] = bv
        cc[:, b_at] = conv(c_ref, p * b_w, b_w, x_total + b_total)
        cols = rolled(fac_ref, p)
        xf = xv.astype(F32)
        for d in range(2):
            scaled = jnp.concatenate(
                [
                    (xf[:, k * 128 : (k + 1) * 128] * two(cols, d * heads + 2 * k)).astype(BF16)
                    for k in range(tiles)
                ],
                axis=1,
            )
            u = lax.dot_general(scaled, bv, (((0,), (0,)), ((), ())), preferred_element_type=F32)
            half = x_w // 2
            rows = pl.ds(pl.multiple_of((p - c * share) * x_w, 128), x_w)
            totals[c][0][d, rows, :] = jnp.concatenate(
                [u[:half, :STATE], u[half:, STATE:]], axis=0
            ).astype(BF16)
        return 0

    for direction, present in ((0, has_prev), (1, has_next)):

        @pl.when(present)
        def _(direction=direction):
            for i in range(3):
                edge_copy(i, direction).wait_recv()

    off = 0
    for i in range(3):
        n = edges[i].shape[1]
        low = edges[i][...].astype(F32)
        high = edges[3 + i][...].astype(F32)
        halo_ref[0:2, off : off + n] = jnp.where(has_prev, low[EDGE - 2 :], 0.0)
        halo_ref[2:3, off : off + n] = jnp.where(has_next, high[0:1], 0.0)
        off += n
    def inner(p, _):
        x_at = pl.ds(pl.multiple_of(p * x_w, 128), x_w)
        b_at = pl.ds(pl.multiple_of(p * b_w, 128), b_w)
        bv, cv, xv = bc[:, b_at], cc[:, b_at], xc[:, x_at]
        cols = rolled(cum_ref, p)
        parts = []
        for g in range(2):
            scores = lax.dot_general(
                cv[:, g * STATE : (g + 1) * STATE],
                bv[:, g * STATE : (g + 1) * STATE],
                (((1,), (1,)), ((), ())),
                preferred_element_type=F32,
            )
            for i in range(per_pair // 2):
                h = g * (per_pair // 2) + i
                hf = p * per_pair + h
                gap_f = cols[:, h : h + 1] - cum_t[pl.ds(hf, 1), :]
                gap_b = cols[:, heads + h : heads + h + 1] - cum_t[pl.ds(heads + hf, 1), :]
                gap = jnp.where(lane < row, gap_f, jnp.where(lane > row, gap_b, 0.0))
                rf, rb = rate_t[pl.ds(hf, 1), :], rate_t[pl.ds(heads + hf, 1), :]
                scale = jnp.where(lane < row, rf, jnp.where(lane > row, rb, rf + rb))
                parts.append((scores * jnp.exp(gap) * scale).astype(BF16))
        for k in range(tiles):
            xt = xv[:, k * 128 : (k + 1) * 128]
            zero = jnp.zeros_like(xt)
            both = jnp.concatenate([jnp.where(left, xt, zero), jnp.where(left, zero, xt)], axis=0)
            w = jnp.concatenate([parts[2 * k], parts[2 * k + 1]], axis=1)
            y_ref[:, pl.ds(pl.multiple_of(p * x_w + k * 128, 128), 128)] = jnp.dot(
                w, both, preferred_element_type=F32
            )
        return 0

    def copy(src, dst, send, recv, level, member):
        return pltpu.make_async_remote_copy(
            src_ref=src,
            dst_ref=dst,
            send_sem=send,
            recv_sem=recv,
            device_id=member_id(level, member),
            device_id_type=pl.DeviceIdType.MESH,
        )

    every_level = levels + (top,)
    head_share = heads // chunks
    bases = [jnp.int32(0)]
    size = head_share
    for level in levels:
        size = size // level[1]
        bases.append(bases[-1] + digit_of(level) * size)
    pending = [[] for _ in range(chunks)]

    def head_rows(h):
        return pl.ds(pl.multiple_of(h * HEAD_DIM, HEAD_DIM), HEAD_DIM)

    def log_copy(k, member, slot):
        sem = log_sem[k]
        return copy(
            logs[k], up_log[k].at[slot], sem.at[0, member], sem.at[1, slot], every_level[k], member
        )

    def start_up(c, k):
        level = every_level[k]
        n, me = level[1], digit_of(level)
        total, sem = totals[c][k], sems[c][k]
        rows = total.shape[1] // n
        for o in range(1, n):
            m = lax.rem(me + o, n)
            if c == 0:
                pending[c].append(log_copy(k, m, me))
            if k < depth:
                part = total.at[:, pl.ds(pl.multiple_of(m * rows, 64), rows), :]
            else:
                part = total.at[jnp.where(m < me, 1, 0)]
            pending[c].append(
                copy(part, up[c][k].at[me], sem.at[0, m], sem.at[1, me], level, m)
            )
        for one in pending[c]:
            one.start()
        if k < depth:
            up[c][k][me] = total[:, pl.ds(pl.multiple_of(me * rows, 64), rows), :]
        if c == 0:
            up_log[k][me] = logs[k][...]

    def flush(c):
        for one in pending[c]:
            one.wait_send()
        pending[c].clear()

    def finish_up(c, k):
        level = every_level[k]
        n, me = level[1], digit_of(level)
        total, sem = totals[c][k], sems[c][k]
        flush(c)
        for o in range(1, n):
            s = lax.rem(me + o, n)
            if c == 0:
                log_copy(k, s, s).wait_recv()
            part = total.at[:, pl.ds(0, total.shape[1] // n), :] if k < depth else total.at[0]
            copy(part, up[c][k].at[s], sem.at[0, s], sem.at[1, s], level, s).wait_recv()
        if c == 0:

            def expand(m, _):
                decay[k][m] = jnp.exp(jnp.broadcast_to(up_log[k][m][0:1, :], (128, 128)).T)
                return 0

            lax.fori_loop(0, n, expand, 0)
            if k < depth:
                log_sum = up_log[k][0]
                for m in range(1, n):
                    log_sum = log_sum + up_log[k][m]
                logs[k + 1][...] = log_sum

    def gather(c, k):
        n = levels[k][1]
        base = c * head_share + bases[k + 1]
        part, new = up[c][k], totals[c][k + 1]

        def one_head(h, _):
            at = head_rows(h)
            f = part[0, 0, at, :].astype(F32)
            b = part[n - 1, 1, at, :].astype(F32)
            for m in range(1, n):
                r = n - 1 - m
                f = f * decay[k][m, pl.ds(base + h, 1), :] + part[m, 0, at, :].astype(F32)
                b = b * decay[k][r, pl.ds(heads + base + h, 1), :] + part[r, 1, at, :].astype(F32)
            new[0, at, :] = f.astype(BF16)
            new[1, at, :] = b.astype(BF16)
            return 0

        lax.fori_loop(0, new.shape[1] // HEAD_DIM, one_head, 0)

    def enter(c):
        n, me = top[1], digit_of(top)
        base = c * head_share + bases[-1]
        into = incoming[c]
        into[...] = jnp.zeros_like(into)

        def carry(s, d):
            def one_head(h, _):
                at = head_rows(h)
                factor = decay[depth][s, pl.ds(d * heads + base + h, 1), :]
                into[d, at, :] = into[d, at, :] * factor + up[c][depth][s, at, :].astype(F32)
                return 0

            lax.fori_loop(0, into.shape[1] // HEAD_DIM, one_head, 0)
            return 0

        lax.fori_loop(0, me, lambda s, _: carry(s, 0), 0)
        lax.fori_loop(0, n - 1 - me, lambda i, _: carry(n - 1 - i, 1), 0)

    def start_down(c, k):
        level = levels[k]
        n, me = level[1], digit_of(level)
        sem = sems[c][k]
        rows = totals[c][k].shape[1] // n
        base = c * head_share + bases[k + 1]
        source = incoming[c] if k == depth - 1 else down[c][k + 1]
        part, out = up[c][k], stage[c][k]

        def spread(h, _):
            at = head_rows(h)
            f = source[0, at, :].astype(F32)
            b = source[1, at, :].astype(F32)
            for m in range(n):
                r = n - 1 - m
                out[m, 0, at, :] = f.astype(BF16)
                out[r, 1, at, :] = b.astype(BF16)
                if m < n - 1:
                    f = f * decay[k][m, pl.ds(base + h, 1), :] + part[m, 0, at, :].astype(F32)
                    down_factor = decay[k][r, pl.ds(heads + base + h, 1), :]
                    b = b * down_factor + part[r, 1, at, :].astype(F32)
            return 0

        lax.fori_loop(0, rows // HEAD_DIM, spread, 0)
        mine = pl.ds(pl.multiple_of(me * rows, 64), rows)
        for o in range(1, n):
            m = lax.rem(me + o, n)
            pending[c].append(
                copy(out.at[m], down[c][k].at[:, mine, :], sem.at[2, m], sem.at[3, me], level, m)
            )
        for one in pending[c]:
            one.start()
        down[c][k][:, mine, :] = out[me]

    def finish_down(c, k):
        level = levels[k]
        n, me = level[1], digit_of(level)
        sem = sems[c][k]
        rows = totals[c][k].shape[1] // n
        flush(c)
        for o in range(1, n):
            s = lax.rem(me + o, n)
            theirs = pl.ds(pl.multiple_of(s * rows, 64), rows)
            copy(
                stage[c][k].at[s], down[c][k].at[:, theirs, :], sem.at[2, s], sem.at[3, s], level, s
            ).wait_recv()

    for c in range(chunks):
        lax.fori_loop(c * share, (c + 1) * share, functools.partial(first, c), 0)
        start_up(c, 0)
    for o in range(1, sp):
        for i in range(5):
            param_copy(i, lax.rem(here + o, sp), here).wait_send()
    for direction, present in ((0, has_next), (1, has_prev)):

        @pl.when(present)
        def _(direction=direction):
            for i in range(3):
                edge_copy(i, direction).wait_send()


    gaps = chunks * depth
    cuts = [(i * pairs) // gaps for i in range(gaps + 1)]
    for k in range(depth):
        for c in range(chunks):
            finish_up(c, k)
            gather(c, k)
            start_up(c, k + 1)
            at = k * chunks + c
            lax.fori_loop(cuts[at], cuts[at + 1], inner, 0)
    for c in range(chunks):
        finish_up(c, depth)
        enter(c)
        start_down(c, depth - 1)
    for k in reversed(range(1, depth)):
        for c in range(chunks):
            finish_down(c, k)
            start_down(c, k - 1)

    cum_ref[...] = jnp.exp(cum_ref[...])

    def last_part(c, p, _):
        cv = cc[:, pl.ds(pl.multiple_of(p * b_w, 128), b_w)]
        cols = rolled(cum_ref, p)
        carried = []
        for d in range(2):
            st = down[c][0][d, pl.ds(pl.multiple_of((p - c * share) * x_w, 128), x_w), :]
            got = [
                lax.dot_general(
                    cv[:, g * STATE : (g + 1) * STATE],
                    st,
                    (((1,), (1,)), ((), ())),
                    preferred_element_type=F32,
                )
                for g in range(2)
            ]
            carried.append(got)
        for k in range(tiles):
            cut = slice(k * 128, (k + 1) * 128)
            at = pl.ds(pl.multiple_of(p * x_w + k * 128, 128), 128)
            y = y_ref[:, at]
            for d in range(2):
                a, b = carried[d][0][:, cut], carried[d][1][:, cut]
                if 2 * k + 1 < per_pair // 2:
                    v = a
                elif 2 * k >= per_pair // 2:
                    v = b
                else:
                    v = jnp.where(left, a, b)
                y = y + v * two(cols, d * heads + 2 * k)
            z = z_ref[:, at].astype(F32)
            gated = y.astype(BF16).astype(F32) * (z / (1.0 + jnp.exp(-z)))
            square = gated * gated
            low = jnp.sum(jnp.where(left, square, 0.0), axis=1, keepdims=True)
            high = jnp.sum(jnp.where(left, 0.0, square), axis=1, keepdims=True)
            mean = jnp.where(left, low, high) * (1.0 / HEAD_DIM)
            out_ref[:, at] = (gated * lax.rsqrt(mean + 1e-6) * gain_ref[0:1, at]).astype(BF16)
        return 0

    for c in range(chunks):
        finish_down(c, 0)
        lax.fori_loop(c * share, (c + 1) * share, functools.partial(last_part, c), 0)


def local(sp, dp, x, b, c, z, ahead, back, spike, wx, wb, wc, offset, fading, gain):
    x, b, c, z = x[0], b[0], c[0], z[0]
    blk, x_total = x.shape
    groups = b.shape[1] // STATE
    heads = ahead.shape[2]
    pairs = groups // 2
    levels, top = levels_of(sp, dp, groups)
    scratch = [
        pltpu.VMEM((blk, x_total), BF16),
        pltpu.VMEM((blk, groups * STATE), BF16),
        pltpu.VMEM((blk, groups * STATE), BF16),
        pltpu.VMEM((blk, x_total), F32),
    ]
    scratch += [pltpu.VMEM((128, 128), F32)] * 5
    params = (wx, wb, wc, offset, fading)
    width = x_total + 2 * b.shape[1]
    early = [pltpu.VMEM((sp,) + one.shape, one.dtype) for one in params]
    early += [pltpu.VMEM((8, width), F32), pltpu.VMEM((8, 128), F32), pltpu.VMEM((8, width), F32)]
    early += [pltpu.VMEM((EDGE, one.shape[1]), BF16) for one in (x, b, c)] * 2
    early += [pltpu.SemaphoreType.DMA((2, 5, sp)), pltpu.SemaphoreType.DMA((2, 2, 3))]
    scratch += early
    split = 1
    for level in levels:
        split *= level[1]
    chunks = 2 if groups % (2 * split) == 0 else 1
    counts = [level[1] for level in levels] + [top[1]]
    scratch += [pltpu.VMEM((8, 128), F32)] * len(counts)
    scratch += [pltpu.VMEM((n, 8, 128), F32) for n in counts]
    scratch += [pltpu.VMEM((n, 128, 128), F32) for n in counts]
    scratch += [pltpu.SemaphoreType.DMA((2, n)) for n in counts]
    for _ in range(chunks):
        held = [x_total // chunks]
        for n in counts[:-1]:
            held.append(held[-1] // n)
        slabs = list(zip(counts[:-1], held[1:]))
        scratch += [pltpu.VMEM((2, rows, STATE), BF16) for rows in held]
        scratch += [pltpu.VMEM((n, 2, rows, STATE), BF16) for n, rows in slabs]
        scratch += [pltpu.VMEM((counts[-1], held[-1], STATE), BF16)]
        scratch += [pltpu.VMEM((2, rows, STATE), BF16) for rows in held[:-1]]
        scratch += [pltpu.VMEM((n, 2, rows, STATE), BF16) for n, rows in slabs]
        scratch += [pltpu.SemaphoreType.DMA((4, n)) for n in counts]
        scratch += [pltpu.VMEM((2, held[-1], STATE), F32)]
    out = pl.pallas_call(
        functools.partial(kernel, levels, top, (heads, pairs, chunks, sp, dp)),
        out_shape=jax.ShapeDtypeStruct((blk, x_total), BF16),
        in_specs=[pl.BlockSpec(memory_space=pltpu.VMEM)] * 13,
        out_specs=pl.BlockSpec(memory_space=pltpu.VMEM),
        scratch_shapes=scratch,
        compiler_params=pltpu.CompilerParams(
            collective_id=0, has_side_effects=True, vmem_limit_bytes=60 * 2**20
        ),
        name="mixer",
    )(x, b, c, z, ahead[0].T, back[0].T, spike[0].T, *params, gain.astype(F32)[None])
    return out[None]


def quad_kernel(sizes, *refs):
    heads, pairs, sp, dp = sizes
    nz = dp // 2
    rounds = nz.bit_length() - 1
    (x_hbm, b_hbm, c_hbm, z_hbm, ahead_hbm, back_hbm, spike_hbm) = refs[:7]
    params = refs[7:12]
    gain_hbm, out_ref = refs[12:14]
    (in_x, in_b, in_c, in_z, inc, inc_out, gain_in, px, pb, pc) = refs[14:24]
    own, got = refs[24:29], refs[29:34]
    edge_out, low_in, high_in = refs[34:37]
    refs = refs[:37] + (None,) * 3 + refs[37:]
    (work, w_ref, prm_ref, gain_ref, cum_ref, fac_ref, col_ref, cum_t, rate_t, mid_t) = refs[40:50]
    low_ref, high_ref, bc, zg, wide_cum = refs[50:55]
    refs = refs[:50] + refs[55:]
    (xc, bt, cc, y_ref, sup, up_in, down_out, down_in) = refs[50:58]
    (logs, qlog, zsum, zlog, dec, wup, zdec, zwt) = refs[58:66]
    (tz, zin, zs, zr, mix_out, mix_in) = refs[66:72]
    (load_sem, prm_sem, edge_sem, half_sem, inc_sem, qlog_sem, zlog_sem) = refs[72:79]
    (up_sem, zsend_sem, zrecv_sem, down_sem, mix_sem) = refs[79:84]

    hh = heads // 2
    hp = pairs // 2
    per_pair = heads // pairs
    tiles = per_pair * HEAD_DIM // 128
    blk = in_x.shape[0]
    tokens = 2 * blk
    x_half = in_x.shape[1] // 2
    b_half = in_b.shape[1] // 2
    x_w = per_pair * HEAD_DIM
    mesh_id = pl.DeviceIdType.MESH

    here, there = lax.axis_index("sp"), lax.axis_index("dp")
    core, cx = lax.rem(here, 2), here // 2
    cy, cz = lax.rem(there, 2), there // 2
    other = 1 - core
    me = cy * 2 + cx
    chip = there * 2 + cx
    chips = dp * 2
    has_next, has_prev = chip < chips - 1, chip > 0
    after, before = lax.rem(chip + 1, chips), lax.rem(chip + chips - 1, chips)
    partner = {"sp": cx * 2 + other}

    def chip_id(c, k):
        return {"sp": lax.rem(c, 2) * 2 + k, "dp": c // 2}

    def quad_id(qy, qx):
        return {"sp": qx * 2 + core, "dp": cz * 2 + qy}

    def z_id(z):
        return {"dp": z * 2 + cy}

    def member(i):
        qy = lax.rem(cy + lax.rem(i + 1, 2), 2)
        qx = lax.rem(cx + (3 - i) // 2, 2)
        return qy, qx, qy * 2 + qx

    def remote(src, dst, send, recv, target):
        return pltpu.make_async_remote_copy(
            src_ref=src, dst_ref=dst, send_sem=send, recv_sem=recv,
            device_id=target, device_id_type=mesh_id,
        )

    barrier = pltpu.get_barrier_semaphore()

    def greet(target):
        pl.semaphore_signal(barrier, inc=1, device_id=target, device_id_type=mesh_id)

    for o in range(1, sp):
        greet({"sp": lax.rem(here + o, sp)})
    for i in range(3):
        qy, qx, _ = member(i)
        greet(quad_id(qy, qx))
    for o in range(1, nz):
        greet(z_id(lax.rem(cz + o, nz)))
    for present, neighbour in ((has_next, after), (has_prev, before)):

        @pl.when(present)
        def _(neighbour=neighbour):
            for k in range(2):
                greet(chip_id(neighbour, k))

    loads = []

    def load(src, dst):
        one = pltpu.make_async_copy(src, dst, load_sem.at[len(loads)])
        one.start()
        loads.append(one)
        return one

    param_loads = [load(params[i], own[i]) for i in range(5)]
    mine = pl.ds(pl.multiple_of(core * hh, 8), hh)
    theirs = pl.ds(pl.multiple_of(other * hh, 8), hh)
    raw = (ahead_hbm, back_hbm, spike_hbm)
    inc_stage = [load(raw[i].at[theirs, :], inc_out.at[i]) for i in range(3)]
    inc_loads = [load(raw[i].at[mine, :], inc.at[core, i]) for i in range(3)]
    b_load = load(b_hbm, in_b)
    x_load = load(x_hbm, in_x)
    c_load = load(c_hbm, in_c)
    gain_load = load(gain_hbm, gain_in)
    z_load = load(z_hbm, in_z)

    for one in param_loads + inc_stage:
        one.wait()
    chip_greets = 2 * ((chip + chips - 1) // chips + (2 * chips - 2 - chip) // chips)
    pl.semaphore_wait(barrier, (sp - 1) + 3 + (nz - 1) + chip_greets)

    holder = here // 2
    slot = lax.rem(here, 2)

    def param_copy(i, x):
        return remote(
            own[i], got[i].at[slot], prm_sem.at[0, i, x], prm_sem.at[1, i, slot],
            {"sp": x * 2 + holder},
        )

    for x in range(2):
        elsewhere = x * 2 + holder != here

        @pl.when(elsewhere)
        def _(x=x):
            for i in range(5):
                param_copy(i, x).start()

        @pl.when(jnp.logical_not(elsewhere))
        def _():
            for i in range(5):
                got[i][slot] = own[i][...]

    def inc_copy(i):
        return remote(
            inc_out.at[i], inc.at[core, i], inc_sem.at[0, i], inc_sem.at[1, i], partner
        )

    for i in range(3):
        inc_copy(i).start()

    sources = (in_x, in_b, in_c)
    halves = (x_half, b_half, b_half)

    edge_from = (0, x_half // 128, (x_half + b_half) // 128)

    def edge_copy(low, k):
        return remote(
            edge_out.at[k], low_in if low else high_in, edge_sem.at[0, k],
            edge_sem.at[1, 0 if low else 1], chip_id(after if low else before, k),
        )

    sends_low = jnp.logical_and(core == 1, has_next)
    sends_high = jnp.logical_and(core == 0, has_prev)

    def half_copy(i):
        cut = pl.ds(pl.multiple_of(other * halves[i], 128), halves[i])
        return remote(
            sources[i].at[:, cut], (px, pb, pc)[i], half_sem.at[0, i], half_sem.at[1, i], partner
        )

    for one in (b_load, x_load, c_load):
        one.wait()
    slab = edge_out.shape[2]
    for k in range(2):
        picked = [[], []]
        for i in range(3):
            for t in range(halves[i] // 128):
                at = slice(k * halves[i] + t * 128, k * halves[i] + (t + 1) * 128)
                end = sources[i][blk - EDGE :, at].astype(F32)[EDGE - 2 :]
                start = sources[i][0:EDGE, at].astype(F32)[0:2]
                both = jnp.where(core == 1, end, start)
                for r in range(2):
                    picked[r].append(both[r : r + 1])
        for r in range(2):
            spare = jnp.zeros((slab - len(picked[r]), 128), F32)
            edge_out[k, r] = jnp.concatenate(picked[r] + [spare], axis=0).astype(BF16)
    for low, sends in ((True, sends_low), (False, sends_high)):

        @pl.when(sends)
        def _(low=low):
            for k in range(2):
                edge_copy(low, k).start()

    for i in (1, 0):
        half_copy(i).start()

    lane = lax.broadcasted_iota(jnp.int32, (blk, 128), 1)
    row = lax.broadcasted_iota(jnp.int32, (blk, 128), 0)
    left = lane < HEAD_DIM
    left1 = left[0:1]
    lower = (lane <= row).astype(F32)
    upper = (lane >= row).astype(F32)
    filler = jnp.zeros((128 - 2 * hh, blk), F32)

    for q in range(2):
        from_q = 2 * core + q != here

        @pl.when(from_q)
        def _(q=q):
            for i in range(5):
                remote(
                    own[i], got[i].at[q], prm_sem.at[0, i, 0], prm_sem.at[1, i, q], partner
                ).wait_recv()

    for one in inc_loads:
        one.wait()
    for i in range(3):
        remote(
            inc_out.at[i], inc.at[other, i], inc_sem.at[0, i], inc_sem.at[1, i], partner
        ).wait_recv()
    prm_ref[...] = jnp.zeros_like(prm_ref)
    wide = own[3].shape[1]
    for q in range(2):
        for kind in range(2):
            for d in range(2):
                at = slice(d * hh + q * wide, d * hh + (q + 1) * wide)
                prm_ref[kind : kind + 1, at] = got[3 + kind][q, d : d + 1, :]
        off = 0
        for i in range(3):
            n = own[i].shape[1]
            part = got[i][q].astype(F32)
            for t in range(n // 128):
                w_ref[off + q * (n // 128) + t, 0:4, :] = part[:, t * 128 : (t + 1) * 128]
            off += 2 * n // 128

    cums, rates = [], []
    for j in range(2):
        pre = jnp.concatenate([inc[j, 0], inc[j, 1], filler], axis=0).T
        spikes = jnp.concatenate([inc[j, 2], inc[j, 2], filler], axis=0).T
        rate = jax.nn.softplus(pre + prm_ref[0:1, :])
        log_decay = -jnp.exp(prm_ref[1:2, :]) * rate + spikes
        cum_f = jnp.dot(lower, log_decay, precision=HIGHEST, preferred_element_type=F32)
        cum_b = jnp.dot(upper, log_decay, precision=HIGHEST, preferred_element_type=F32)
        cums.append((cum_f, cum_b))
        rates.append(rate)
    ahead_lane = lane < hh
    ahead1 = ahead_lane[0:1]
    mid_f, mid_b = cums[0][0][blk - 1 : blk], cums[1][1][0:1]
    total = jnp.where(ahead1, mid_f + cums[1][0][blk - 1 : blk], cums[0][1][0:1] + mid_b)
    logs[...] = jnp.broadcast_to(total, (8, 128))

    def qlog_copy(i):
        qy, qx, q = member(i)
        return remote(
            logs, qlog.at[me], qlog_sem.at[0, i], qlog_sem.at[1, me], quad_id(qy, qx)
        )

    for i in range(3):
        qlog_copy(i).start()
    qlog[me] = logs[...]
    for j in range(2):
        cum_f, cum_b = cums[j]
        far = jnp.where(ahead_lane, mid_f if j == 1 else 0.0, mid_b if j == 0 else 0.0)
        near = jnp.where(ahead_lane, cum_f, cum_b)
        at = slice(j * blk, (j + 1) * blk)
        cum = near + far
        cum_ref[at, :] = jnp.exp(cum)
        fac_ref[at, :] = rates[j] * jnp.exp(total - cum)
        col_ref[at, :] = cum
        cum_t[:, at] = cum.T
        rate_t[:, at] = rates[j].T
        mid = rates[j] * jnp.exp(jnp.minimum((mid_f if j == 0 else mid_b) - near, 0.0))
        mid_t[:, at] = mid.T

    gain_load.wait()
    gain_ref[...] = gain_in[...].astype(F32)

    def half_wait(i):
        remote(
            sources[i].at[:, pl.ds(0, halves[i])], (px, pb, pc)[i], half_sem.at[0, i],
            half_sem.at[1, i], partner,
        ).wait_recv()

    def rolled(v, p):
        return pltpu.roll(v, lax.rem(128 - p * per_pair, 128), 1)

    def two(cols, i):
        mask = lax.broadcasted_iota(jnp.int32, (cols.shape[0], 128), 1) < HEAD_DIM
        return jnp.where(mask, cols[:, i : i + 1], cols[:, i + 1 : i + 2])

    tiles_of = [half // 128 for half in halves]
    starts = (0, tiles_of[0], tiles_of[0] + tiles_of[1])

    def silu(s):
        h = 0.5 * s
        return h + h * jnp.tanh(h)

    def store(i, t, rows, v):
        if i == 1:
            bc[t, rows, :] = v
        else:
            (xc, None, cc)[i][t, rows, :] = v.astype(BF16)

    def conv(i, k, base):
        for p in range(hp):
            t = p * (tiles_of[i] // hp) + k
            spot = base + p
            mine_at = pl.ds(pl.multiple_of(core * halves[i] + t * 128, 128), 128)
            at = pl.ds(pl.multiple_of(t * 128, 128), 128)
            buf = work.at[spot]
            here_at = pl.ds(pl.multiple_of(8 + core * blk, 8), blk)
            there_at = pl.ds(pl.multiple_of(8 + other * blk, 8), blk)
            buf[here_at, :] = sources[i][:, mine_at].astype(F32)
            buf[there_at, :] = (px, pb, pc)[i][:, at].astype(F32)
            s = buf[6 : 6 + tokens, :] * w_ref[starts[i] + t, 0:1, :]
            for tap in range(1, 4):
                near = buf[6 + tap : 6 + tap + tokens, :]
                s = s + near * w_ref[starts[i] + t, tap : tap + 1, :]
            store(i, t, slice(0, tokens), silu(s))

    def edge_wait():
        for low, present in ((True, has_prev), (False, has_next)):

            @pl.when(present)
            def _(low=low):
                edge_copy(low, 0).wait_recv()

    def fix(i, k):
        half = halves[i]
        mine_tiles = [p * (tiles_of[i] // hp) + k for p in range(hp)]
        row16 = row[0:16]
        lows = [low_in[r].astype(F32) for r in range(2)]
        highs = high_in[0].astype(F32)
        own_part = sources[i]
        their_part = (px, pb, pc)[i]
        for t in mine_tiles:
            mine_at = pl.ds(pl.multiple_of(core * half + t * 128, 128), 128)
            at = slice(t * 128, (t + 1) * 128)
            start = jnp.where(core == 0, own_part[0:8, mine_at], their_part[0:8, at])
            end = jnp.where(core == 1, own_part[blk - 8 :, mine_at], their_part[blk - 8 :, at])
            e = edge_from[i] + t
            for r in range(2):
                before_row = jnp.where(has_prev, lows[r][e : e + 1], 0.0)
                low_ref[t, 6 + r : 7 + r, :] = before_row
            low_ref[t, 8:16, :] = start.astype(F32)
            high_ref[t, 8:16, :] = end.astype(F32)
            high_ref[t, 16:17, :] = jnp.where(has_next, highs[e : e + 1], 0.0)
        dst = (xc, bc, cc)[i]
        for t in mine_tiles:
            for ref, low in ((low_ref, True), (high_ref, False)):
                s = ref[t, 6:14, :] * w_ref[starts[i] + t, 0:1, :]
                for k in range(1, 4):
                    s = s + ref[t, 6 + k : 14 + k, :] * w_ref[starts[i] + t, k : k + 1, :]
                s = silu(s)
                rows = slice(0, 16) if low else slice(tokens - 16, tokens)
                s = jnp.concatenate([s, s], axis=0)
                keep = row16 >= 2 if low else row16 < 15
                store(i, t, rows, jnp.where(keep, dst[t, rows, :].astype(F32), s))

    def up_copy(k, d, i):
        qy, qx, q = member(i)
        return remote(
            sup.at[k, q, d], up_in.at[k, me, d], up_sem.at[0, 2 * k + d, i],
            up_sem.at[1, 2 * k + d, me], quad_id(qy, qx),
        )

    def wide_left(n):
        return lax.rem(lax.broadcasted_iota(jnp.int32, (128, n), 1), 128) < HEAD_DIM

    def first(k):
        for p in range(hp):
            if k < 2:
                bt[2 * p + k] = bc[2 * p + k].T.astype(BF16)
            xf = xc[p * tiles + k].astype(F32)
            rhs = jnp.concatenate(
                [(xf * wide_cum[k, p, d]).astype(BF16) for d in range(2)], axis=1
            )
            u = jnp.dot(bt[2 * p + k // 2], rhs, preferred_element_type=F32)
            if k == 1:
                v = jnp.dot(bt[2 * p + 1], rhs, preferred_element_type=F32)
                u = jnp.where(wide_left(256), u, v)
            u = u.astype(BF16)
            sup[k, p, 0] = u[:, :128]
            sup[k, p, 1] = u[:, 128:]
        for d in range(2):
            for i in range(3):
                up_copy(k, d, i).start()
        up_in[k, me] = sup[k, me]

    def inner(p, r):
        rows = slice(r * blk, (r + 1) * blk)
        cols = rolled(col_ref[rows, :], p)
        mid_row = mid_f if r == 1 else mid_b
        shift = rolled(jnp.exp(jnp.minimum(col_ref[rows, :] - mid_row, 0.0)), p)
        parts = []
        for g in range(2):
            scores = jnp.dot(cc[2 * p + g, rows], bt[2 * p + g], preferred_element_type=F32)
            on = scores[:, r * blk : (r + 1) * blk]
            away = scores[:, (1 - r) * blk : (2 - r) * blk]
            for h in range(g * per_pair // 2, (g + 1) * per_pair // 2):
                f = pl.ds(p * per_pair + h, 1)
                b = pl.ds(hh + p * per_pair + h, 1)
                gap_f = cols[:, h : h + 1] - cum_t[f, rows]
                gap_b = cols[:, hh + h : hh + h + 1] - cum_t[b, rows]
                gap = jnp.where(lane < row, gap_f, jnp.where(lane > row, gap_b, 0.0))
                rf, rb = rate_t[f, rows], rate_t[b, rows]
                scale = jnp.where(lane < row, rf, jnp.where(lane > row, rb, rf + rb))
                near = (on * jnp.exp(gap) * scale).astype(BF16)
                d = 1 - r
                c = d * hh + h
                far_rows = slice((1 - r) * blk, (2 - r) * blk)
                far_row = mid_t[f if d == 0 else b, far_rows]
                far = (away * shift[:, c : c + 1] * far_row).astype(BF16)
                parts.append(jnp.concatenate([near, far] if r == 0 else [far, near], axis=1))
        for k in range(tiles):
            xt = xc[p * tiles + k]
            zero = jnp.zeros_like(xt)
            mask = lax.broadcasted_iota(jnp.int32, xt.shape, 1) < HEAD_DIM
            both = jnp.concatenate(
                [jnp.where(mask, xt, zero), jnp.where(mask, zero, xt)], axis=0
            )
            w = jnp.concatenate([parts[2 * k], parts[2 * k + 1]], axis=1)
            y_ref[p * tiles + k, rows] = jnp.dot(w, both, preferred_element_type=F32)

    def zlog_copy(o):
        return remote(
            zsum, zlog.at[cz], zlog_sem.at[0, o], zlog_sem.at[1, cz], z_id(lax.rem(cz + o, nz))
        )

    def lanes_of(log_row, d, k):
        return two(rolled(log_row, me), d * hh + 2 * k)

    def quad_logs():
        for i in range(3):
            _, _, q = member(i)
            remote(
                logs, qlog.at[q], qlog_sem.at[0, i], qlog_sem.at[1, q], partner
            ).wait_recv()
        zsum[...] = qlog[0] + qlog[1] + qlog[2] + qlog[3]
        for o in range(1, nz):
            zlog_copy(o).start()
        zlog[cz] = zsum[...]
        for d in range(2):
            for k in range(tiles):
                zdec[d, k] = jnp.exp(lanes_of(zsum[...], d, k))
                each = [lanes_of(qlog[q], d, k) for q in range(4)]
                reach = jnp.zeros_like(each[0])
                for q in reversed(range(4)) if d == 0 else range(4):
                    dec[q, d, k] = jnp.exp(each[q])
                    wup[q, d, k] = jnp.exp(reach)
                    reach = reach + each[q]

    def z_logs():
        for o in range(1, nz):
            s = lax.rem(cz + o, nz)
            remote(
                zsum, zlog.at[s], zlog_sem.at[0, o], zlog_sem.at[1, s], partner
            ).wait_recv()
        reach = [[jnp.zeros((8, 128), F32) for _ in range(2)] for _ in range(rounds)]
        for s in range(nz):
            for r in range(rounds):
                h = 1 << r
                pos = lax.rem(cz, 2 * h)
                middle = cz - pos + h
                f_in = jnp.logical_and(s >= middle, s < cz)
                b_in = jnp.logical_and(s > cz, s < middle)
                reach[r][0] = reach[r][0] + jnp.where(f_in, zlog[s], 0.0)
                reach[r][1] = reach[r][1] + jnp.where(b_in, zlog[s], 0.0)
        for d in range(2):
            for k in range(tiles):
                for r in range(rounds):
                    zwt[r, d, k] = jnp.exp(lanes_of(reach[r][d], d, k))

    def combine(k, d):
        for i in range(3):
            _, _, q = member(i)
            remote(
                sup.at[k, q, d], up_in.at[k, q, d], up_sem.at[0, 2 * k + d, i],
                up_sem.at[1, 2 * k + d, q], partner,
            ).wait_recv()
        acc = up_in[k, 0, d].astype(F32) * wup[0, d, k, 0:1, :]
        for q in range(1, 4):
            acc = acc + up_in[k, q, d].astype(F32) * wup[q, d, k, 0:1, :]
        tz[k, d] = acc
        zin[k, d] = jnp.zeros_like(acc)
        z_send(0, k, d)

    def z_copy(r, k, o, d):
        return remote(
            zs.at[r, k], zr.at[r, k], zsend_sem.at[r, k, o - 1], zrecv_sem.at[r, k],
            z_id(cz + o if d == 0 else cz - o),
        )

    def z_parts(r):
        h = 1 << r
        pos = lax.rem(cz, 2 * h)
        return h, pos, ((0, pos == h - 1), (1, pos == h))

    def z_send(r, k, d):
        h, _, senders = z_parts(r)

        @pl.when(senders[d][1])
        def _():
            zs[r, k] = (zin[k, d] * zdec[d, k, 0:1, :] + tz[k, d]).astype(BF16)
            for o in reversed(range(1, h + 1)):
                z_copy(r, k, o, d).start()

    def z_recv(r, k, d):
        h, pos, _ = z_parts(r)

        @pl.when(pos >= h if d == 0 else pos < h)
        def _():
            remote(
                zs.at[r, k], zr.at[r, k], zsend_sem.at[r, k, 0], zrecv_sem.at[r, k], partner
            ).wait_recv()
            zin[k, d] = zin[k, d] + zr[r, k].astype(F32) * zwt[r, d, k, 0:1, :]

        if r + 1 < rounds:
            z_send(r + 1, k, d)
        else:
            down(k, d)

    def down_copy(k, d, i):
        qy, qx, q = member(i)
        return remote(
            down_out.at[k, q, d], down_in.at[k, me, d], down_sem.at[0, 2 * k + d, i],
            down_sem.at[1, 2 * k + d, me], quad_id(qy, qx),
        )

    def down(k, d):
        g = zin[k, d]
        order = list(range(4)) if d == 0 else list(reversed(range(4)))
        for q in order:
            down_out[k, q, d] = g.astype(BF16)
            if q != order[-1]:
                g = g * dec[q, d, k, 0:1, :] + up_in[k, q, d].astype(F32)
        for i in range(3):
            down_copy(k, d, i).start()
        down_in[k, me, d] = down_out[k, me, d]

    def gates(group, _):
        for spot in range(4):
            t = group * 4 + spot
            z = in_z[:, pl.ds(pl.multiple_of(t * 128, 128), 128)].astype(F32)
            zg[t] = silu(z)
        return 0

    def gate(mixed, t):
        gated = mixed.astype(F32) * zg[t]
        square = gated * gated
        low = jnp.sum(jnp.where(left, square, 0.0), axis=1, keepdims=True)
        high = jnp.sum(jnp.where(left, 0.0, square), axis=1, keepdims=True)
        mean = jnp.where(left, low, high) * (1.0 / HEAD_DIM)
        scale = lax.rsqrt(mean + 1e-6) * gain_ref[pl.ds(t, 1), :]
        out_ref[:, pl.ds(pl.multiple_of(t * 128, 128), 128)] = (gated * scale).astype(BF16)

    def mix_copy(k):
        return remote(
            mix_out.at[k], mix_in.at[k], mix_sem.at[0, k], mix_sem.at[1, k], partner
        )

    def spread(k, ref=cum_ref):
        for j in range(2):
            cols = ref[j * blk : (j + 1) * blk, :]
            for p in range(hp):
                head = p * per_pair + 2 * k
                for d in range(2):
                    wide_cum[k, p, d, j * blk : (j + 1) * blk, :] = two(cols, d * hh + head)

    def last(k):
        for i in range(3):
            _, _, q = member(i)
            for d in range(2):
                remote(
                    down_out.at[k, q, d], down_in.at[k, q, d], down_sem.at[0, 2 * k + d, i],
                    down_sem.at[1, 2 * k + d, q], partner,
                ).wait_recv()
        for mine in (False, True):
            rows = pl.ds(pl.multiple_of((core if mine else other) * blk, 128), blk)
            for p in range(hp):
                rhs = jnp.concatenate([down_in[k, p, 0], down_in[k, p, 1]], axis=1)
                v = jnp.dot(cc[2 * p + k // 2, rows], rhs, preferred_element_type=F32)
                if k == 1:
                    u = jnp.dot(cc[2 * p + 1, rows], rhs, preferred_element_type=F32)
                    v = jnp.where(wide_left(256), v, u)
                t = p * tiles + k
                y = y_ref[t, rows] + v[:, :128] * wide_cum[k, p, 0, rows]
                y = y + v[:, 128:] * wide_cum[k, p, 1, rows]
                mixed = y.astype(BF16)
                if mine:
                    gate(mixed, core * tiles_of[0] + t)
                else:
                    mix_out[k, p] = mixed
            if not mine:
                mix_copy(k).start()

    def finish(k):
        mix_copy(k).wait_recv()
        for p in range(hp):
            gate(mix_in[k, p], other * tiles_of[0] + p * tiles + k)

    for spot in range(2 * hp):
        work[spot, 0:8, :] = jnp.zeros((8, 128), F32)
        work[spot, 8 + tokens :, :] = jnp.zeros((8, 128), F32)
    low_ref[...] = jnp.zeros_like(low_ref)
    high_ref[...] = jnp.zeros_like(high_ref)
    half_copy(2).start()
    spread(0, fac_ref)
    half_wait(1)
    conv(1, 0, 0)
    half_wait(0)
    conv(0, 0, hp)
    edge_wait()
    fix(1, 0)
    fix(0, 0)
    first(0)
    spread(1, fac_ref)
    conv(1, 1, 0)
    conv(0, 1, hp)
    fix(1, 1)
    fix(0, 1)
    first(1)
    spread(2, fac_ref)
    conv(0, 2, 0)
    fix(0, 2)
    first(2)
    quad_logs()
    half_wait(2)
    for k in range(2):
        conv(2, k, k * hp)
    for k in range(2):
        fix(2, k)
    z_load.wait()

    up_step, z_first, z_next = 1.4, 2.7, 3.5
    plan = [(z_first - 0.01, z_logs)]
    for k in range(3):
        for d in range(2):
            when = up_step * (2 * k + d)
            plan.append((when, functools.partial(combine, k, d)))
            for r in range(rounds):
                plan.append((when + z_first + r * z_next, functools.partial(z_recv, r, k, d)))
    for p in range(hp):
        for r in range(2):
            plan.append((up_step * p + 0.1 + 0.01 * r, functools.partial(inner, p, r)))
    all_gates = functools.partial(
        lax.fori_loop, 0, 2 * tiles_of[0] // 4, gates, 0
    )
    plan.append((up_step * hp + 0.1, all_gates))
    done = z_first + (rounds - 1) * z_next
    for k in range(3):
        plan.append((done + up_step * k + 0.1, functools.partial(spread, k)))
    for _, step in sorted(plan, key=lambda one: one[0]):
        step()
    last(0)
    last(1)
    finish(0)
    last(2)
    finish(1)
    finish(2)

    for x in range(2):

        @pl.when(x * 2 + holder != here)
        def _(x=x):
            for i in range(5):
                param_copy(i, x).wait_send()

    for low, sends in ((True, sends_low), (False, sends_high)):

        @pl.when(sends)
        def _(low=low):
            for k in range(2):
                edge_copy(low, k).wait_send()

    for i in range(3):
        inc_copy(i).wait_send()
        half_copy(i).wait_send()
        qlog_copy(i).wait_send()
    for o in range(1, nz):
        zlog_copy(o).wait_send()
    for k in range(3):
        for i in range(3):
            for d in range(2):
                up_copy(k, d, i).wait_send()
                down_copy(k, d, i).wait_send()
        mix_copy(k).wait_send()
        for r in range(rounds):
            h, _, senders = z_parts(r)
            for d, sender in senders:

                @pl.when(sender)
                def _(k=k, r=r, d=d, h=h):
                    for o in range(1, h + 1):
                        z_copy(r, k, o, d).wait_send()


def fits_quad(sp, dp, blk, heads, groups):
    nz = dp // 2
    power = dp % 2 == 0 and nz > 1 and nz & (nz - 1) == 0
    shares = sp == 4 and groups % 4 == 0 and groups // 4 == sp
    return power and shares and blk == 128 and 2 * heads * HEAD_DIM == 3 * groups * 128


def quad_local(sp, dp, x, b, c, z, ahead, back, spike, wx, wb, wc, offset, fading, gain):
    x, b, c, z = x[0], b[0], c[0], z[0]
    blk, x_total = x.shape
    b_total = b.shape[1]
    groups = b_total // STATE
    heads = ahead.shape[2]
    pairs = groups // 2
    nz = dp // 2
    rounds = nz.bit_length() - 1
    tiles = heads // pairs * HEAD_DIM // 128
    hp, hh = pairs // 2, heads // 2
    x_half, b_half = x_total // 2, b_total // 2
    width = x_half + 2 * b_half
    slab = pl.cdiv(width // 128, 16) * 16
    params = (wx, wb, wc, offset, fading)
    vm = pltpu.VMEM
    gains = gain.reshape(x_total // 128, 128)
    scratch = [vm(one.shape, BF16) for one in (x, b, c, z)]
    scratch += [vm((2, 3, hh, blk), F32), vm((3, hh, blk), F32), vm(gains.shape, BF16)]
    scratch += [vm((blk, x_half), BF16), vm((blk, b_half), BF16), vm((blk, b_half), BF16)]
    scratch += [vm(one.shape, one.dtype) for one in params]
    scratch += [vm((2,) + one.shape, one.dtype) for one in params]
    scratch += [vm((2, 2, slab, 128), BF16)] + [vm((2, slab, 128), BF16)] * 2
    scratch += [vm((2 * hp, 2 * blk + 16, 128), F32), vm((width // 128, 8, 128), F32)]
    scratch += [vm((8, 128), F32), vm(gains.shape, F32)] + [vm((2 * blk, 128), F32)] * 3
    scratch += [vm((128, 2 * blk), F32)] * 3
    scratch += [vm((x_half // 128, 24, 128), F32)] * 2
    scratch += [vm((2 * hp, 2 * blk, STATE), F32), vm((x_total // 128, blk, 128), F32)]
    scratch += [vm((tiles, hp, 2, 2 * blk, 128), F32)]
    scratch += [vm((x_half // 128, 2 * blk, 128), BF16), vm((2 * hp, STATE, 2 * blk), BF16)]
    scratch += [vm((2 * hp, 2 * blk, 128), BF16), vm((x_half // 128, 2 * blk, 128), F32)]
    scratch += [vm((tiles, 4, 2, STATE, 128), BF16)] * 4
    scratch += [vm((8, 128), F32), vm((4, 8, 128), F32), vm((8, 128), F32), vm((nz, 8, 128), F32)]
    scratch += [vm((4, 2, tiles, 8, 128), F32)] * 2 + [vm((2, tiles, 8, 128), F32)]
    scratch += [vm((rounds, 2, tiles, 8, 128), F32)]
    scratch += [vm((tiles, 2, STATE, 128), F32)] * 2 + [vm((rounds, tiles, STATE, 128), BF16)] * 2
    scratch += [vm((tiles, hp, blk, 128), BF16)] * 2
    dma = pltpu.SemaphoreType.DMA
    scratch += [dma((16,)), dma((2, 5, 2)), dma((2, 2)), dma((2, 3)), dma((2, 3))]
    scratch += [dma((2, 4)), dma((2, nz)), dma((2, 2 * tiles, 4)), dma((rounds, tiles, nz))]
    scratch += [dma((rounds, tiles)), dma((2, 2 * tiles, 4)), dma((2, tiles))]
    out = pl.pallas_call(
        functools.partial(quad_kernel, (heads, pairs, sp, dp)),
        out_shape=pltpu.VMEM((blk, x_total), BF16),
        in_specs=[pl.BlockSpec(memory_space=pltpu.HBM)] * 13,
        out_specs=pl.BlockSpec(memory_space=pltpu.VMEM),
        scratch_shapes=scratch,
        compiler_params=pltpu.CompilerParams(
            collective_id=0, has_side_effects=True, vmem_limit_bytes=60 * 2**20
        ),
        name="mixer",
    )(x, b, c, z, ahead[0].T, back[0].T, spike[0].T, *params, gains)
    return out[None]


def pick(sp, dp, x, b, *rest):
    blk, heads = x.shape[1], rest[2].shape[2]
    if fits_quad(sp, dp, blk, heads, b.shape[2] // STATE):
        return quad_local(sp, dp, x, b, *rest)
    return local(sp, dp, x, b, *rest)


def solution(mesh):
    tokens = P("dp", "sp", None)
    placed = (tokens,) * 7 + (P(None, "sp"),) * 5 + (P(),)
    return jax.shard_map(
        functools.partial(pick, mesh.shape["sp"], mesh.shape["dp"]),
        mesh=mesh,
        in_specs=placed,
        out_specs=tokens,
        check_vma=False,
    )
```

```python
import functools

import jax
import jax.numpy as jnp
from jax import lax
from jax.experimental import pallas as pl
from jax.experimental.pallas import tpu as pltpu
from jax.sharding import PartitionSpec as P

F32 = jnp.float32
BF16 = jnp.bfloat16
HEAD_DIM = 64
STATE = 128
EDGE = 8
HIGHEST = lax.Precision.HIGHEST


def levels_of(sp, dp, groups):
    found = []
    split = 1
    core = 2 if sp % 2 == 0 else 1
    inner = 2 if dp % 2 == 0 and groups % (2 * sp) == 0 else 1
    for axis, count, stride in (("sp", core, 1), ("sp", sp // core, core), ("dp", inner, 1)):
        if count > 1:
            found.append((axis, count, stride))
            split *= count
    return tuple(found), ("dp", dp // inner, inner)


def digit_of(level):
    axis, count, stride = level
    return lax.rem(lax.axis_index(axis) // stride, count)


def member_id(level, member):
    axis, count, stride = level
    return {axis: lax.axis_index(axis) + (member - digit_of(level)) * stride}


def kernel(levels, top, sizes, *refs):
    heads, pairs, chunks, sp, dp = sizes
    (x_ref, b_ref, c_ref, z_ref, ahead_ref, back_ref, spike_ref) = refs[:7]
    params = refs[7:12]
    gain_ref, out_ref = refs[12:14]
    (xc, bc, cc, y_ref, cum_ref, rate_ref, cum_t, rate_t, fac_ref) = refs[14:23]
    refs = refs[:14] + refs[23:]
    got, w_ref, prm_ref, halo_ref, edges, early_sem, edge_sem = (
        refs[14:19], refs[19], refs[20], refs[21], refs[22:28], refs[28], refs[29]
    )
    rest = list(refs[30:])
    depth = len(levels)
    logs = [rest.pop(0) for _ in range(depth + 1)]
    up_log = [rest.pop(0) for _ in range(depth + 1)]
    decay = [rest.pop(0) for _ in range(depth + 1)]
    log_sem = [rest.pop(0) for _ in range(depth + 1)]
    totals, up, down, stage, sems, incoming = ([] for _ in range(6))
    for _ in range(chunks):
        totals.append([rest.pop(0) for _ in range(depth + 1)])
        up.append([rest.pop(0) for _ in range(depth + 1)])
        down.append([rest.pop(0) for _ in range(depth)])
        stage.append([rest.pop(0) for _ in range(depth)])
        sems.append([rest.pop(0) for _ in range(depth + 1)])
        incoming.append(rest.pop(0))
    blk = x_ref.shape[0]
    per_pair = heads // pairs
    x_w = per_pair * HEAD_DIM
    b_w = 2 * STATE
    tiles = x_w // 128
    lane = lax.broadcasted_iota(jnp.int32, (blk, 128), 1)
    left = lane < HEAD_DIM
    row = lax.broadcasted_iota(jnp.int32, (blk, 128), 0)

    segment = ("sp", sp, 1)
    here, there = lax.axis_index("sp"), lax.axis_index("dp")
    rank = there * sp + here
    has_next, has_prev = rank < sp * dp - 1, rank > 0
    after = {"sp": lax.rem(here + 1, sp), "dp": lax.rem(there + (here + 1) // sp, dp)}
    before = {
        "sp": lax.rem(here + sp - 1, sp),
        "dp": lax.rem(there + dp - (sp - here) // sp, dp),
    }
    mesh_id = pl.DeviceIdType.MESH
    barrier = pltpu.get_barrier_semaphore()
    greeted = 0
    for level in levels + (top, segment):
        me = digit_of(level)
        for o in range(1, level[1]):
            target = member_id(level, lax.rem(me + o, level[1]))
            pl.semaphore_signal(barrier, inc=1, device_id=target, device_id_type=mesh_id)
            greeted += 1
    for present, target in ((has_next, after), (has_prev, before)):

        @pl.when(present)
        def _(target=target):
            pl.semaphore_signal(barrier, inc=1, device_id=target, device_id_type=mesh_id)

    filler = jnp.zeros((128 - 2 * heads, blk), F32)
    inc = jnp.concatenate([ahead_ref[...], back_ref[...], filler], axis=0).T
    spikes = jnp.concatenate([spike_ref[...], spike_ref[...], filler], axis=0).T
    count = sp * dp
    neighbours = (rank + count - 1) // count + (2 * count - 2 - rank) // count
    pl.semaphore_wait(barrier, greeted + neighbours)

    def edge_copy(i, direction):
        src = (x_ref, b_ref, c_ref)[i]
        start = blk - EDGE if direction == 0 else 0
        return pltpu.make_async_remote_copy(
            src_ref=src.at[pl.ds(start, EDGE), :],
            dst_ref=edges[3 * direction + i],
            send_sem=edge_sem.at[0, direction, i],
            recv_sem=edge_sem.at[1, direction, i],
            device_id=(after, before)[direction],
            device_id_type=mesh_id,
        )

    def param_copy(i, member, slot):
        return pltpu.make_async_remote_copy(
            src_ref=params[i],
            dst_ref=got[i].at[slot],
            send_sem=early_sem.at[0, i, member],
            recv_sem=early_sem.at[1, i, slot],
            device_id=member_id(segment, member),
            device_id_type=mesh_id,
        )

    for o in range(1, sp):
        for i in range(5):
            param_copy(i, lax.rem(here + o, sp), here).start()
    for direction, present in ((0, has_next), (1, has_prev)):

        @pl.when(present)
        def _(direction=direction):
            for i in range(3):
                edge_copy(i, direction).start()

    for i in range(5):
        got[i][here] = params[i][...]
    for o in range(1, sp):
        for i in range(5):
            s = lax.rem(here + o, sp)
            param_copy(i, s, s).wait_recv()
    prm_ref[...] = jnp.zeros_like(prm_ref)
    wide = got[3].shape[2]
    for q in range(sp):
        for kind in range(2):
            for d in range(2):
                at = slice(d * heads + q * wide, d * heads + (q + 1) * wide)
                prm_ref[kind : kind + 1, at] = got[3 + kind][q, d : d + 1, :]
        off = 0
        for i in range(3):
            n = got[i].shape[2]
            w_ref[0:4, off + q * n : off + (q + 1) * n] = got[i][q].astype(F32)
            off += n * sp
    rate = jax.nn.softplus(inc + prm_ref[0:1, :])
    log_decay = -jnp.exp(prm_ref[1:2, :]) * rate + spikes
    lower = (lane <= row).astype(F32)
    upper = (lane >= row).astype(F32)
    cum_f = jnp.dot(lower, log_decay, precision=HIGHEST, preferred_element_type=F32)
    cum_b = jnp.dot(upper, log_decay, precision=HIGHEST, preferred_element_type=F32)
    cum = jnp.where(lane < heads, cum_f, cum_b)
    lane1 = lane[0:1]
    last = jnp.where(lane1 < heads, cum_f[blk - 1 : blk], cum_b[0:1])
    cum_ref[...] = cum
    rate_ref[...] = rate
    cum_t[...] = cum.T
    rate_t[...] = rate.T
    fac_ref[...] = rate * jnp.exp(last - cum)
    logs[0][...] = jnp.broadcast_to(last, (8, 128))

    def rolled(ref, p):
        return pltpu.roll(ref[...], lax.rem(128 - p * per_pair, 128), 1)

    def two(cols, i):
        return jnp.where(left, cols[:, i : i + 1], cols[:, i + 1 : i + 2])

    def conv(src, col, width, off):
        at = pl.ds(pl.multiple_of(off + col, 128), width)
        v = src[:, pl.ds(pl.multiple_of(col, 128), width)].astype(F32)
        r = lax.broadcasted_iota(jnp.int32, (blk, width), 0)
        h0, h1, h2 = halo_ref[0:1, at], halo_ref[1:2, at], halo_ref[2:3, at]
        m1 = jnp.where(r == 0, h1, pltpu.roll(v, 1, 0))
        m2 = jnp.where(r == 0, h0, jnp.where(r == 1, h1, pltpu.roll(v, 2, 0)))
        p1 = jnp.where(r == blk - 1, h2, pltpu.roll(v, blk - 1, 0))
        s = m2 * w_ref[0:1, at] + m1 * w_ref[1:2, at] + v * w_ref[2:3, at] + p1 * w_ref[3:4, at]
        return (s / (1.0 + jnp.exp(-s))).astype(BF16)

    share = pairs // chunks
    x_total = x_ref.shape[1]
    b_total = b_ref.shape[1]

    def first(c, p, _):
        x_at = pl.ds(pl.multiple_of(p * x_w, 128), x_w)
        b_at = pl.ds(pl.multiple_of(p * b_w, 128), b_w)
        xv = conv(x_ref, p * x_w, x_w, 0)
        bv = conv(b_ref, p * b_w, b_w, x_total)
        xc[:, x_at] = xv
        bc[:, b_at] = bv
        cc[:, b_at] = conv(c_ref, p * b_w, b_w, x_total + b_total)
        cols = rolled(fac_ref, p)
        xf = xv.astype(F32)
        for d in range(2):
            scaled = jnp.concatenate(
                [
                    (xf[:, k * 128 : (k + 1) * 128] * two(cols, d * heads + 2 * k)).astype(BF16)
                    for k in range(tiles)
                ],
                axis=1,
            )
            u = lax.dot_general(scaled, bv, (((0,), (0,)), ((), ())), preferred_element_type=F32)
            half = x_w // 2
            rows = pl.ds(pl.multiple_of((p - c * share) * x_w, 128), x_w)
            totals[c][0][d, rows, :] = jnp.concatenate(
                [u[:half, :STATE], u[half:, STATE:]], axis=0
            ).astype(BF16)
        return 0

    for direction, present in ((0, has_prev), (1, has_next)):

        @pl.when(present)
        def _(direction=direction):
            for i in range(3):
                edge_copy(i, direction).wait_recv()

    off = 0
    for i in range(3):
        n = edges[i].shape[1]
        low = edges[i][...].astype(F32)
        high = edges[3 + i][...].astype(F32)
        halo_ref[0:2, off : off + n] = jnp.where(has_prev, low[EDGE - 2 :], 0.0)
        halo_ref[2:3, off : off + n] = jnp.where(has_next, high[0:1], 0.0)
        off += n
    def inner(p, _):
        x_at = pl.ds(pl.multiple_of(p * x_w, 128), x_w)
        b_at = pl.ds(pl.multiple_of(p * b_w, 128), b_w)
        bv, cv, xv = bc[:, b_at], cc[:, b_at], xc[:, x_at]
        cols = rolled(cum_ref, p)
        parts = []
        for g in range(2):
            scores = lax.dot_general(
                cv[:, g * STATE : (g + 1) * STATE],
                bv[:, g * STATE : (g + 1) * STATE],
                (((1,), (1,)), ((), ())),
                preferred_element_type=F32,
            )
            for i in range(per_pair // 2):
                h = g * (per_pair // 2) + i
                hf = p * per_pair + h
                gap_f = cols[:, h : h + 1] - cum_t[pl.ds(hf, 1), :]
                gap_b = cols[:, heads + h : heads + h + 1] - cum_t[pl.ds(heads + hf, 1), :]
                gap = jnp.where(lane < row, gap_f, jnp.where(lane > row, gap_b, 0.0))
                rf, rb = rate_t[pl.ds(hf, 1), :], rate_t[pl.ds(heads + hf, 1), :]
                scale = jnp.where(lane < row, rf, jnp.where(lane > row, rb, rf + rb))
                parts.append((scores * jnp.exp(gap) * scale).astype(BF16))
        for k in range(tiles):
            xt = xv[:, k * 128 : (k + 1) * 128]
            zero = jnp.zeros_like(xt)
            both = jnp.concatenate([jnp.where(left, xt, zero), jnp.where(left, zero, xt)], axis=0)
            w = jnp.concatenate([parts[2 * k], parts[2 * k + 1]], axis=1)
            y_ref[:, pl.ds(pl.multiple_of(p * x_w + k * 128, 128), 128)] = jnp.dot(
                w, both, preferred_element_type=F32
            )
        return 0

    def copy(src, dst, send, recv, level, member):
        return pltpu.make_async_remote_copy(
            src_ref=src,
            dst_ref=dst,
            send_sem=send,
            recv_sem=recv,
            device_id=member_id(level, member),
            device_id_type=pl.DeviceIdType.MESH,
        )

    every_level = levels + (top,)
    head_share = heads // chunks
    bases = [jnp.int32(0)]
    size = head_share
    for level in levels:
        size = size // level[1]
        bases.append(bases[-1] + digit_of(level) * size)
    pending = [[] for _ in range(chunks)]

    def head_rows(h):
        return pl.ds(pl.multiple_of(h * HEAD_DIM, HEAD_DIM), HEAD_DIM)

    def log_copy(k, member, slot):
        sem = log_sem[k]
        return copy(
            logs[k], up_log[k].at[slot], sem.at[0, member], sem.at[1, slot], every_level[k], member
        )

    def start_up(c, k):
        level = every_level[k]
        n, me = level[1], digit_of(level)
        total, sem = totals[c][k], sems[c][k]
        rows = total.shape[1] // n
        for o in range(1, n):
            m = lax.rem(me + o, n)
            if c == 0:
                pending[c].append(log_copy(k, m, me))
            if k < depth:
                part = total.at[:, pl.ds(pl.multiple_of(m * rows, 64), rows), :]
            else:
                part = total.at[jnp.where(m < me, 1, 0)]
            pending[c].append(
                copy(part, up[c][k].at[me], sem.at[0, m], sem.at[1, me], level, m)
            )
        for one in pending[c]:
            one.start()
        if k < depth:
            up[c][k][me] = total[:, pl.ds(pl.multiple_of(me * rows, 64), rows), :]
        if c == 0:
            up_log[k][me] = logs[k][...]

    def flush(c):
        for one in pending[c]:
            one.wait_send()
        pending[c].clear()

    def finish_up(c, k):
        level = every_level[k]
        n, me = level[1], digit_of(level)
        total, sem = totals[c][k], sems[c][k]
        flush(c)
        for o in range(1, n):
            s = lax.rem(me + o, n)
            if c == 0:
                log_copy(k, s, s).wait_recv()
            part = total.at[:, pl.ds(0, total.shape[1] // n), :] if k < depth else total.at[0]
            copy(part, up[c][k].at[s], sem.at[0, s], sem.at[1, s], level, s).wait_recv()
        if c == 0:

            def expand(m, _):
                decay[k][m] = jnp.exp(jnp.broadcast_to(up_log[k][m][0:1, :], (128, 128)).T)
                return 0

            lax.fori_loop(0, n, expand, 0)
            if k < depth:
                log_sum = up_log[k][0]
                for m in range(1, n):
                    log_sum = log_sum + up_log[k][m]
                logs[k + 1][...] = log_sum

    def gather(c, k):
        n = levels[k][1]
        base = c * head_share + bases[k + 1]
        part, new = up[c][k], totals[c][k + 1]

        def one_head(h, _):
            at = head_rows(h)
            f = part[0, 0, at, :].astype(F32)
            b = part[n - 1, 1, at, :].astype(F32)
            for m in range(1, n):
                r = n - 1 - m
                f = f * decay[k][m, pl.ds(base + h, 1), :] + part[m, 0, at, :].astype(F32)
                b = b * decay[k][r, pl.ds(heads + base + h, 1), :] + part[r, 1, at, :].astype(F32)
            new[0, at, :] = f.astype(BF16)
            new[1, at, :] = b.astype(BF16)
            return 0

        lax.fori_loop(0, new.shape[1] // HEAD_DIM, one_head, 0)

    def enter(c):
        n, me = top[1], digit_of(top)
        base = c * head_share + bases[-1]
        into = incoming[c]
        into[...] = jnp.zeros_like(into)

        def carry(s, d):
            def one_head(h, _):
                at = head_rows(h)
                factor = decay[depth][s, pl.ds(d * heads + base + h, 1), :]
                into[d, at, :] = into[d, at, :] * factor + up[c][depth][s, at, :].astype(F32)
                return 0

            lax.fori_loop(0, into.shape[1] // HEAD_DIM, one_head, 0)
            return 0

        lax.fori_loop(0, me, lambda s, _: carry(s, 0), 0)
        lax.fori_loop(0, n - 1 - me, lambda i, _: carry(n - 1 - i, 1), 0)

    def start_down(c, k):
        level = levels[k]
        n, me = level[1], digit_of(level)
        sem = sems[c][k]
        rows = totals[c][k].shape[1] // n
        base = c * head_share + bases[k + 1]
        source = incoming[c] if k == depth - 1 else down[c][k + 1]
        part, out = up[c][k], stage[c][k]

        def spread(h, _):
            at = head_rows(h)
            f = source[0, at, :].astype(F32)
            b = source[1, at, :].astype(F32)
            for m in range(n):
                r = n - 1 - m
                out[m, 0, at, :] = f.astype(BF16)
                out[r, 1, at, :] = b.astype(BF16)
                if m < n - 1:
                    f = f * decay[k][m, pl.ds(base + h, 1), :] + part[m, 0, at, :].astype(F32)
                    down_factor = decay[k][r, pl.ds(heads + base + h, 1), :]
                    b = b * down_factor + part[r, 1, at, :].astype(F32)
            return 0

        lax.fori_loop(0, rows // HEAD_DIM, spread, 0)
        mine = pl.ds(pl.multiple_of(me * rows, 64), rows)
        for o in range(1, n):
            m = lax.rem(me + o, n)
            pending[c].append(
                copy(out.at[m], down[c][k].at[:, mine, :], sem.at[2, m], sem.at[3, me], level, m)
            )
        for one in pending[c]:
            one.start()
        down[c][k][:, mine, :] = out[me]

    def finish_down(c, k):
        level = levels[k]
        n, me = level[1], digit_of(level)
        sem = sems[c][k]
        rows = totals[c][k].shape[1] // n
        flush(c)
        for o in range(1, n):
            s = lax.rem(me + o, n)
            theirs = pl.ds(pl.multiple_of(s * rows, 64), rows)
            copy(
                stage[c][k].at[s], down[c][k].at[:, theirs, :], sem.at[2, s], sem.at[3, s], level, s
            ).wait_recv()

    for c in range(chunks):
        lax.fori_loop(c * share, (c + 1) * share, functools.partial(first, c), 0)
        start_up(c, 0)
    for o in range(1, sp):
        for i in range(5):
            param_copy(i, lax.rem(here + o, sp), here).wait_send()
    for direction, present in ((0, has_next), (1, has_prev)):

        @pl.when(present)
        def _(direction=direction):
            for i in range(3):
                edge_copy(i, direction).wait_send()


    gaps = chunks * depth
    cuts = [(i * pairs) // gaps for i in range(gaps + 1)]
    for k in range(depth):
        for c in range(chunks):
            finish_up(c, k)
            gather(c, k)
            start_up(c, k + 1)
            at = k * chunks + c
            lax.fori_loop(cuts[at], cuts[at + 1], inner, 0)
    for c in range(chunks):
        finish_up(c, depth)
        enter(c)
        start_down(c, depth - 1)
    for k in reversed(range(1, depth)):
        for c in range(chunks):
            finish_down(c, k)
            start_down(c, k - 1)

    cum_ref[...] = jnp.exp(cum_ref[...])

    def last_part(c, p, _):
        cv = cc[:, pl.ds(pl.multiple_of(p * b_w, 128), b_w)]
        cols = rolled(cum_ref, p)
        carried = []
        for d in range(2):
            st = down[c][0][d, pl.ds(pl.multiple_of((p - c * share) * x_w, 128), x_w), :]
            got = [
                lax.dot_general(
                    cv[:, g * STATE : (g + 1) * STATE],
                    st,
                    (((1,), (1,)), ((), ())),
                    preferred_element_type=F32,
                )
                for g in range(2)
            ]
            carried.append(got)
        for k in range(tiles):
            cut = slice(k * 128, (k + 1) * 128)
            at = pl.ds(pl.multiple_of(p * x_w + k * 128, 128), 128)
            y = y_ref[:, at]
            for d in range(2):
                a, b = carried[d][0][:, cut], carried[d][1][:, cut]
                if 2 * k + 1 < per_pair // 2:
                    v = a
                elif 2 * k >= per_pair // 2:
                    v = b
                else:
                    v = jnp.where(left, a, b)
                y = y + v * two(cols, d * heads + 2 * k)
            z = z_ref[:, at].astype(F32)
            gated = y.astype(BF16).astype(F32) * (z / (1.0 + jnp.exp(-z)))
            square = gated * gated
            low = jnp.sum(jnp.where(left, square, 0.0), axis=1, keepdims=True)
            high = jnp.sum(jnp.where(left, 0.0, square), axis=1, keepdims=True)
            mean = jnp.where(left, low, high) * (1.0 / HEAD_DIM)
            out_ref[:, at] = (gated * lax.rsqrt(mean + 1e-6) * gain_ref[0:1, at]).astype(BF16)
        return 0

    for c in range(chunks):
        finish_down(c, 0)
        lax.fori_loop(c * share, (c + 1) * share, functools.partial(last_part, c), 0)


def local(sp, dp, x, b, c, z, ahead, back, spike, wx, wb, wc, offset, fading, gain):
    x, b, c, z = x[0], b[0], c[0], z[0]
    blk, x_total = x.shape
    groups = b.shape[1] // STATE
    heads = ahead.shape[2]
    pairs = groups // 2
    levels, top = levels_of(sp, dp, groups)
    scratch = [
        pltpu.VMEM((blk, x_total), BF16),
        pltpu.VMEM((blk, groups * STATE), BF16),
        pltpu.VMEM((blk, groups * STATE), BF16),
        pltpu.VMEM((blk, x_total), F32),
    ]
    scratch += [pltpu.VMEM((128, 128), F32)] * 5
    params = (wx, wb, wc, offset, fading)
    width = x_total + 2 * b.shape[1]
    early = [pltpu.VMEM((sp,) + one.shape, one.dtype) for one in params]
    early += [pltpu.VMEM((8, width), F32), pltpu.VMEM((8, 128), F32), pltpu.VMEM((8, width), F32)]
    early += [pltpu.VMEM((EDGE, one.shape[1]), BF16) for one in (x, b, c)] * 2
    early += [pltpu.SemaphoreType.DMA((2, 5, sp)), pltpu.SemaphoreType.DMA((2, 2, 3))]
    scratch += early
    split = 1
    for level in levels:
        split *= level[1]
    chunks = 2 if groups % (2 * split) == 0 else 1
    counts = [level[1] for level in levels] + [top[1]]
    scratch += [pltpu.VMEM((8, 128), F32)] * len(counts)
    scratch += [pltpu.VMEM((n, 8, 128), F32) for n in counts]
    scratch += [pltpu.VMEM((n, 128, 128), F32) for n in counts]
    scratch += [pltpu.SemaphoreType.DMA((2, n)) for n in counts]
    for _ in range(chunks):
        held = [x_total // chunks]
        for n in counts[:-1]:
            held.append(held[-1] // n)
        slabs = list(zip(counts[:-1], held[1:]))
        scratch += [pltpu.VMEM((2, rows, STATE), BF16) for rows in held]
        scratch += [pltpu.VMEM((n, 2, rows, STATE), BF16) for n, rows in slabs]
        scratch += [pltpu.VMEM((counts[-1], held[-1], STATE), BF16)]
        scratch += [pltpu.VMEM((2, rows, STATE), BF16) for rows in held[:-1]]
        scratch += [pltpu.VMEM((n, 2, rows, STATE), BF16) for n, rows in slabs]
        scratch += [pltpu.SemaphoreType.DMA((4, n)) for n in counts]
        scratch += [pltpu.VMEM((2, held[-1], STATE), F32)]
    out = pl.pallas_call(
        functools.partial(kernel, levels, top, (heads, pairs, chunks, sp, dp)),
        out_shape=jax.ShapeDtypeStruct((blk, x_total), BF16),
        in_specs=[pl.BlockSpec(memory_space=pltpu.VMEM)] * 13,
        out_specs=pl.BlockSpec(memory_space=pltpu.VMEM),
        scratch_shapes=scratch,
        compiler_params=pltpu.CompilerParams(
            collective_id=0, has_side_effects=True, vmem_limit_bytes=60 * 2**20
        ),
        name="mixer",
    )(x, b, c, z, ahead[0].T, back[0].T, spike[0].T, *params, gain.astype(F32)[None])
    return out[None]


def quad_kernel(sizes, *refs):
    heads, pairs, sp, dp = sizes
    nz = dp // 2
    rounds = nz.bit_length() - 1
    (x_hbm, b_hbm, c_hbm, z_hbm, ahead_hbm, back_hbm, spike_hbm) = refs[:7]
    params = refs[7:12]
    gain_hbm, out_ref = refs[12:14]
    (in_x, in_b, in_c, in_z, inc, inc_out, gain_in, px, pb, pc) = refs[14:24]
    own, got = refs[24:29], refs[29:34]
    edge_out, low_in, high_in = refs[34:37]
    refs = refs[:37] + (None,) * 3 + refs[37:]
    (work, w_ref, prm_ref, gain_ref, cum_ref, fac_ref, col_ref, cum_t, rate_t, mid_t) = refs[40:50]
    low_ref, high_ref, bc, zg, wide_cum = refs[50:55]
    refs = refs[:50] + refs[55:]
    (xc, bt, cc, y_ref, sup, up_in, down_out, down_in) = refs[50:58]
    (logs, qlog, zsum, zlog, dec, wup, zdec, zwt) = refs[58:66]
    (tz, zin, zs, zr, mix_out, mix_in) = refs[66:72]
    (load_sem, prm_sem, edge_sem, half_sem, inc_sem, qlog_sem, zlog_sem) = refs[72:79]
    (up_sem, zsend_sem, zrecv_sem, down_sem, mix_sem) = refs[79:84]

    hh = heads // 2
    hp = pairs // 2
    per_pair = heads // pairs
    tiles = per_pair * HEAD_DIM // 128
    blk = in_x.shape[0]
    tokens = 2 * blk
    x_half = in_x.shape[1] // 2
    b_half = in_b.shape[1] // 2
    x_w = per_pair * HEAD_DIM
    mesh_id = pl.DeviceIdType.MESH

    here, there = lax.axis_index("sp"), lax.axis_index("dp")
    core, cx = lax.rem(here, 2), here // 2
    cy, cz = lax.rem(there, 2), there // 2
    other = 1 - core
    me = cy * 2 + cx
    chip = there * 2 + cx
    chips = dp * 2
    has_next, has_prev = chip < chips - 1, chip > 0
    after, before = lax.rem(chip + 1, chips), lax.rem(chip + chips - 1, chips)
    partner = {"sp": cx * 2 + other}

    def chip_id(c, k):
        return {"sp": lax.rem(c, 2) * 2 + k, "dp": c // 2}

    def quad_id(qy, qx):
        return {"sp": qx * 2 + core, "dp": cz * 2 + qy}

    def z_id(z):
        return {"dp": z * 2 + cy}

    def member(i):
        qy = lax.rem(cy + lax.rem(i + 1, 2), 2)
        qx = lax.rem(cx + (3 - i) // 2, 2)
        return qy, qx, qy * 2 + qx

    def remote(src, dst, send, recv, target):
        return pltpu.make_async_remote_copy(
            src_ref=src, dst_ref=dst, send_sem=send, recv_sem=recv,
            device_id=target, device_id_type=mesh_id,
        )

    barrier = pltpu.get_barrier_semaphore()

    def greet(target):
        pl.semaphore_signal(barrier, inc=1, device_id=target, device_id_type=mesh_id)

    for o in range(1, sp):
        greet({"sp": lax.rem(here + o, sp)})
    for i in range(3):
        qy, qx, _ = member(i)
        greet(quad_id(qy, qx))
    for o in range(1, nz):
        greet(z_id(lax.rem(cz + o, nz)))
    for present, neighbour in ((has_next, after), (has_prev, before)):

        @pl.when(present)
        def _(neighbour=neighbour):
            for k in range(2):
                greet(chip_id(neighbour, k))

    loads = []

    def load(src, dst):
        one = pltpu.make_async_copy(src, dst, load_sem.at[len(loads)])
        one.start()
        loads.append(one)
        return one

    param_loads = [load(params[i], own[i]) for i in range(5)]
    mine = pl.ds(pl.multiple_of(core * hh, 8), hh)
    theirs = pl.ds(pl.multiple_of(other * hh, 8), hh)
    raw = (ahead_hbm, back_hbm, spike_hbm)
    for i in range(3):
        pltpu.make_async_copy(raw[i].at[theirs, :], inc_out.at[i], load_sem.at[10]).start()
        pltpu.make_async_copy(raw[i].at[mine, :], inc.at[core, i], load_sem.at[11]).start()
    b_load = load(b_hbm, in_b)
    x_load = load(x_hbm, in_x)
    c_load = load(c_hbm, in_c)
    gain_load = load(gain_hbm, gain_in)
    z_load = load(z_hbm, in_z)

    for spot in range(2 * hp):
        work[spot, 0:8, :] = jnp.zeros((8, 128), F32)
        work[spot, 8 + tokens :, :] = jnp.zeros((8, 128), F32)
    low_ref[...] = jnp.zeros_like(low_ref)
    high_ref[...] = jnp.zeros_like(high_ref)
    for one in param_loads:
        one.wait()
    pltpu.make_async_copy(inc_out, inc_out, load_sem.at[10]).wait()
    chip_greets = 2 * ((chip + chips - 1) // chips + (2 * chips - 2 - chip) // chips)
    pl.semaphore_wait(barrier, (sp - 1) + 3 + (nz - 1) + chip_greets)

    holder = here // 2
    slot = lax.rem(here, 2)

    def param_copy(i, x):
        return remote(
            own[i], got[i].at[slot], prm_sem.at[0, i, x], prm_sem.at[1, i, slot],
            {"sp": x * 2 + holder},
        )

    for x in range(2):
        elsewhere = x * 2 + holder != here

        @pl.when(elsewhere)
        def _(x=x):
            for i in range(5):
                param_copy(i, x).start()

        @pl.when(jnp.logical_not(elsewhere))
        def _():
            for i in range(5):
                got[i][slot] = own[i][...]

    inc_copy = remote(inc_out, inc.at[core], inc_sem.at[0], inc_sem.at[1], partner)
    inc_copy.start()

    sources = (in_x, in_b, in_c)
    halves = (x_half, b_half, b_half)

    edge_from = (0, x_half // 128, (x_half + b_half) // 128)

    def edge_copy(low, k):
        return remote(
            edge_out.at[k], low_in if low else high_in, edge_sem.at[0, k],
            edge_sem.at[1, 0 if low else 1], chip_id(after if low else before, k),
        )

    sends_low = jnp.logical_and(core == 1, has_next)
    sends_high = jnp.logical_and(core == 0, has_prev)

    def half_copy(i):
        cut = pl.ds(pl.multiple_of(other * halves[i], 128), halves[i])
        return remote(
            sources[i].at[:, cut], (px, pb, pc)[i], half_sem.at[0, i], half_sem.at[1, i], partner
        )

    for one in (b_load, x_load, c_load):
        one.wait()
    slab = edge_out.shape[2]
    for k in range(2):
        picked = [[], []]
        for i in range(3):
            for t in range(halves[i] // 128):
                at = slice(k * halves[i] + t * 128, k * halves[i] + (t + 1) * 128)
                end = sources[i][blk - EDGE :, at].astype(F32)[EDGE - 2 :]
                start = sources[i][0:EDGE, at].astype(F32)[0:2]
                both = jnp.where(core == 1, end, start)
                for r in range(2):
                    picked[r].append(both[r : r + 1])
        for r in range(2):
            spare = jnp.zeros((slab - len(picked[r]), 128), F32)
            edge_out[k, r] = jnp.concatenate(picked[r] + [spare], axis=0).astype(BF16)
    for low, sends in ((True, sends_low), (False, sends_high)):

        @pl.when(sends)
        def _(low=low):
            for k in range(2):
                edge_copy(low, k).start()

    for i in (1, 0):
        half_copy(i).start()

    lane = lax.broadcasted_iota(jnp.int32, (blk, 128), 1)
    row = lax.broadcasted_iota(jnp.int32, (blk, 128), 0)
    left = lane < HEAD_DIM
    left1 = left[0:1]
    lower = (lane <= row).astype(F32)
    upper = (lane >= row).astype(F32)
    filler = jnp.zeros((128 - 2 * hh, blk), F32)

    for q in range(2):
        from_q = 2 * core + q != here

        @pl.when(from_q)
        def _(q=q):
            for i in range(5):
                remote(
                    own[i], got[i].at[q], prm_sem.at[0, i, 0], prm_sem.at[1, i, q], partner
                ).wait_recv()

    pltpu.make_async_copy(inc.at[core], inc.at[core], load_sem.at[11]).wait()
    remote(inc_out, inc.at[other], inc_sem.at[0], inc_sem.at[1], partner).wait_recv()

    def half_wait(i):
        remote(
            sources[i].at[:, pl.ds(0, halves[i])], (px, pb, pc)[i], half_sem.at[0, i],
            half_sem.at[1, i], partner,
        ).wait_recv()

    def rolled(v, p):
        return pltpu.roll(v, lax.rem(128 - p * per_pair, 128), 1)

    def two(cols, i):
        mask = lax.broadcasted_iota(jnp.int32, (cols.shape[0], 128), 1) < HEAD_DIM
        return jnp.where(mask, cols[:, i : i + 1], cols[:, i + 1 : i + 2])

    tiles_of = [half // 128 for half in halves]
    starts = (0, tiles_of[0], tiles_of[0] + tiles_of[1])

    def silu(s):
        h = 0.5 * s
        return h + h * jnp.tanh(h)

    def store(i, t, rows, v):
        if i == 1:
            bc[t, rows, :] = v
        else:
            (xc, None, cc)[i][t, rows, :] = v.astype(BF16)

    def conv(i, k, base):
        for p in range(hp):
            t = p * (tiles_of[i] // hp) + k
            spot = base + p
            mine_at = pl.ds(pl.multiple_of(core * halves[i] + t * 128, 128), 128)
            at = pl.ds(pl.multiple_of(t * 128, 128), 128)
            buf = work.at[spot]
            here_at = pl.ds(pl.multiple_of(8 + core * blk, 8), blk)
            there_at = pl.ds(pl.multiple_of(8 + other * blk, 8), blk)
            buf[here_at, :] = sources[i][:, mine_at].astype(F32)
            buf[there_at, :] = (px, pb, pc)[i][:, at].astype(F32)
            s = buf[6 : 6 + tokens, :] * w_ref[starts[i] + t, 0:1, :]
            for tap in range(1, 4):
                near = buf[6 + tap : 6 + tap + tokens, :]
                s = s + near * w_ref[starts[i] + t, tap : tap + 1, :]
            store(i, t, slice(0, tokens), silu(s))

    def edge_wait():
        for low, present in ((True, has_prev), (False, has_next)):

            @pl.when(present)
            def _(low=low):
                edge_copy(low, 0).wait_recv()

    def fix(i, k):
        half = halves[i]
        mine_tiles = [p * (tiles_of[i] // hp) + k for p in range(hp)]
        row16 = row[0:16]
        lows = [low_in[r].astype(F32) for r in range(2)]
        highs = high_in[0].astype(F32)
        own_part = sources[i]
        their_part = (px, pb, pc)[i]
        for t in mine_tiles:
            mine_at = pl.ds(pl.multiple_of(core * half + t * 128, 128), 128)
            at = slice(t * 128, (t + 1) * 128)
            start = jnp.where(core == 0, own_part[0:8, mine_at], their_part[0:8, at])
            end = jnp.where(core == 1, own_part[blk - 8 :, mine_at], their_part[blk - 8 :, at])
            e = edge_from[i] + t
            for r in range(2):
                before_row = jnp.where(has_prev, lows[r][e : e + 1], 0.0)
                low_ref[t, 6 + r : 7 + r, :] = before_row
            low_ref[t, 8:16, :] = start.astype(F32)
            high_ref[t, 8:16, :] = end.astype(F32)
            high_ref[t, 16:17, :] = jnp.where(has_next, highs[e : e + 1], 0.0)
        dst = (xc, bc, cc)[i]
        for t in mine_tiles:
            for ref, low in ((low_ref, True), (high_ref, False)):
                s = ref[t, 6:14, :] * w_ref[starts[i] + t, 0:1, :]
                for k in range(1, 4):
                    s = s + ref[t, 6 + k : 14 + k, :] * w_ref[starts[i] + t, k : k + 1, :]
                s = silu(s)
                rows = slice(0, 16) if low else slice(tokens - 16, tokens)
                s = jnp.concatenate([s, s], axis=0)
                keep = row16 >= 2 if low else row16 < 15
                store(i, t, rows, jnp.where(keep, dst[t, rows, :].astype(F32), s))

    def up_copy(k, d, i):
        qy, qx, q = member(i)
        return remote(
            sup.at[k, q, d], up_in.at[k, me, d], up_sem.at[0], up_sem.at[1 + 2 * k + d],
            quad_id(qy, qx),
        )

    def wide_left(n):
        return lax.rem(lax.broadcasted_iota(jnp.int32, (128, n), 1), 128) < HEAD_DIM

    def first(k):
        for p in range(hp):
            if k < 2:
                bt[2 * p + k] = bc[2 * p + k].T.astype(BF16)
            xf = xc[p * tiles + k].astype(F32)
            rhs = jnp.concatenate(
                [(xf * wide_cum[k, p, d]).astype(BF16) for d in range(2)], axis=1
            )
            u = jnp.dot(bt[2 * p + k // 2], rhs, preferred_element_type=F32)
            if k == 1:
                v = jnp.dot(bt[2 * p + 1], rhs, preferred_element_type=F32)
                u = jnp.where(wide_left(256), u, v)
            u = u.astype(BF16)
            sup[k, p, 0] = u[:, :128]
            sup[k, p, 1] = u[:, 128:]
        for d in range(2):
            for i in range(3):
                up_copy(k, d, i).start()
        up_in[k, me] = sup[k, me]

    def inner(p, r):
        rows = slice(r * blk, (r + 1) * blk)
        cols = rolled(col_ref[rows, :], p)
        mid_row = mid_f if r == 1 else mid_b
        shift = rolled(jnp.exp(jnp.minimum(col_ref[rows, :] - mid_row, 0.0)), p)
        parts = []
        for g in range(2):
            scores = jnp.dot(cc[2 * p + g, rows], bt[2 * p + g], preferred_element_type=F32)
            on = scores[:, r * blk : (r + 1) * blk]
            away = scores[:, (1 - r) * blk : (2 - r) * blk]
            for h in range(g * per_pair // 2, (g + 1) * per_pair // 2):
                f = pl.ds(p * per_pair + h, 1)
                b = pl.ds(hh + p * per_pair + h, 1)
                gap_f = cols[:, h : h + 1] - cum_t[f, rows]
                gap_b = cols[:, hh + h : hh + h + 1] - cum_t[b, rows]
                gap = jnp.where(lane < row, gap_f, jnp.where(lane > row, gap_b, 0.0))
                rf, rb = rate_t[f, rows], rate_t[b, rows]
                scale = jnp.where(lane < row, rf, jnp.where(lane > row, rb, rf + rb))
                near = (on * jnp.exp(gap) * scale).astype(BF16)
                d = 1 - r
                c = d * hh + h
                far_rows = slice((1 - r) * blk, (2 - r) * blk)
                far_row = mid_t[f if d == 0 else b, far_rows]
                far = (away * shift[:, c : c + 1] * far_row).astype(BF16)
                parts.append(jnp.concatenate([near, far] if r == 0 else [far, near], axis=1))
        for k in range(tiles):
            xt = xc[p * tiles + k]
            zero = jnp.zeros_like(xt)
            mask = lax.broadcasted_iota(jnp.int32, xt.shape, 1) < HEAD_DIM
            both = jnp.concatenate(
                [jnp.where(mask, xt, zero), jnp.where(mask, zero, xt)], axis=0
            )
            w = jnp.concatenate([parts[2 * k], parts[2 * k + 1]], axis=1)
            y_ref[p * tiles + k, rows] = jnp.dot(w, both, preferred_element_type=F32)

    def zlog_copy(o):
        return remote(
            zsum, zlog.at[cz], zlog_sem.at[0], zlog_sem.at[1], z_id(lax.rem(cz + o, nz))
        )

    def quad_logs():
        three = qlog.at[0:3]
        remote(three, three, qlog_sem.at[0], qlog_sem.at[1], partner).wait_recv()
        zsum[...] = qlog[0] + qlog[1] + qlog[2] + qlog[3]
        for o in range(1, nz):
            zlog_copy(o).start()
        zlog[cz] = zsum[...]
        all_of = rolled(zsum[...], me)
        each_of = [rolled(qlog[q], me) for q in range(4)]
        for d in range(2):
            for k in range(tiles):
                zdec[d, k] = jnp.exp(two(all_of, d * hh + 2 * k))
                each = [two(one, d * hh + 2 * k) for one in each_of]
                reach = jnp.zeros_like(each[0])
                for q in reversed(range(4)) if d == 0 else range(4):
                    dec[q, d, k] = jnp.exp(each[q])
                    wup[q, d, k] = jnp.exp(reach)
                    reach = reach + each[q]

    def z_logs():
        rest = zlog.at[0 : nz - 1]
        remote(rest, rest, zlog_sem.at[0], zlog_sem.at[1], partner).wait_recv()
        reach = [[jnp.zeros((8, 128), F32) for _ in range(2)] for _ in range(rounds)]
        for s in range(nz):
            for r in range(rounds):
                h = 1 << r
                pos = lax.rem(cz, 2 * h)
                middle = cz - pos + h
                f_in = jnp.logical_and(s >= middle, s < cz)
                b_in = jnp.logical_and(s > cz, s < middle)
                reach[r][0] = reach[r][0] + jnp.where(f_in, zlog[s], 0.0)
                reach[r][1] = reach[r][1] + jnp.where(b_in, zlog[s], 0.0)
        for d in range(2):
            for r in range(rounds):
                total = rolled(reach[r][d], me)
                for k in range(tiles):
                    zwt[r, d, k] = jnp.exp(two(total, d * hh + 2 * k))

    def combine(k, d):
        three = up_in.at[k, 0:3, d]
        remote(three, three, up_sem.at[0], up_sem.at[1 + 2 * k + d], partner).wait_recv()
        acc = up_in[k, 0, d].astype(F32) * wup[0, d, k, 0:1, :]
        for q in range(1, 4):
            acc = acc + up_in[k, q, d].astype(F32) * wup[q, d, k, 0:1, :]
        tz[k, d] = acc
        zin[k, d] = jnp.zeros_like(acc)
        z_send(0, k, d)

    def z_copy(r, k, o, d):
        return remote(
            zs.at[r, k], zr.at[r, k], zsend_sem.at[r, o - 1], zrecv_sem.at[r, k],
            z_id(cz + o if d == 0 else cz - o),
        )

    def z_parts(r):
        h = 1 << r
        pos = lax.rem(cz, 2 * h)
        return h, pos, ((0, pos == h - 1), (1, pos == h))

    def z_send(r, k, d):
        h, _, senders = z_parts(r)

        @pl.when(senders[d][1])
        def _():
            zs[r, k] = (zin[k, d] * zdec[d, k, 0:1, :] + tz[k, d]).astype(BF16)
            for o in reversed(range(1, h + 1)):
                z_copy(r, k, o, d).start()

    def z_recv(r, k, d):
        h, pos, _ = z_parts(r)

        @pl.when(pos >= h if d == 0 else pos < h)
        def _():
            remote(
                zs.at[r, k], zr.at[r, k], zsend_sem.at[r, 0], zrecv_sem.at[r, k], partner
            ).wait_recv()
            zin[k, d] = zin[k, d] + zr[r, k].astype(F32) * zwt[r, d, k, 0:1, :]

        if r + 1 < rounds:
            z_send(r + 1, k, d)
        else:
            down(k, d)

    def down_copy(k, d, i):
        qy, qx, q = member(i)
        return remote(
            down_out.at[k, q, d], down_in.at[k, me, d], down_sem.at[0], down_sem.at[1 + k],
            quad_id(qy, qx),
        )

    def down(k, d):
        g = zin[k, d]
        order = list(range(4)) if d == 0 else list(reversed(range(4)))
        for q in order:
            down_out[k, q, d] = g.astype(BF16)
            if q != order[-1]:
                g = g * dec[q, d, k, 0:1, :] + up_in[k, q, d].astype(F32)
        for i in range(3):
            down_copy(k, d, i).start()
        down_in[k, me, d] = down_out[k, me, d]

    def gates(group, _):
        for spot in range(4):
            t = group * 4 + spot
            z = in_z[:, pl.ds(pl.multiple_of(t * 128, 128), 128)].astype(F32)
            zg[t] = silu(z)
        return 0

    def gate(mixed, t):
        gated = mixed.astype(F32) * zg[t]
        square = gated * gated
        low = jnp.sum(jnp.where(left, square, 0.0), axis=1, keepdims=True)
        high = jnp.sum(jnp.where(left, 0.0, square), axis=1, keepdims=True)
        mean = jnp.where(left, low, high) * (1.0 / HEAD_DIM)
        scale = lax.rsqrt(mean + 1e-6) * gain_ref[pl.ds(t, 1), :]
        out_ref[:, pl.ds(pl.multiple_of(t * 128, 128), 128)] = (gated * scale).astype(BF16)

    def mix_copy(k):
        return remote(
            mix_out.at[k], mix_in.at[k], mix_sem.at[0], mix_sem.at[1 + k], partner
        )

    def spread(k, ref=cum_ref):
        for j in range(2):
            cols = ref[j * blk : (j + 1) * blk, :]
            for p in range(hp):
                head = p * per_pair + 2 * k
                for d in range(2):
                    wide_cum[k, p, d, j * blk : (j + 1) * blk, :] = two(cols, d * hh + head)

    def last(k):
        three = down_in.at[k, 0:3]
        remote(three, three, down_sem.at[0], down_sem.at[1 + k], partner).wait_recv()
        for mine in (False, True):
            rows = pl.ds(pl.multiple_of((core if mine else other) * blk, 128), blk)
            for p in range(hp):
                rhs = jnp.concatenate([down_in[k, p, 0], down_in[k, p, 1]], axis=1)
                v = jnp.dot(cc[2 * p + k // 2, rows], rhs, preferred_element_type=F32)
                if k == 1:
                    u = jnp.dot(cc[2 * p + 1, rows], rhs, preferred_element_type=F32)
                    v = jnp.where(wide_left(256), v, u)
                t = p * tiles + k
                y = y_ref[t, rows] + v[:, :128] * wide_cum[k, p, 0, rows]
                y = y + v[:, 128:] * wide_cum[k, p, 1, rows]
                mixed = y.astype(BF16)
                if mine:
                    gate(mixed, core * tiles_of[0] + t)
                else:
                    mix_out[k, p] = mixed
            if not mine:
                mix_copy(k).start()

    def finish(k):
        mix_copy(k).wait_recv()
        for p in range(hp):
            gate(mix_in[k, p], other * tiles_of[0] + p * tiles + k)

    def early_sent():
        for x in range(2):

            @pl.when(x * 2 + holder != here)
            def _(x=x):
                for i in range(5):
                    param_copy(i, x).wait_send()

        for low, sends in ((True, sends_low), (False, sends_high)):

            @pl.when(sends)
            def _(low=low):
                for k in range(2):
                    edge_copy(low, k).wait_send()

        inc_copy.wait_send()
        for i in range(3):
            half_copy(i).wait_send()
        for all_of, sem in ((qlog.at[0:3], qlog_sem), (zlog.at[0 : nz - 1], zlog_sem)):
            remote(all_of, all_of, sem.at[0], sem.at[1], partner).wait_send()
        sent = sup.at[:, 0:3]
        remote(sent, sent, up_sem.at[0], up_sem.at[1], partner).wait_send()

    def z_sent():
        for r in range(rounds):
            h, _, senders = z_parts(r)

            @pl.when(jnp.logical_or(senders[0][1], senders[1][1]))
            def _(r=r, h=h):
                for o in range(h):
                    remote(
                        zs.at[r], zr.at[r], zsend_sem.at[r, o], zrecv_sem.at[r, 0], partner
                    ).wait_send()

    def rest_sent():
        sent = down_out.at[:, 0:3]
        remote(sent, sent, down_sem.at[0], down_sem.at[1], partner).wait_send()
        remote(mix_out, mix_in, mix_sem.at[0], mix_sem.at[1], partner).wait_send()

    half_wait(1)
    half_wait(0)
    prm_ref[...] = jnp.zeros_like(prm_ref)
    wide = own[3].shape[1]
    for q in range(2):
        for kind in range(2):
            for d in range(2):
                at = slice(d * hh + q * wide, d * hh + (q + 1) * wide)
                prm_ref[kind : kind + 1, at] = got[3 + kind][q, d : d + 1, :]
        off = 0
        for i in range(3):
            n = own[i].shape[1]
            part = got[i][q].astype(F32)
            for t in range(n // 128):
                w_ref[off + q * (n // 128) + t, 0:4, :] = part[:, t * 128 : (t + 1) * 128]
            off += 2 * n // 128

    cums, rates = [], []
    for j in range(2):
        pre = jnp.concatenate([inc[j, 0], inc[j, 1], filler], axis=0).T
        spikes = jnp.concatenate([inc[j, 2], inc[j, 2], filler], axis=0).T
        rate = jax.nn.softplus(pre + prm_ref[0:1, :])
        log_decay = -jnp.exp(prm_ref[1:2, :]) * rate + spikes
        cum_f = jnp.dot(lower, log_decay, precision=HIGHEST, preferred_element_type=F32)
        cum_b = jnp.dot(upper, log_decay, precision=HIGHEST, preferred_element_type=F32)
        cums.append((cum_f, cum_b))
        rates.append(rate)
    ahead_lane = lane < hh
    ahead1 = ahead_lane[0:1]
    mid_f, mid_b = cums[0][0][blk - 1 : blk], cums[1][1][0:1]
    total = jnp.where(ahead1, mid_f + cums[1][0][blk - 1 : blk], cums[0][1][0:1] + mid_b)
    logs[...] = jnp.broadcast_to(total, (8, 128))

    for j in range(2):
        cum_f, cum_b = cums[j]
        far = jnp.where(ahead_lane, mid_f if j == 1 else 0.0, mid_b if j == 0 else 0.0)
        near = jnp.where(ahead_lane, cum_f, cum_b)
        at = slice(j * blk, (j + 1) * blk)
        cum = near + far
        cum_ref[at, :] = jnp.exp(cum)
        fac_ref[at, :] = rates[j] * jnp.exp(total - cum)
        col_ref[at, :] = cum
        cum_t[:, at] = cum.T
        rate_t[:, at] = rates[j].T
        mid = rates[j] * jnp.exp(jnp.minimum((mid_f if j == 0 else mid_b) - near, 0.0))
        mid_t[:, at] = mid.T

    spread(0, fac_ref)
    conv(1, 0, 0)
    conv(0, 0, hp)
    def qlog_copy(i):
        qy, qx, q = member(i)
        return remote(
            logs, qlog.at[me], qlog_sem.at[0], qlog_sem.at[1], quad_id(qy, qx)
        )

    for i in range(3):
        qlog_copy(i).start()
    qlog[me] = logs[...]
    gain_load.wait()
    gain_ref[...] = gain_in[...].astype(F32)
    half_copy(2).start()
    edge_wait()
    fix(1, 0)
    fix(0, 0)
    first(0)
    spread(1, fac_ref)
    conv(1, 1, 0)
    conv(0, 1, hp)
    fix(1, 1)
    fix(0, 1)
    first(1)
    spread(2, fac_ref)
    conv(0, 2, 0)
    fix(0, 2)
    first(2)
    quad_logs()
    half_wait(2)
    for k in range(2):
        conv(2, k, k * hp)
    for k in range(2):
        fix(2, k)
    z_load.wait()

    up_step, z_first, z_next = 1.4, 2.7, 3.5
    plan = [(z_first - 0.01, z_logs)]
    for k in range(3):
        for d in range(2):
            when = up_step * (2 * k + d)
            plan.append((when, functools.partial(combine, k, d)))
            for r in range(rounds):
                plan.append((when + z_first + r * z_next, functools.partial(z_recv, r, k, d)))
    for p in range(hp):
        for r in range(2):
            when = up_step * max(2 * p + r - 1, 0) + 0.1 if p < 3 else up_step * 5 + 0.1
            plan.append((when, functools.partial(inner, p, r)))
    all_gates = functools.partial(
        lax.fori_loop, 0, 2 * tiles_of[0] // 4, gates, 0
    )
    plan.append((up_step * 6 + 0.1, all_gates))
    done = z_first + (rounds - 1) * z_next
    plan.append((up_step * 7 + 0.1, functools.partial(spread, 0)))
    for _, step in sorted(plan, key=lambda one: one[0]):
        step()
    spread(1)
    last(0)
    spread(2)
    early_sent()
    last(1)
    finish(0)
    z_sent()
    last(2)
    finish(1)
    finish(2)
    rest_sent()


def fits_quad(sp, dp, blk, heads, groups):
    nz = dp // 2
    power = dp % 2 == 0 and nz > 1 and nz & (nz - 1) == 0
    shares = sp == 4 and groups % 4 == 0 and groups // 4 == sp
    return power and shares and blk == 128 and 2 * heads * HEAD_DIM == 3 * groups * 128


def quad_local(sp, dp, x, b, c, z, ahead, back, spike, wx, wb, wc, offset, fading, gain):
    x, b, c, z = x[0], b[0], c[0], z[0]
    blk, x_total = x.shape
    b_total = b.shape[1]
    groups = b_total // STATE
    heads = ahead.shape[2]
    pairs = groups // 2
    nz = dp // 2
    rounds = nz.bit_length() - 1
    tiles = heads // pairs * HEAD_DIM // 128
    hp, hh = pairs // 2, heads // 2
    x_half, b_half = x_total // 2, b_total // 2
    width = x_half + 2 * b_half
    slab = pl.cdiv(width // 128, 16) * 16
    params = (wx, wb, wc, offset, fading)
    vm = pltpu.VMEM
    gains = gain.reshape(x_total // 128, 128)
    scratch = [vm(one.shape, BF16) for one in (x, b, c, z)]
    scratch += [vm((2, 3, hh, blk), F32), vm((3, hh, blk), F32), vm(gains.shape, BF16)]
    scratch += [vm((blk, x_half), BF16), vm((blk, b_half), BF16), vm((blk, b_half), BF16)]
    scratch += [vm(one.shape, one.dtype) for one in params]
    scratch += [vm((2,) + one.shape, one.dtype) for one in params]
    scratch += [vm((2, 2, slab, 128), BF16)] + [vm((2, slab, 128), BF16)] * 2
    scratch += [vm((2 * hp, 2 * blk + 16, 128), F32), vm((width // 128, 8, 128), F32)]
    scratch += [vm((8, 128), F32), vm(gains.shape, F32)] + [vm((2 * blk, 128), F32)] * 3
    scratch += [vm((128, 2 * blk), F32)] * 3
    scratch += [vm((x_half // 128, 24, 128), F32)] * 2
    scratch += [vm((2 * hp, 2 * blk, STATE), F32), vm((x_total // 128, blk, 128), F32)]
    scratch += [vm((tiles, hp, 2, 2 * blk, 128), F32)]
    scratch += [vm((x_half // 128, 2 * blk, 128), BF16), vm((2 * hp, STATE, 2 * blk), BF16)]
    scratch += [vm((2 * hp, 2 * blk, 128), BF16), vm((x_half // 128, 2 * blk, 128), F32)]
    scratch += [vm((tiles, 4, 2, STATE, 128), BF16)] * 4
    scratch += [vm((8, 128), F32), vm((4, 8, 128), F32), vm((8, 128), F32), vm((nz, 8, 128), F32)]
    scratch += [vm((4, 2, tiles, 8, 128), F32)] * 2 + [vm((2, tiles, 8, 128), F32)]
    scratch += [vm((rounds, 2, tiles, 8, 128), F32)]
    scratch += [vm((tiles, 2, STATE, 128), F32)] * 2 + [vm((rounds, tiles, STATE, 128), BF16)] * 2
    scratch += [vm((tiles, hp, blk, 128), BF16)] * 2
    dma = pltpu.SemaphoreType.DMA
    scratch += [dma((12,)), dma((2, 5, 2)), dma((2, 2)), dma((2, 3)), dma((2,))]
    scratch += [dma((2,)), dma((2,)), dma((1 + 2 * tiles,)), dma((rounds, nz // 2))]
    scratch += [dma((rounds, tiles)), dma((1 + tiles,)), dma((1 + tiles,))]
    out = pl.pallas_call(
        functools.partial(quad_kernel, (heads, pairs, sp, dp)),
        out_shape=pltpu.VMEM((blk, x_total), BF16),
        in_specs=[pl.BlockSpec(memory_space=pltpu.HBM)] * 13,
        out_specs=pl.BlockSpec(memory_space=pltpu.VMEM),
        scratch_shapes=scratch,
        compiler_params=pltpu.CompilerParams(
            collective_id=0, has_side_effects=True, vmem_limit_bytes=60 * 2**20
        ),
        name="mixer",
    )(x, b, c, z, ahead[0].T, back[0].T, spike[0].T, *params, gains)
    return out[None]


def pick(sp, dp, x, b, *rest):
    blk, heads = x.shape[1], rest[2].shape[2]
    if fits_quad(sp, dp, blk, heads, b.shape[2] // STATE):
        return quad_local(sp, dp, x, b, *rest)
    return local(sp, dp, x, b, *rest)


def solution(mesh):
    tokens = P("dp", "sp", None)
    placed = (tokens,) * 7 + (P(None, "sp"),) * 5 + (P(),)
    return jax.shard_map(
        functools.partial(pick, mesh.shape["sp"], mesh.shape["dp"]),
        mesh=mesh,
        in_specs=placed,
        out_specs=tokens,
        check_vma=False,
    )
```

```python
import functools

import jax
import jax.numpy as jnp
from jax import lax
from jax.experimental import pallas as pl
from jax.experimental.pallas import tpu as pltpu
from jax.sharding import PartitionSpec as P

F32 = jnp.float32
BF16 = jnp.bfloat16
HEAD_DIM = 64
STATE = 128
EDGE = 8
HIGHEST = lax.Precision.HIGHEST


def levels_of(sp, dp, groups):
    found = []
    split = 1
    core = 2 if sp % 2 == 0 else 1
    inner = 2 if dp % 2 == 0 and groups % (2 * sp) == 0 else 1
    for axis, count, stride in (("sp", core, 1), ("sp", sp // core, core), ("dp", inner, 1)):
        if count > 1:
            found.append((axis, count, stride))
            split *= count
    return tuple(found), ("dp", dp // inner, inner)


def digit_of(level):
    axis, count, stride = level
    return lax.rem(lax.axis_index(axis) // stride, count)


def member_id(level, member):
    axis, count, stride = level
    return {axis: lax.axis_index(axis) + (member - digit_of(level)) * stride}


def kernel(levels, top, sizes, *refs):
    heads, pairs, chunks, sp, dp = sizes
    (x_ref, b_ref, c_ref, z_ref, ahead_ref, back_ref, spike_ref) = refs[:7]
    params = refs[7:12]
    gain_ref, out_ref = refs[12:14]
    (xc, bc, cc, y_ref, cum_ref, rate_ref, cum_t, rate_t, fac_ref) = refs[14:23]
    refs = refs[:14] + refs[23:]
    got, w_ref, prm_ref, halo_ref, edges, early_sem, edge_sem = (
        refs[14:19], refs[19], refs[20], refs[21], refs[22:28], refs[28], refs[29]
    )
    rest = list(refs[30:])
    depth = len(levels)
    logs = [rest.pop(0) for _ in range(depth + 1)]
    up_log = [rest.pop(0) for _ in range(depth + 1)]
    decay = [rest.pop(0) for _ in range(depth + 1)]
    log_sem = [rest.pop(0) for _ in range(depth + 1)]
    totals, up, down, stage, sems, incoming = ([] for _ in range(6))
    for _ in range(chunks):
        totals.append([rest.pop(0) for _ in range(depth + 1)])
        up.append([rest.pop(0) for _ in range(depth + 1)])
        down.append([rest.pop(0) for _ in range(depth)])
        stage.append([rest.pop(0) for _ in range(depth)])
        sems.append([rest.pop(0) for _ in range(depth + 1)])
        incoming.append(rest.pop(0))
    blk = x_ref.shape[0]
    per_pair = heads // pairs
    x_w = per_pair * HEAD_DIM
    b_w = 2 * STATE
    tiles = x_w // 128
    lane = lax.broadcasted_iota(jnp.int32, (blk, 128), 1)
    left = lane < HEAD_DIM
    row = lax.broadcasted_iota(jnp.int32, (blk, 128), 0)

    segment = ("sp", sp, 1)
    here, there = lax.axis_index("sp"), lax.axis_index("dp")
    rank = there * sp + here
    has_next, has_prev = rank < sp * dp - 1, rank > 0
    after = {"sp": lax.rem(here + 1, sp), "dp": lax.rem(there + (here + 1) // sp, dp)}
    before = {
        "sp": lax.rem(here + sp - 1, sp),
        "dp": lax.rem(there + dp - (sp - here) // sp, dp),
    }
    mesh_id = pl.DeviceIdType.MESH
    barrier = pltpu.get_barrier_semaphore()
    greeted = 0
    for level in levels + (top, segment):
        me = digit_of(level)
        for o in range(1, level[1]):
            target = member_id(level, lax.rem(me + o, level[1]))
            pl.semaphore_signal(barrier, inc=1, device_id=target, device_id_type=mesh_id)
            greeted += 1
    for present, target in ((has_next, after), (has_prev, before)):

        @pl.when(present)
        def _(target=target):
            pl.semaphore_signal(barrier, inc=1, device_id=target, device_id_type=mesh_id)

    filler = jnp.zeros((128 - 2 * heads, blk), F32)
    inc = jnp.concatenate([ahead_ref[...], back_ref[...], filler], axis=0).T
    spikes = jnp.concatenate([spike_ref[...], spike_ref[...], filler], axis=0).T
    count = sp * dp
    neighbours = (rank + count - 1) // count + (2 * count - 2 - rank) // count
    pl.semaphore_wait(barrier, greeted + neighbours)

    def edge_copy(i, direction):
        src = (x_ref, b_ref, c_ref)[i]
        start = blk - EDGE if direction == 0 else 0
        return pltpu.make_async_remote_copy(
            src_ref=src.at[pl.ds(start, EDGE), :],
            dst_ref=edges[3 * direction + i],
            send_sem=edge_sem.at[0, direction, i],
            recv_sem=edge_sem.at[1, direction, i],
            device_id=(after, before)[direction],
            device_id_type=mesh_id,
        )

    def param_copy(i, member, slot):
        return pltpu.make_async_remote_copy(
            src_ref=params[i],
            dst_ref=got[i].at[slot],
            send_sem=early_sem.at[0, i, member],
            recv_sem=early_sem.at[1, i, slot],
            device_id=member_id(segment, member),
            device_id_type=mesh_id,
        )

    for o in range(1, sp):
        for i in range(5):
            param_copy(i, lax.rem(here + o, sp), here).start()
    for direction, present in ((0, has_next), (1, has_prev)):

        @pl.when(present)
        def _(direction=direction):
            for i in range(3):
                edge_copy(i, direction).start()

    for i in range(5):
        got[i][here] = params[i][...]
    for o in range(1, sp):
        for i in range(5):
            s = lax.rem(here + o, sp)
            param_copy(i, s, s).wait_recv()
    prm_ref[...] = jnp.zeros_like(prm_ref)
    wide = got[3].shape[2]
    for q in range(sp):
        for kind in range(2):
            for d in range(2):
                at = slice(d * heads + q * wide, d * heads + (q + 1) * wide)
                prm_ref[kind : kind + 1, at] = got[3 + kind][q, d : d + 1, :]
        off = 0
        for i in range(3):
            n = got[i].shape[2]
            w_ref[0:4, off + q * n : off + (q + 1) * n] = got[i][q].astype(F32)
            off += n * sp
    rate = jax.nn.softplus(inc + prm_ref[0:1, :])
    log_decay = -jnp.exp(prm_ref[1:2, :]) * rate + spikes
    lower = (lane <= row).astype(F32)
    upper = (lane >= row).astype(F32)
    cum_f = jnp.dot(lower, log_decay, precision=HIGHEST, preferred_element_type=F32)
    cum_b = jnp.dot(upper, log_decay, precision=HIGHEST, preferred_element_type=F32)
    cum = jnp.where(lane < heads, cum_f, cum_b)
    lane1 = lane[0:1]
    last = jnp.where(lane1 < heads, cum_f[blk - 1 : blk], cum_b[0:1])
    cum_ref[...] = cum
    rate_ref[...] = rate
    cum_t[...] = cum.T
    rate_t[...] = rate.T
    fac_ref[...] = rate * jnp.exp(last - cum)
    logs[0][...] = jnp.broadcast_to(last, (8, 128))

    def rolled(ref, p):
        return pltpu.roll(ref[...], lax.rem(128 - p * per_pair, 128), 1)

    def two(cols, i):
        return jnp.where(left, cols[:, i : i + 1], cols[:, i + 1 : i + 2])

    def conv(src, col, width, off):
        at = pl.ds(pl.multiple_of(off + col, 128), width)
        v = src[:, pl.ds(pl.multiple_of(col, 128), width)].astype(F32)
        r = lax.broadcasted_iota(jnp.int32, (blk, width), 0)
        h0, h1, h2 = halo_ref[0:1, at], halo_ref[1:2, at], halo_ref[2:3, at]
        m1 = jnp.where(r == 0, h1, pltpu.roll(v, 1, 0))
        m2 = jnp.where(r == 0, h0, jnp.where(r == 1, h1, pltpu.roll(v, 2, 0)))
        p1 = jnp.where(r == blk - 1, h2, pltpu.roll(v, blk - 1, 0))
        s = m2 * w_ref[0:1, at] + m1 * w_ref[1:2, at] + v * w_ref[2:3, at] + p1 * w_ref[3:4, at]
        return (s / (1.0 + jnp.exp(-s))).astype(BF16)

    share = pairs // chunks
    x_total = x_ref.shape[1]
    b_total = b_ref.shape[1]

    def first(c, p, _):
        x_at = pl.ds(pl.multiple_of(p * x_w, 128), x_w)
        b_at = pl.ds(pl.multiple_of(p * b_w, 128), b_w)
        xv = conv(x_ref, p * x_w, x_w, 0)
        bv = conv(b_ref, p * b_w, b_w, x_total)
        xc[:, x_at] = xv
        bc[:, b_at] = bv
        cc[:, b_at] = conv(c_ref, p * b_w, b_w, x_total + b_total)
        cols = rolled(fac_ref, p)
        xf = xv.astype(F32)
        for d in range(2):
            scaled = jnp.concatenate(
                [
                    (xf[:, k * 128 : (k + 1) * 128] * two(cols, d * heads + 2 * k)).astype(BF16)
                    for k in range(tiles)
                ],
                axis=1,
            )
            u = lax.dot_general(scaled, bv, (((0,), (0,)), ((), ())), preferred_element_type=F32)
            half = x_w // 2
            rows = pl.ds(pl.multiple_of((p - c * share) * x_w, 128), x_w)
            totals[c][0][d, rows, :] = jnp.concatenate(
                [u[:half, :STATE], u[half:, STATE:]], axis=0
            ).astype(BF16)
        return 0

    for direction, present in ((0, has_prev), (1, has_next)):

        @pl.when(present)
        def _(direction=direction):
            for i in range(3):
                edge_copy(i, direction).wait_recv()

    off = 0
    for i in range(3):
        n = edges[i].shape[1]
        low = edges[i][...].astype(F32)
        high = edges[3 + i][...].astype(F32)
        halo_ref[0:2, off : off + n] = jnp.where(has_prev, low[EDGE - 2 :], 0.0)
        halo_ref[2:3, off : off + n] = jnp.where(has_next, high[0:1], 0.0)
        off += n
    def inner(p, _):
        x_at = pl.ds(pl.multiple_of(p * x_w, 128), x_w)
        b_at = pl.ds(pl.multiple_of(p * b_w, 128), b_w)
        bv, cv, xv = bc[:, b_at], cc[:, b_at], xc[:, x_at]
        cols = rolled(cum_ref, p)
        parts = []
        for g in range(2):
            scores = lax.dot_general(
                cv[:, g * STATE : (g + 1) * STATE],
                bv[:, g * STATE : (g + 1) * STATE],
                (((1,), (1,)), ((), ())),
                preferred_element_type=F32,
            )
            for i in range(per_pair // 2):
                h = g * (per_pair // 2) + i
                hf = p * per_pair + h
                gap_f = cols[:, h : h + 1] - cum_t[pl.ds(hf, 1), :]
                gap_b = cols[:, heads + h : heads + h + 1] - cum_t[pl.ds(heads + hf, 1), :]
                gap = jnp.where(lane < row, gap_f, jnp.where(lane > row, gap_b, 0.0))
                rf, rb = rate_t[pl.ds(hf, 1), :], rate_t[pl.ds(heads + hf, 1), :]
                scale = jnp.where(lane < row, rf, jnp.where(lane > row, rb, rf + rb))
                parts.append((scores * jnp.exp(gap) * scale).astype(BF16))
        for k in range(tiles):
            xt = xv[:, k * 128 : (k + 1) * 128]
            zero = jnp.zeros_like(xt)
            both = jnp.concatenate([jnp.where(left, xt, zero), jnp.where(left, zero, xt)], axis=0)
            w = jnp.concatenate([parts[2 * k], parts[2 * k + 1]], axis=1)
            y_ref[:, pl.ds(pl.multiple_of(p * x_w + k * 128, 128), 128)] = jnp.dot(
                w, both, preferred_element_type=F32
            )
        return 0

    def copy(src, dst, send, recv, level, member):
        return pltpu.make_async_remote_copy(
            src_ref=src,
            dst_ref=dst,
            send_sem=send,
            recv_sem=recv,
            device_id=member_id(level, member),
            device_id_type=pl.DeviceIdType.MESH,
        )

    every_level = levels + (top,)
    head_share = heads // chunks
    bases = [jnp.int32(0)]
    size = head_share
    for level in levels:
        size = size // level[1]
        bases.append(bases[-1] + digit_of(level) * size)
    pending = [[] for _ in range(chunks)]

    def head_rows(h):
        return pl.ds(pl.multiple_of(h * HEAD_DIM, HEAD_DIM), HEAD_DIM)

    def log_copy(k, member, slot):
        sem = log_sem[k]
        return copy(
            logs[k], up_log[k].at[slot], sem.at[0, member], sem.at[1, slot], every_level[k], member
        )

    def start_up(c, k):
        level = every_level[k]
        n, me = level[1], digit_of(level)
        total, sem = totals[c][k], sems[c][k]
        rows = total.shape[1] // n
        for o in range(1, n):
            m = lax.rem(me + o, n)
            if c == 0:
                pending[c].append(log_copy(k, m, me))
            if k < depth:
                part = total.at[:, pl.ds(pl.multiple_of(m * rows, 64), rows), :]
            else:
                part = total.at[jnp.where(m < me, 1, 0)]
            pending[c].append(
                copy(part, up[c][k].at[me], sem.at[0, m], sem.at[1, me], level, m)
            )
        for one in pending[c]:
            one.start()
        if k < depth:
            up[c][k][me] = total[:, pl.ds(pl.multiple_of(me * rows, 64), rows), :]
        if c == 0:
            up_log[k][me] = logs[k][...]

    def flush(c):
        for one in pending[c]:
            one.wait_send()
        pending[c].clear()

    def finish_up(c, k):
        level = every_level[k]
        n, me = level[1], digit_of(level)
        total, sem = totals[c][k], sems[c][k]
        flush(c)
        for o in range(1, n):
            s = lax.rem(me + o, n)
            if c == 0:
                log_copy(k, s, s).wait_recv()
            part = total.at[:, pl.ds(0, total.shape[1] // n), :] if k < depth else total.at[0]
            copy(part, up[c][k].at[s], sem.at[0, s], sem.at[1, s], level, s).wait_recv()
        if c == 0:

            def expand(m, _):
                decay[k][m] = jnp.exp(jnp.broadcast_to(up_log[k][m][0:1, :], (128, 128)).T)
                return 0

            lax.fori_loop(0, n, expand, 0)
            if k < depth:
                log_sum = up_log[k][0]
                for m in range(1, n):
                    log_sum = log_sum + up_log[k][m]
                logs[k + 1][...] = log_sum

    def gather(c, k):
        n = levels[k][1]
        base = c * head_share + bases[k + 1]
        part, new = up[c][k], totals[c][k + 1]

        def one_head(h, _):
            at = head_rows(h)
            f = part[0, 0, at, :].astype(F32)
            b = part[n - 1, 1, at, :].astype(F32)
            for m in range(1, n):
                r = n - 1 - m
                f = f * decay[k][m, pl.ds(base + h, 1), :] + part[m, 0, at, :].astype(F32)
                b = b * decay[k][r, pl.ds(heads + base + h, 1), :] + part[r, 1, at, :].astype(F32)
            new[0, at, :] = f.astype(BF16)
            new[1, at, :] = b.astype(BF16)
            return 0

        lax.fori_loop(0, new.shape[1] // HEAD_DIM, one_head, 0)

    def enter(c):
        n, me = top[1], digit_of(top)
        base = c * head_share + bases[-1]
        into = incoming[c]
        into[...] = jnp.zeros_like(into)

        def carry(s, d):
            def one_head(h, _):
                at = head_rows(h)
                factor = decay[depth][s, pl.ds(d * heads + base + h, 1), :]
                into[d, at, :] = into[d, at, :] * factor + up[c][depth][s, at, :].astype(F32)
                return 0

            lax.fori_loop(0, into.shape[1] // HEAD_DIM, one_head, 0)
            return 0

        lax.fori_loop(0, me, lambda s, _: carry(s, 0), 0)
        lax.fori_loop(0, n - 1 - me, lambda i, _: carry(n - 1 - i, 1), 0)

    def start_down(c, k):
        level = levels[k]
        n, me = level[1], digit_of(level)
        sem = sems[c][k]
        rows = totals[c][k].shape[1] // n
        base = c * head_share + bases[k + 1]
        source = incoming[c] if k == depth - 1 else down[c][k + 1]
        part, out = up[c][k], stage[c][k]

        def spread(h, _):
            at = head_rows(h)
            f = source[0, at, :].astype(F32)
            b = source[1, at, :].astype(F32)
            for m in range(n):
                r = n - 1 - m
                out[m, 0, at, :] = f.astype(BF16)
                out[r, 1, at, :] = b.astype(BF16)
                if m < n - 1:
                    f = f * decay[k][m, pl.ds(base + h, 1), :] + part[m, 0, at, :].astype(F32)
                    down_factor = decay[k][r, pl.ds(heads + base + h, 1), :]
                    b = b * down_factor + part[r, 1, at, :].astype(F32)
            return 0

        lax.fori_loop(0, rows // HEAD_DIM, spread, 0)
        mine = pl.ds(pl.multiple_of(me * rows, 64), rows)
        for o in range(1, n):
            m = lax.rem(me + o, n)
            pending[c].append(
                copy(out.at[m], down[c][k].at[:, mine, :], sem.at[2, m], sem.at[3, me], level, m)
            )
        for one in pending[c]:
            one.start()
        down[c][k][:, mine, :] = out[me]

    def finish_down(c, k):
        level = levels[k]
        n, me = level[1], digit_of(level)
        sem = sems[c][k]
        rows = totals[c][k].shape[1] // n
        flush(c)
        for o in range(1, n):
            s = lax.rem(me + o, n)
            theirs = pl.ds(pl.multiple_of(s * rows, 64), rows)
            copy(
                stage[c][k].at[s], down[c][k].at[:, theirs, :], sem.at[2, s], sem.at[3, s], level, s
            ).wait_recv()

    for c in range(chunks):
        lax.fori_loop(c * share, (c + 1) * share, functools.partial(first, c), 0)
        start_up(c, 0)
    for o in range(1, sp):
        for i in range(5):
            param_copy(i, lax.rem(here + o, sp), here).wait_send()
    for direction, present in ((0, has_next), (1, has_prev)):

        @pl.when(present)
        def _(direction=direction):
            for i in range(3):
                edge_copy(i, direction).wait_send()


    gaps = chunks * depth
    cuts = [(i * pairs) // gaps for i in range(gaps + 1)]
    for k in range(depth):
        for c in range(chunks):
            finish_up(c, k)
            gather(c, k)
            start_up(c, k + 1)
            at = k * chunks + c
            lax.fori_loop(cuts[at], cuts[at + 1], inner, 0)
    for c in range(chunks):
        finish_up(c, depth)
        enter(c)
        start_down(c, depth - 1)
    for k in reversed(range(1, depth)):
        for c in range(chunks):
            finish_down(c, k)
            start_down(c, k - 1)

    cum_ref[...] = jnp.exp(cum_ref[...])

    def last_part(c, p, _):
        cv = cc[:, pl.ds(pl.multiple_of(p * b_w, 128), b_w)]
        cols = rolled(cum_ref, p)
        carried = []
        for d in range(2):
            st = down[c][0][d, pl.ds(pl.multiple_of((p - c * share) * x_w, 128), x_w), :]
            got = [
                lax.dot_general(
                    cv[:, g * STATE : (g + 1) * STATE],
                    st,
                    (((1,), (1,)), ((), ())),
                    preferred_element_type=F32,
                )
                for g in range(2)
            ]
            carried.append(got)
        for k in range(tiles):
            cut = slice(k * 128, (k + 1) * 128)
            at = pl.ds(pl.multiple_of(p * x_w + k * 128, 128), 128)
            y = y_ref[:, at]
            for d in range(2):
                a, b = carried[d][0][:, cut], carried[d][1][:, cut]
                if 2 * k + 1 < per_pair // 2:
                    v = a
                elif 2 * k >= per_pair // 2:
                    v = b
                else:
                    v = jnp.where(left, a, b)
                y = y + v * two(cols, d * heads + 2 * k)
            z = z_ref[:, at].astype(F32)
            gated = y.astype(BF16).astype(F32) * (z / (1.0 + jnp.exp(-z)))
            square = gated * gated
            low = jnp.sum(jnp.where(left, square, 0.0), axis=1, keepdims=True)
            high = jnp.sum(jnp.where(left, 0.0, square), axis=1, keepdims=True)
            mean = jnp.where(left, low, high) * (1.0 / HEAD_DIM)
            out_ref[:, at] = (gated * lax.rsqrt(mean + 1e-6) * gain_ref[0:1, at]).astype(BF16)
        return 0

    for c in range(chunks):
        finish_down(c, 0)
        lax.fori_loop(c * share, (c + 1) * share, functools.partial(last_part, c), 0)


def local(sp, dp, x, b, c, z, ahead, back, spike, wx, wb, wc, offset, fading, gain):
    x, b, c, z = x[0], b[0], c[0], z[0]
    blk, x_total = x.shape
    groups = b.shape[1] // STATE
    heads = ahead.shape[2]
    pairs = groups // 2
    levels, top = levels_of(sp, dp, groups)
    scratch = [
        pltpu.VMEM((blk, x_total), BF16),
        pltpu.VMEM((blk, groups * STATE), BF16),
        pltpu.VMEM((blk, groups * STATE), BF16),
        pltpu.VMEM((blk, x_total), F32),
    ]
    scratch += [pltpu.VMEM((128, 128), F32)] * 5
    params = (wx, wb, wc, offset, fading)
    width = x_total + 2 * b.shape[1]
    early = [pltpu.VMEM((sp,) + one.shape, one.dtype) for one in params]
    early += [pltpu.VMEM((8, width), F32), pltpu.VMEM((8, 128), F32), pltpu.VMEM((8, width), F32)]
    early += [pltpu.VMEM((EDGE, one.shape[1]), BF16) for one in (x, b, c)] * 2
    early += [pltpu.SemaphoreType.DMA((2, 5, sp)), pltpu.SemaphoreType.DMA((2, 2, 3))]
    scratch += early
    split = 1
    for level in levels:
        split *= level[1]
    chunks = 2 if groups % (2 * split) == 0 else 1
    counts = [level[1] for level in levels] + [top[1]]
    scratch += [pltpu.VMEM((8, 128), F32)] * len(counts)
    scratch += [pltpu.VMEM((n, 8, 128), F32) for n in counts]
    scratch += [pltpu.VMEM((n, 128, 128), F32) for n in counts]
    scratch += [pltpu.SemaphoreType.DMA((2, n)) for n in counts]
    for _ in range(chunks):
        held = [x_total // chunks]
        for n in counts[:-1]:
            held.append(held[-1] // n)
        slabs = list(zip(counts[:-1], held[1:]))
        scratch += [pltpu.VMEM((2, rows, STATE), BF16) for rows in held]
        scratch += [pltpu.VMEM((n, 2, rows, STATE), BF16) for n, rows in slabs]
        scratch += [pltpu.VMEM((counts[-1], held[-1], STATE), BF16)]
        scratch += [pltpu.VMEM((2, rows, STATE), BF16) for rows in held[:-1]]
        scratch += [pltpu.VMEM((n, 2, rows, STATE), BF16) for n, rows in slabs]
        scratch += [pltpu.SemaphoreType.DMA((4, n)) for n in counts]
        scratch += [pltpu.VMEM((2, held[-1], STATE), F32)]
    out = pl.pallas_call(
        functools.partial(kernel, levels, top, (heads, pairs, chunks, sp, dp)),
        out_shape=jax.ShapeDtypeStruct((blk, x_total), BF16),
        in_specs=[pl.BlockSpec(memory_space=pltpu.VMEM)] * 13,
        out_specs=pl.BlockSpec(memory_space=pltpu.VMEM),
        scratch_shapes=scratch,
        compiler_params=pltpu.CompilerParams(
            collective_id=0, has_side_effects=True, vmem_limit_bytes=60 * 2**20
        ),
        name="mixer",
    )(x, b, c, z, ahead[0].T, back[0].T, spike[0].T, *params, gain.astype(F32)[None])
    return out[None]


def quad_kernel(sizes, *refs):
    heads, pairs, sp, dp = sizes
    nz = dp // 2
    rounds = nz.bit_length() - 1
    (x_hbm, b_hbm, c_hbm, z_hbm, ahead_hbm, back_hbm, spike_hbm) = refs[:7]
    params = refs[7:12]
    gain_hbm, out_ref = refs[12:14]
    (in_x, in_b, in_c, in_z, inc, inc_out, gain_in, px, pb, pc) = refs[14:24]
    own, got = refs[24:29], refs[29:34]
    edge_out, low_in, high_in = refs[34:37]
    refs = refs[:37] + (None,) * 3 + refs[37:]
    (work, w_ref, prm_ref, gain_ref, cum_ref, fac_ref, col_ref, cum_t, rate_t, mid_t) = refs[40:50]
    low_ref, high_ref, bc, zg, wide_cum = refs[50:55]
    refs = refs[:50] + refs[55:]
    (xc, bt, cc, y_ref, sup, up_in, down_out, down_in) = refs[50:58]
    (logs, qlog, zsum, zlog, dec, wup, zdec, zwt) = refs[58:66]
    (tz, zin, zs, zr, mix_out, mix_in) = refs[66:72]
    (load_sem, prm_sem, edge_sem, half_sem, inc_sem, qlog_sem, zlog_sem) = refs[72:79]
    (up_sem, zsend_sem, zrecv_sem, down_sem, mix_sem) = refs[79:84]

    hh = heads // 2
    hp = pairs // 2
    per_pair = heads // pairs
    tiles = per_pair * HEAD_DIM // 128
    blk = in_x.shape[0]
    tokens = 2 * blk
    x_half = in_x.shape[1] // 2
    b_half = in_b.shape[1] // 2
    x_w = per_pair * HEAD_DIM
    mesh_id = pl.DeviceIdType.MESH

    here, there = lax.axis_index("sp"), lax.axis_index("dp")
    core, cx = lax.rem(here, 2), here // 2
    cy, cz = lax.rem(there, 2), there // 2
    other = 1 - core
    me = cy * 2 + cx
    chip = there * 2 + cx
    chips = dp * 2
    has_next, has_prev = chip < chips - 1, chip > 0
    after, before = lax.rem(chip + 1, chips), lax.rem(chip + chips - 1, chips)
    partner = {"sp": cx * 2 + other}

    def chip_id(c, k):
        return {"sp": lax.rem(c, 2) * 2 + k, "dp": c // 2}

    def quad_id(qy, qx):
        return {"sp": qx * 2 + core, "dp": cz * 2 + qy}

    def z_id(z):
        return {"dp": z * 2 + cy}

    def member(i):
        qy = lax.rem(cy + lax.rem(i + 1, 2), 2)
        qx = lax.rem(cx + (3 - i) // 2, 2)
        return qy, qx, qy * 2 + qx

    def remote(src, dst, send, recv, target):
        return pltpu.make_async_remote_copy(
            src_ref=src, dst_ref=dst, send_sem=send, recv_sem=recv,
            device_id=target, device_id_type=mesh_id,
        )

    barrier = pltpu.get_barrier_semaphore()

    def greet(target):
        pl.semaphore_signal(barrier, inc=1, device_id=target, device_id_type=mesh_id)

    for o in range(1, sp):
        greet({"sp": lax.rem(here + o, sp)})
    for i in range(3):
        qy, qx, _ = member(i)
        greet(quad_id(qy, qx))
    for o in range(1, nz):
        greet(z_id(lax.rem(cz + o, nz)))
    for present, neighbour in ((has_next, after), (has_prev, before)):

        @pl.when(present)
        def _(neighbour=neighbour):
            for k in range(2):
                greet(chip_id(neighbour, k))

    loads = []

    def load(src, dst):
        one = pltpu.make_async_copy(src, dst, load_sem.at[len(loads)])
        one.start()
        loads.append(one)
        return one

    param_loads = [load(params[i], own[i]) for i in range(5)]
    mine = pl.ds(pl.multiple_of(core * hh, 8), hh)
    theirs = pl.ds(pl.multiple_of(other * hh, 8), hh)
    raw = (ahead_hbm, back_hbm, spike_hbm)
    for i in range(3):
        pltpu.make_async_copy(raw[i].at[theirs, :], inc_out.at[i], load_sem.at[10]).start()
        pltpu.make_async_copy(raw[i].at[mine, :], inc.at[core, i], load_sem.at[11]).start()
    b_load = load(b_hbm, in_b)
    x_load = load(x_hbm, in_x)
    c_load = load(c_hbm, in_c)

    for spot in range(2 * hp):
        work[spot, 0:8, :] = jnp.zeros((8, 128), F32)
        work[spot, 8 + tokens :, :] = jnp.zeros((8, 128), F32)
    low_ref[...] = jnp.zeros_like(low_ref)
    high_ref[...] = jnp.zeros_like(high_ref)
    for one in param_loads:
        one.wait()
    pltpu.make_async_copy(inc_out, inc_out, load_sem.at[10]).wait()
    chip_greets = 2 * ((chip + chips - 1) // chips + (2 * chips - 2 - chip) // chips)
    pl.semaphore_wait(barrier, (sp - 1) + 3 + (nz - 1) + chip_greets)

    holder = here // 2
    slot = lax.rem(here, 2)

    def param_copy(i, x):
        return remote(
            own[i], got[i].at[slot], prm_sem.at[0, i, x], prm_sem.at[1, i, slot],
            {"sp": x * 2 + holder},
        )

    for x in range(2):
        elsewhere = x * 2 + holder != here

        @pl.when(elsewhere)
        def _(x=x):
            for i in range(5):
                param_copy(i, x).start()

        @pl.when(jnp.logical_not(elsewhere))
        def _():
            for i in range(5):
                got[i][slot] = own[i][...]

    inc_copy = remote(inc_out, inc.at[core], inc_sem.at[0], inc_sem.at[1], partner)
    inc_copy.start()

    sources = (in_x, in_b, in_c)
    halves = (x_half, b_half, b_half)

    edge_from = (0, x_half // 128, (x_half + b_half) // 128)

    def edge_copy(low, k):
        return remote(
            edge_out.at[k], low_in if low else high_in, edge_sem.at[0, k],
            edge_sem.at[1, 0 if low else 1], chip_id(after if low else before, k),
        )

    sends_low = jnp.logical_and(core == 1, has_next)
    sends_high = jnp.logical_and(core == 0, has_prev)

    def half_copy(i):
        cut = pl.ds(pl.multiple_of(other * halves[i], 128), halves[i])
        return remote(
            sources[i].at[:, cut], (px, pb, pc)[i], half_sem.at[0, i], half_sem.at[1, i], partner
        )

    for one in (b_load, x_load, c_load):
        one.wait()
    slab = edge_out.shape[2]
    for k in range(2):
        picked = [[], []]
        for i in range(3):
            for t in range(halves[i] // 128):
                at = slice(k * halves[i] + t * 128, k * halves[i] + (t + 1) * 128)
                end = sources[i][blk - EDGE :, at].astype(F32)[EDGE - 2 :]
                start = sources[i][0:EDGE, at].astype(F32)[0:2]
                both = jnp.where(core == 1, end, start)
                for r in range(2):
                    picked[r].append(both[r : r + 1])
        for r in range(2):
            spare = jnp.zeros((slab - len(picked[r]), 128), F32)
            edge_out[k, r] = jnp.concatenate(picked[r] + [spare], axis=0).astype(BF16)
    for low, sends in ((True, sends_low), (False, sends_high)):

        @pl.when(sends)
        def _(low=low):
            for k in range(2):
                edge_copy(low, k).start()

    for i in (1, 0):
        half_copy(i).start()
    gain_load = load(gain_hbm, gain_in)
    z_load = load(z_hbm, in_z)

    lane = lax.broadcasted_iota(jnp.int32, (blk, 128), 1)
    row = lax.broadcasted_iota(jnp.int32, (blk, 128), 0)
    left = lane < HEAD_DIM
    left1 = left[0:1]
    lower = (lane <= row).astype(F32)
    upper = (lane >= row).astype(F32)
    filler = jnp.zeros((128 - 2 * hh, blk), F32)

    for q in range(2):
        from_q = 2 * core + q != here

        @pl.when(from_q)
        def _(q=q):
            for i in range(5):
                remote(
                    own[i], got[i].at[q], prm_sem.at[0, i, 0], prm_sem.at[1, i, q], partner
                ).wait_recv()

    pltpu.make_async_copy(inc.at[core], inc.at[core], load_sem.at[11]).wait()
    remote(inc_out, inc.at[other], inc_sem.at[0], inc_sem.at[1], partner).wait_recv()

    def half_wait(i):
        remote(
            sources[i].at[:, pl.ds(0, halves[i])], (px, pb, pc)[i], half_sem.at[0, i],
            half_sem.at[1, i], partner,
        ).wait_recv()

    def rolled(v, p):
        return pltpu.roll(v, lax.rem(128 - p * per_pair, 128), 1)

    def two(cols, i):
        mask = lax.broadcasted_iota(jnp.int32, (cols.shape[0], 128), 1) < HEAD_DIM
        return jnp.where(mask, cols[:, i : i + 1], cols[:, i + 1 : i + 2])

    tiles_of = [half // 128 for half in halves]
    starts = (0, tiles_of[0], tiles_of[0] + tiles_of[1])

    def silu(s):
        h = 0.5 * s
        return h + h * jnp.tanh(h)

    def store(i, t, rows, v):
        if i == 1:
            bc[t, rows, :] = v
        else:
            (xc, None, cc)[i][t, rows, :] = v.astype(BF16)

    def conv(i, k, base):
        for p in range(hp):
            t = p * (tiles_of[i] // hp) + k
            spot = base + p
            mine_at = pl.ds(pl.multiple_of(core * halves[i] + t * 128, 128), 128)
            at = pl.ds(pl.multiple_of(t * 128, 128), 128)
            buf = work.at[spot]
            here_at = pl.ds(pl.multiple_of(8 + core * blk, 8), blk)
            there_at = pl.ds(pl.multiple_of(8 + other * blk, 8), blk)
            buf[here_at, :] = sources[i][:, mine_at].astype(F32)
            buf[there_at, :] = (px, pb, pc)[i][:, at].astype(F32)
            s = buf[6 : 6 + tokens, :] * w_ref[starts[i] + t, 0:1, :]
            for tap in range(1, 4):
                near = buf[6 + tap : 6 + tap + tokens, :]
                s = s + near * w_ref[starts[i] + t, tap : tap + 1, :]
            store(i, t, slice(0, tokens), silu(s))

    def edge_wait():
        for low, present in ((True, has_prev), (False, has_next)):

            @pl.when(present)
            def _(low=low):
                edge_copy(low, 0).wait_recv()

    def fix(i, k):
        half = halves[i]
        mine_tiles = [p * (tiles_of[i] // hp) + k for p in range(hp)]
        row16 = row[0:16]
        lows = [low_in[r].astype(F32) for r in range(2)]
        highs = high_in[0].astype(F32)
        own_part = sources[i]
        their_part = (px, pb, pc)[i]
        for t in mine_tiles:
            mine_at = pl.ds(pl.multiple_of(core * half + t * 128, 128), 128)
            at = slice(t * 128, (t + 1) * 128)
            start = jnp.where(core == 0, own_part[0:8, mine_at], their_part[0:8, at])
            end = jnp.where(core == 1, own_part[blk - 8 :, mine_at], their_part[blk - 8 :, at])
            e = edge_from[i] + t
            for r in range(2):
                before_row = jnp.where(has_prev, lows[r][e : e + 1], 0.0)
                low_ref[t, 6 + r : 7 + r, :] = before_row
            low_ref[t, 8:16, :] = start.astype(F32)
            high_ref[t, 8:16, :] = end.astype(F32)
            high_ref[t, 16:17, :] = jnp.where(has_next, highs[e : e + 1], 0.0)
        dst = (xc, bc, cc)[i]
        for t in mine_tiles:
            for ref, low in ((low_ref, True), (high_ref, False)):
                s = ref[t, 6:14, :] * w_ref[starts[i] + t, 0:1, :]
                for k in range(1, 4):
                    s = s + ref[t, 6 + k : 14 + k, :] * w_ref[starts[i] + t, k : k + 1, :]
                s = silu(s)
                rows = slice(0, 16) if low else slice(tokens - 16, tokens)
                s = jnp.concatenate([s, s], axis=0)
                keep = row16 >= 2 if low else row16 < 15
                store(i, t, rows, jnp.where(keep, dst[t, rows, :].astype(F32), s))

    def up_copy(k, d, i):
        qy, qx, q = member(i)
        return remote(
            sup.at[k, q, d], up_in.at[k, me, d], up_sem.at[0], up_sem.at[1 + 2 * k + d],
            quad_id(qy, qx),
        )

    def wide_left(n):
        return lax.rem(lax.broadcasted_iota(jnp.int32, (128, n), 1), 128) < HEAD_DIM

    def first(k):
        for p in range(hp):
            if k < 2:
                bt[2 * p + k] = bc[2 * p + k].T.astype(BF16)
            xf = xc[p * tiles + k].astype(F32)
            rhs = jnp.concatenate(
                [(xf * wide_cum[k, p, d]).astype(BF16) for d in range(2)], axis=1
            )
            u = jnp.dot(bt[2 * p + k // 2], rhs, preferred_element_type=F32)
            if k == 1:
                v = jnp.dot(bt[2 * p + 1], rhs, preferred_element_type=F32)
                u = jnp.where(wide_left(256), u, v)
            u = u.astype(BF16)
            sup[k, p, 0] = u[:, :128]
            sup[k, p, 1] = u[:, 128:]
        for d in range(2):
            for i in range(3):
                up_copy(k, d, i).start()
        up_in[k, me] = sup[k, me]

    def inner(p, r):
        rows = slice(r * blk, (r + 1) * blk)
        cols = rolled(col_ref[rows, :], p)
        mid_row = mid_f if r == 1 else mid_b
        shift = rolled(jnp.exp(jnp.minimum(col_ref[rows, :] - mid_row, 0.0)), p)
        parts = []
        for g in range(2):
            scores = jnp.dot(cc[2 * p + g, rows], bt[2 * p + g], preferred_element_type=F32)
            on = scores[:, r * blk : (r + 1) * blk]
            away = scores[:, (1 - r) * blk : (2 - r) * blk]
            for h in range(g * per_pair // 2, (g + 1) * per_pair // 2):
                f = pl.ds(p * per_pair + h, 1)
                b = pl.ds(hh + p * per_pair + h, 1)
                gap_f = cols[:, h : h + 1] - cum_t[f, rows]
                gap_b = cols[:, hh + h : hh + h + 1] - cum_t[b, rows]
                gap = jnp.where(lane < row, gap_f, jnp.where(lane > row, gap_b, 0.0))
                rf, rb = rate_t[f, rows], rate_t[b, rows]
                scale = jnp.where(lane < row, rf, jnp.where(lane > row, rb, rf + rb))
                near = (on * jnp.exp(gap) * scale).astype(BF16)
                d = 1 - r
                c = d * hh + h
                far_rows = slice((1 - r) * blk, (2 - r) * blk)
                far_row = mid_t[f if d == 0 else b, far_rows]
                far = (away * shift[:, c : c + 1] * far_row).astype(BF16)
                parts.append(jnp.concatenate([near, far] if r == 0 else [far, near], axis=1))
        for k in range(tiles):
            xt = xc[p * tiles + k]
            zero = jnp.zeros_like(xt)
            mask = lax.broadcasted_iota(jnp.int32, xt.shape, 1) < HEAD_DIM
            both = jnp.concatenate(
                [jnp.where(mask, xt, zero), jnp.where(mask, zero, xt)], axis=0
            )
            w = jnp.concatenate([parts[2 * k], parts[2 * k + 1]], axis=1)
            y_ref[p * tiles + k, rows] = jnp.dot(w, both, preferred_element_type=F32)

    def zlog_copy(o):
        return remote(
            zsum, zlog.at[cz], zlog_sem.at[0], zlog_sem.at[1], z_id(lax.rem(cz + o, nz))
        )

    def quad_logs():
        three = qlog.at[0:3]
        remote(three, three, qlog_sem.at[0], qlog_sem.at[1], partner).wait_recv()
        zsum[...] = qlog[0] + qlog[1] + qlog[2] + qlog[3]
        for o in range(1, nz):
            zlog_copy(o).start()
        zlog[cz] = zsum[...]
        all_of = rolled(zsum[...], me)
        each_of = [rolled(qlog[q], me) for q in range(4)]
        for d in range(2):
            for k in range(tiles):
                zdec[d, k] = jnp.exp(two(all_of, d * hh + 2 * k))
                each = [two(one, d * hh + 2 * k) for one in each_of]
                reach = jnp.zeros_like(each[0])
                for q in reversed(range(4)) if d == 0 else range(4):
                    dec[q, d, k] = jnp.exp(each[q])
                    wup[q, d, k] = jnp.exp(reach)
                    reach = reach + each[q]

    def z_logs():
        rest = zlog.at[0 : nz - 1]
        remote(rest, rest, zlog_sem.at[0], zlog_sem.at[1], partner).wait_recv()
        reach = [[jnp.zeros((8, 128), F32) for _ in range(2)] for _ in range(rounds)]
        for s in range(nz):
            for r in range(rounds):
                h = 1 << r
                pos = lax.rem(cz, 2 * h)
                middle = cz - pos + h
                f_in = jnp.logical_and(s >= middle, s < cz)
                b_in = jnp.logical_and(s > cz, s < middle)
                reach[r][0] = reach[r][0] + jnp.where(f_in, zlog[s], 0.0)
                reach[r][1] = reach[r][1] + jnp.where(b_in, zlog[s], 0.0)
        for d in range(2):
            for r in range(rounds):
                total = rolled(reach[r][d], me)
                for k in range(tiles):
                    zwt[r, d, k] = jnp.exp(two(total, d * hh + 2 * k))

    def combine(k, d):
        three = up_in.at[k, 0:3, d]
        remote(three, three, up_sem.at[0], up_sem.at[1 + 2 * k + d], partner).wait_recv()
        acc = up_in[k, 0, d].astype(F32) * wup[0, d, k, 0:1, :]
        for q in range(1, 4):
            acc = acc + up_in[k, q, d].astype(F32) * wup[q, d, k, 0:1, :]
        tz[k, d] = acc
        zin[k, d] = jnp.zeros_like(acc)
        z_send(0, k, d)

    def z_copy(r, k, o, d):
        return remote(
            zs.at[r, k], zr.at[r, k], zsend_sem.at[r, o - 1], zrecv_sem.at[r, k],
            z_id(cz + o if d == 0 else cz - o),
        )

    def z_parts(r):
        h = 1 << r
        pos = lax.rem(cz, 2 * h)
        return h, pos, ((0, pos == h - 1), (1, pos == h))

    def z_send(r, k, d):
        h, _, senders = z_parts(r)

        @pl.when(senders[d][1])
        def _():
            zs[r, k] = (zin[k, d] * zdec[d, k, 0:1, :] + tz[k, d]).astype(BF16)
            for o in reversed(range(1, h + 1)):
                z_copy(r, k, o, d).start()

    def z_recv(r, k, d):
        h, pos, _ = z_parts(r)

        @pl.when(pos >= h if d == 0 else pos < h)
        def _():
            remote(
                zs.at[r, k], zr.at[r, k], zsend_sem.at[r, 0], zrecv_sem.at[r, k], partner
            ).wait_recv()
            zin[k, d] = zin[k, d] + zr[r, k].astype(F32) * zwt[r, d, k, 0:1, :]

        if r + 1 < rounds:
            z_send(r + 1, k, d)
        else:
            down(k, d)

    def down_copy(k, d, i):
        qy, qx, q = member(i)
        return remote(
            down_out.at[k, q, d], down_in.at[k, me, d], down_sem.at[0], down_sem.at[1 + k],
            quad_id(qy, qx),
        )

    def down(k, d):
        g = zin[k, d]
        order = list(range(4)) if d == 0 else list(reversed(range(4)))
        for q in order:
            down_out[k, q, d] = g.astype(BF16)
            if q != order[-1]:
                g = g * dec[q, d, k, 0:1, :] + up_in[k, q, d].astype(F32)
        for i in range(3):
            down_copy(k, d, i).start()
        down_in[k, me, d] = down_out[k, me, d]

    def gates(group, _):
        for spot in range(4):
            t = group * 4 + spot
            z = in_z[:, pl.ds(pl.multiple_of(t * 128, 128), 128)].astype(F32)
            zg[t] = silu(z)
        return 0

    def gate(mixed, t):
        gated = mixed.astype(F32) * zg[t]
        square = gated * gated
        low = jnp.sum(jnp.where(left, square, 0.0), axis=1, keepdims=True)
        high = jnp.sum(jnp.where(left, 0.0, square), axis=1, keepdims=True)
        mean = jnp.where(left, low, high) * (1.0 / HEAD_DIM)
        scale = lax.rsqrt(mean + 1e-6) * gain_ref[pl.ds(t, 1), :]
        out_ref[:, pl.ds(pl.multiple_of(t * 128, 128), 128)] = (gated * scale).astype(BF16)

    def mix_copy(k):
        return remote(
            mix_out.at[k], mix_in.at[k], mix_sem.at[0], mix_sem.at[1 + k], partner
        )

    def spread(k, ref=cum_ref):
        for j in range(2):
            cols = ref[j * blk : (j + 1) * blk, :]
            for p in range(hp):
                head = p * per_pair + 2 * k
                for d in range(2):
                    wide_cum[k, p, d, j * blk : (j + 1) * blk, :] = two(cols, d * hh + head)

    def last(k):
        three = down_in.at[k, 0:3]
        remote(three, three, down_sem.at[0], down_sem.at[1 + k], partner).wait_recv()
        for mine in (False, True):
            rows = pl.ds(pl.multiple_of((core if mine else other) * blk, 128), blk)
            for p in range(hp):
                rhs = jnp.concatenate([down_in[k, p, 0], down_in[k, p, 1]], axis=1)
                v = jnp.dot(cc[2 * p + k // 2, rows], rhs, preferred_element_type=F32)
                if k == 1:
                    u = jnp.dot(cc[2 * p + 1, rows], rhs, preferred_element_type=F32)
                    v = jnp.where(wide_left(256), v, u)
                t = p * tiles + k
                y = y_ref[t, rows] + v[:, :128] * wide_cum[k, p, 0, rows]
                y = y + v[:, 128:] * wide_cum[k, p, 1, rows]
                mixed = y.astype(BF16)
                if mine:
                    gate(mixed, core * tiles_of[0] + t)
                else:
                    mix_out[k, p] = mixed
            if not mine:
                mix_copy(k).start()

    def finish(k):
        mix_copy(k).wait_recv()
        for p in range(hp):
            gate(mix_in[k, p], other * tiles_of[0] + p * tiles + k)

    def early_sent():
        for x in range(2):

            @pl.when(x * 2 + holder != here)
            def _(x=x):
                for i in range(5):
                    param_copy(i, x).wait_send()

        for low, sends in ((True, sends_low), (False, sends_high)):

            @pl.when(sends)
            def _(low=low):
                for k in range(2):
                    edge_copy(low, k).wait_send()

        inc_copy.wait_send()
        for i in range(3):
            half_copy(i).wait_send()
        for all_of, sem in ((qlog.at[0:3], qlog_sem), (zlog.at[0 : nz - 1], zlog_sem)):
            remote(all_of, all_of, sem.at[0], sem.at[1], partner).wait_send()
        sent = sup.at[:, 0:3]
        remote(sent, sent, up_sem.at[0], up_sem.at[1], partner).wait_send()

    def z_sent():
        for r in range(rounds):
            h, _, senders = z_parts(r)

            @pl.when(jnp.logical_or(senders[0][1], senders[1][1]))
            def _(r=r, h=h):
                for o in range(h):
                    remote(
                        zs.at[r], zr.at[r], zsend_sem.at[r, o], zrecv_sem.at[r, 0], partner
                    ).wait_send()

    def rest_sent():
        sent = down_out.at[:, 0:3]
        remote(sent, sent, down_sem.at[0], down_sem.at[1], partner).wait_send()
        remote(mix_out, mix_in, mix_sem.at[0], mix_sem.at[1], partner).wait_send()

    half_wait(1)
    half_wait(0)
    prm_ref[...] = jnp.zeros_like(prm_ref)
    wide = own[3].shape[1]
    for q in range(2):
        for kind in range(2):
            for d in range(2):
                at = slice(d * hh + q * wide, d * hh + (q + 1) * wide)
                prm_ref[kind : kind + 1, at] = got[3 + kind][q, d : d + 1, :]
        off = 0
        for i in range(3):
            n = own[i].shape[1]
            part = got[i][q].astype(F32)
            for t in range(n // 128):
                w_ref[off + q * (n // 128) + t, 0:4, :] = part[:, t * 128 : (t + 1) * 128]
            off += 2 * n // 128

    cums, rates = [], []
    for j in range(2):
        pre = jnp.concatenate([inc[j, 0], inc[j, 1], filler], axis=0).T
        spikes = jnp.concatenate([inc[j, 2], inc[j, 2], filler], axis=0).T
        rate = jax.nn.softplus(pre + prm_ref[0:1, :])
        log_decay = -jnp.exp(prm_ref[1:2, :]) * rate + spikes
        cum_f = jnp.dot(lower, log_decay, precision=HIGHEST, preferred_element_type=F32)
        cum_b = jnp.dot(upper, log_decay, precision=HIGHEST, preferred_element_type=F32)
        cums.append((cum_f, cum_b))
        rates.append(rate)
    ahead_lane = lane < hh
    ahead1 = ahead_lane[0:1]
    mid_f, mid_b = cums[0][0][blk - 1 : blk], cums[1][1][0:1]
    total = jnp.where(ahead1, mid_f + cums[1][0][blk - 1 : blk], cums[0][1][0:1] + mid_b)
    logs[...] = jnp.broadcast_to(total, (8, 128))

    for j in range(2):
        cum_f, cum_b = cums[j]
        far = jnp.where(ahead_lane, mid_f if j == 1 else 0.0, mid_b if j == 0 else 0.0)
        near = jnp.where(ahead_lane, cum_f, cum_b)
        at = slice(j * blk, (j + 1) * blk)
        cum = near + far
        cum_ref[at, :] = jnp.exp(cum)
        fac_ref[at, :] = rates[j] * jnp.exp(total - cum)
        col_ref[at, :] = cum
        cum_t[:, at] = cum.T
        rate_t[:, at] = rates[j].T
        mid = rates[j] * jnp.exp(jnp.minimum((mid_f if j == 0 else mid_b) - near, 0.0))
        mid_t[:, at] = mid.T

    spread(0, fac_ref)
    conv(1, 0, 0)
    conv(0, 0, hp)
    def qlog_copy(i):
        qy, qx, q = member(i)
        return remote(
            logs, qlog.at[me], qlog_sem.at[0], qlog_sem.at[1], quad_id(qy, qx)
        )

    for i in range(3):
        qlog_copy(i).start()
    qlog[me] = logs[...]
    gain_load.wait()
    gain_ref[...] = gain_in[...].astype(F32)
    half_copy(2).start()
    edge_wait()
    fix(1, 0)
    fix(0, 0)
    first(0)
    spread(1, fac_ref)
    conv(1, 1, 0)
    conv(0, 1, hp)
    fix(1, 1)
    fix(0, 1)
    first(1)
    spread(2, fac_ref)
    conv(0, 2, 0)
    fix(0, 2)
    first(2)
    quad_logs()

    def ready_c():
        half_wait(2)
        for k in range(2):
            conv(2, k, k * hp)
        for k in range(2):
            fix(2, k)

    z_load.wait()

    up_step, z_first, z_next = 1.4, 2.7, 3.5
    plan = [(z_first - 0.01, z_logs), (0.05, ready_c)]
    for k in range(3):
        for d in range(2):
            when = up_step * (2 * k + d)
            plan.append((when, functools.partial(combine, k, d)))
            for r in range(rounds):
                plan.append((when + z_first + r * z_next, functools.partial(z_recv, r, k, d)))
    for p in range(hp):
        for r in range(2):
            when = up_step * (2 * p + r) + 0.1
            plan.append((when, functools.partial(inner, p, r)))
    all_gates = functools.partial(
        lax.fori_loop, 0, 2 * tiles_of[0] // 4, gates, 0
    )
    plan.append((up_step * 8 + 0.1, all_gates))
    done = z_first + (rounds - 1) * z_next
    plan.append((up_step * 9 + 0.1, functools.partial(spread, 0)))
    for _, step in sorted(plan, key=lambda one: one[0]):
        step()
    spread(1)
    last(0)
    spread(2)
    early_sent()
    last(1)
    finish(0)
    z_sent()
    last(2)
    finish(1)
    finish(2)
    rest_sent()


def fits_quad(sp, dp, blk, heads, groups):
    nz = dp // 2
    power = dp % 2 == 0 and nz > 1 and nz & (nz - 1) == 0
    shares = sp == 4 and groups % 4 == 0 and groups // 4 == sp
    return power and shares and blk == 128 and 2 * heads * HEAD_DIM == 3 * groups * 128


def quad_local(sp, dp, x, b, c, z, ahead, back, spike, wx, wb, wc, offset, fading, gain):
    x, b, c, z = x[0], b[0], c[0], z[0]
    blk, x_total = x.shape
    b_total = b.shape[1]
    groups = b_total // STATE
    heads = ahead.shape[2]
    pairs = groups // 2
    nz = dp // 2
    rounds = nz.bit_length() - 1
    tiles = heads // pairs * HEAD_DIM // 128
    hp, hh = pairs // 2, heads // 2
    x_half, b_half = x_total // 2, b_total // 2
    width = x_half + 2 * b_half
    slab = pl.cdiv(width // 128, 16) * 16
    params = (wx, wb, wc, offset, fading)
    vm = pltpu.VMEM
    gains = gain.reshape(x_total // 128, 128)
    scratch = [vm(one.shape, BF16) for one in (x, b, c, z)]
    scratch += [vm((2, 3, hh, blk), F32), vm((3, hh, blk), F32), vm(gains.shape, BF16)]
    scratch += [vm((blk, x_half), BF16), vm((blk, b_half), BF16), vm((blk, b_half), BF16)]
    scratch += [vm(one.shape, one.dtype) for one in params]
    scratch += [vm((2,) + one.shape, one.dtype) for one in params]
    scratch += [vm((2, 2, slab, 128), BF16)] + [vm((2, slab, 128), BF16)] * 2
    scratch += [vm((2 * hp, 2 * blk + 16, 128), F32), vm((width // 128, 8, 128), F32)]
    scratch += [vm((8, 128), F32), vm(gains.shape, F32)] + [vm((2 * blk, 128), F32)] * 3
    scratch += [vm((128, 2 * blk), F32)] * 3
    scratch += [vm((x_half // 128, 24, 128), F32)] * 2
    scratch += [vm((2 * hp, 2 * blk, STATE), F32), vm((x_total // 128, blk, 128), F32)]
    scratch += [vm((tiles, hp, 2, 2 * blk, 128), F32)]
    scratch += [vm((x_half // 128, 2 * blk, 128), BF16), vm((2 * hp, STATE, 2 * blk), BF16)]
    scratch += [vm((2 * hp, 2 * blk, 128), BF16), vm((x_half // 128, 2 * blk, 128), F32)]
    scratch += [vm((tiles, 4, 2, STATE, 128), BF16)] * 4
    scratch += [vm((8, 128), F32), vm((4, 8, 128), F32), vm((8, 128), F32), vm((nz, 8, 128), F32)]
    scratch += [vm((4, 2, tiles, 8, 128), F32)] * 2 + [vm((2, tiles, 8, 128), F32)]
    scratch += [vm((rounds, 2, tiles, 8, 128), F32)]
    scratch += [vm((tiles, 2, STATE, 128), F32)] * 2 + [vm((rounds, tiles, STATE, 128), BF16)] * 2
    scratch += [vm((tiles, hp, blk, 128), BF16)] * 2
    dma = pltpu.SemaphoreType.DMA
    scratch += [dma((12,)), dma((2, 5, 2)), dma((2, 2)), dma((2, 3)), dma((2,))]
    scratch += [dma((2,)), dma((2,)), dma((1 + 2 * tiles,)), dma((rounds, nz // 2))]
    scratch += [dma((rounds, tiles)), dma((1 + tiles,)), dma((1 + tiles,))]
    out = pl.pallas_call(
        functools.partial(quad_kernel, (heads, pairs, sp, dp)),
        out_shape=pltpu.VMEM((blk, x_total), BF16),
        in_specs=[pl.BlockSpec(memory_space=pltpu.HBM)] * 13,
        out_specs=pl.BlockSpec(memory_space=pltpu.VMEM),
        scratch_shapes=scratch,
        compiler_params=pltpu.CompilerParams(
            collective_id=0, has_side_effects=True, vmem_limit_bytes=60 * 2**20
        ),
        name="mixer",
    )(x, b, c, z, ahead[0].T, back[0].T, spike[0].T, *params, gains)
    return out[None]


def pick(sp, dp, x, b, *rest):
    blk, heads = x.shape[1], rest[2].shape[2]
    if fits_quad(sp, dp, blk, heads, b.shape[2] // STATE):
        return quad_local(sp, dp, x, b, *rest)
    return local(sp, dp, x, b, *rest)


def solution(mesh):
    tokens = P("dp", "sp", None)
    placed = (tokens,) * 7 + (P(None, "sp"),) * 5 + (P(),)
    return jax.shard_map(
        functools.partial(pick, mesh.shape["sp"], mesh.shape["dp"]),
        mesh=mesh,
        in_specs=placed,
        out_specs=tokens,
        check_vma=False,
    )
```
